128 devices in a mesh: sp: 32 (over z, y, core), tp: 4 (over x).
Axes of the slice: x: 4, y: 4, z: 4, core: 2. Of those that a mesh axis runs over, the one named last changes fastest.
Arguments:
- stream: bfloat16 [32768, 2048], P('sp'), may hold values from -6 to 6
- queries: bfloat16 [32768, 1024], P('sp', 'tp'), may hold values from -6 to 6
- projected_keys: bfloat16 [32768, 1024], P('sp', 'tp'), may hold values from -6 to 6
- values: bfloat16 [32768, 2048], P('sp', 'tp'), may hold values from -6 to 6
- decay_gate_logits: bfloat16 [32768, 1024], P('sp', 'tp'), may hold values from -7 to 7
- decay_gate_bias: float32 [1024], P('tp')
- extra_log_decay: float32 [32768, 8], P('sp', 'tp'), may hold values from -0.7 to 0
- document_index: int32 [32768], P('sp'), may hold values from 0 to 7, never falling along the last dimension, each value on 1 to 16384 neighbouring positions
- output_gate: bfloat16 [32768, 2048], P('sp', 'tp'), may hold values from -6 to 6
- head_norm_gain: bfloat16 [256], replicated, may hold values from 0.099609375 to 1.8984375
- output_weight: bfloat16 [2048, 2048], P('tp'), may hold values from -0.125 to 0.125
- feedforward_norm_gain: bfloat16 [2048], replicated, may hold values from 0.099609375 to 1.8984375
- gate_weight: bfloat16 [2048, 5632], P('sp', 'tp'), may hold values from -0.125 to 0.125
- up_weight: bfloat16 [2048, 5632], P('sp', 'tp'), may hold values from -0.125 to 0.125
- down_weight: bfloat16 [5632, 2048], P('tp', 'sp'), may hold values from -0.078125 to 0.078125
Outputs:
- updated: bfloat16 [32768, 2048], P(('sp', 'tp'))
The draws below stay inside these ranges and needn't reach their ends.
All inputs are finite; a program needn't handle non-finite values.
Results may differ from the reference program's by a relative error of at most 0.015.
Values may be sent and summed in bfloat16 or wider, within the bound.
A program may use at most 128 MiB of HBM per device.

```python
import math
import jax
import jax.numpy as jnp
import numpy as np
from jax import lax

D = 2048
FF = 5632
HEAD_TOTAL = 8
DK = 128
DV = 256
BLOCK_LENGTH = 64
TOK_DEV = 1024
TOKENS = 32768
QK = 1024
VDIM = 2048
N_SP = 32
N_TP = 4


def draw_decay_gate_logits(key, part):
    noise_key, shift_key = jax.random.split(jax.random.fold_in(key, 11))
    blocks = TOKENS // TOK_DEV
    block_shift = jax.random.uniform(shift_key, (blocks, 1, 1), jnp.float32, -0.7, 0.7)
    noise_part = jnp.clip(jax.random.normal(noise_key, (blocks, TOK_DEV, QK), jnp.float32), -6.0, 6.0)
    return (noise_part + block_shift).reshape(TOKENS, QK).astype(jnp.bfloat16)


def draw_decay_gate_bias(key, part):
    slow_key, fast_key, level_key = jax.random.split(jax.random.fold_in(key, 23), 3)
    slow_heads = jax.random.uniform(slow_key, (HEAD_TOTAL,), jnp.float32) < 0.5
    base_level = jnp.log(jnp.float32(TOKENS)) - 2.0
    slow_level = base_level + jax.random.uniform(level_key, (HEAD_TOTAL, DK), jnp.float32, 0.0, 2.0)
    fast_level = jax.random.uniform(fast_key, (HEAD_TOTAL, DK), jnp.float32, 0.0, 1.0)
    return jnp.where(slow_heads[:, None], slow_level, fast_level).reshape(HEAD_TOTAL * DK)


def draw_extra_log_decay(key, part):
    place_key, size_random_key = jax.random.split(jax.random.fold_in(key, 37))
    head_keys = jax.random.split(place_key, HEAD_TOTAL)
    orders = jax.vmap(lambda single: jax.random.permutation(single, TOKENS))(head_keys)
    places = jnp.transpose(orders[:, :3])
    extra_decay_sizes = jnp.log(jax.random.uniform(size_random_key, (3, HEAD_TOTAL), jnp.float32, 0.5, 0.8))
    positions = jnp.arange(TOKENS)[:, None, None]
    matched_positions = (positions == places[None]).astype(jnp.float32)
    return jnp.sum(matched_positions * extra_decay_sizes[None], axis=1)


def steps_of(stream_key, dims, cuts, smallest, high):
    def one(dim, blocks):
        draws = jax.random.uniform(jax.random.fold_in(jax.random.fold_in(stream_key, 6), dim), (blocks,), jnp.float32, smallest / len(cuts), high / len(cuts))
        return jnp.repeat(jnp.exp(draws), dims[dim] // blocks).reshape((-1,) + (1,) * (len(dims) - dim - 1))

    level = one(*cuts[0])
    for cut in cuts[1:]:
        level = level * one(*cut)
    return level


def split_up(number_of, total, reach, slope):
    loads = [(1 << 20) // math.isqrt(rank ** slope) + 1 for rank in range(2, number_of + 1)]
    spare, given = total - reach - (number_of - 1), [1] * (number_of - 1)
    while spare > 0:
        free = [i for i in range(number_of - 1) if given[i] < reach]
        whole, budget = sum([loads[i] for i in free]), spare
        for i in free:
            addition = min(reach - given[i], max(1, budget * loads[i] // whole), spare)
            given[i] = given[i] + addition
            spare = spare - addition
    return np.array([reach] + given)


def uneven_parts(stream_key, number_of, total, most, skew):
    if number_of == 2:
        one = jax.random.randint(stream_key, (), max(1, total - most), min(most, total - 1) + 1)
        return jnp.stack([one, total - one])
    lengths = jnp.asarray(split_up(number_of, total, most, skew), jnp.int32)
    couples = (number_of - 1) // 2
    giver, receiver = lengths[1:1 + 2 * couples:2], lengths[2:2 + 2 * couples:2]
    margin = jnp.minimum(giver - 1, most - receiver)
    passed = jax.random.randint(jax.random.fold_in(stream_key, 1), (couples,), 0, 1 << 20) % (margin + 1)
    lengths = lengths.at[1:1 + 2 * couples:2].set(giver - passed).at[2:2 + 2 * couples:2].set(receiver + passed)
    return lengths[jax.random.permutation(jax.random.fold_in(stream_key, 2), number_of)]


def gaussian(rng, dims, spread, reach, shards=(), kind=jnp.bfloat16):
    values = jax.random.normal(rng, dims, jnp.float32) * spread
    if len(shards) > 0:
        values = steps_of(rng, dims, shards, -0.22, 0.18) * values
    return jnp.clip(values, min=-reach, max=reach).astype(kind)


def setup_inputs(seed: int = 0) -> dict:
    splits = jax.random.split(jax.random.key(seed), 16)
    stream = gaussian(splits[0], (TOKENS, D), 1.0, 6.0, ((0, 32),))
    queries = gaussian(splits[1], (TOKENS, QK), 1.0, 6.0, ((0, 32), (1, 4)))
    projected_keys = gaussian(splits[2], (TOKENS, QK), 1.0, 6.0, ((0, 32), (1, 4)))
    values = gaussian(splits[3], (TOKENS, VDIM), 1.0, 6.0, ((0, 32), (1, 4)))
    decay_gate_logits = draw_decay_gate_logits(jax.random.fold_in(splits[15], 71), 0)
    decay_gate_bias = draw_decay_gate_bias(jax.random.fold_in(splits[15], 71), 0)
    extra_log_decay = draw_extra_log_decay(jax.random.fold_in(splits[15], 71), 0)
    document_index = jnp.searchsorted(jnp.cumsum(uneven_parts(splits[7], N_SP // 4, TOKENS, TOKENS // 2, 0)), jnp.arange(TOKENS), side="right").astype(jnp.int32)
    output_gate = gaussian(splits[8], (TOKENS, VDIM), 1.0, 6.0, ((0, 32), (1, 4)))
    head_norm_gain = jnp.clip(1.0 + 0.18 * jax.random.normal(splits[9], (DV,), jnp.float32), 0.099609375, 1.8984375).astype(jnp.bfloat16)
    output_weight = gaussian(splits[10], (VDIM, D), VDIM ** -0.5, 0.125, ((0, 4),))
    feedforward_norm_gain = jnp.clip(1.0 + 0.18 * jax.random.normal(splits[11], (D,), jnp.float32), 0.099609375, 1.8984375).astype(jnp.bfloat16)
    gate_weight = gaussian(splits[12], (D, FF), D ** -0.5, 0.125, ((0, 32), (1, 4)))
    up_weight = gaussian(splits[13], (D, FF), D ** -0.5, 0.125, ((0, 32), (1, 4)))
    down_weight = gaussian(splits[14], (FF, D), FF ** -0.5, 0.078125, ((0, 4), (1, 32)))
    return {"stream": stream, "queries": queries, "projected_keys": projected_keys, "values": values, "decay_gate_logits": decay_gate_logits, "decay_gate_bias": decay_gate_bias, "extra_log_decay": extra_log_decay, "document_index": document_index, "output_gate": output_gate, "head_norm_gain": head_norm_gain, "output_weight": output_weight, "feedforward_norm_gain": feedforward_norm_gain, "gate_weight": gate_weight, "up_weight": up_weight, "down_weight": down_weight}


TAU = 16.0
EPS = 1e-06
HIGH = lax.Precision.HIGHEST

def combine(earlier, later):
    decay_e, state_e, entry_e, exit_e = earlier
    decay_l, state_l, entry_l, exit_l = later
    joined = (exit_e == entry_l) | (exit_e < 0.0) | (entry_l < 0.0)
    passing = decay_l * joined.astype(decay_l.dtype)[..., None, None]
    merged_state = state_l + passing[..., None] * state_e
    merged_decay = decay_e * passing
    entry_doc = jnp.where(entry_e < 0.0, entry_l, entry_e)
    exit_doc = jnp.where(exit_l < 0.0, exit_e, exit_l)
    return (merged_decay, merged_state, entry_doc, exit_doc)

def neutral(head_number, key_channels, val_dim):
    return (jnp.ones((head_number, key_channels), jnp.float32), jnp.zeros((head_number, key_channels, val_dim), jnp.float32), jnp.full((), -1.0, jnp.float32), jnp.full((), -1.0, jnp.float32))

def block_prefix(elements, initial, reverse_dir):

    def advance(running, element):
        return (combine(running, element), running)
    totals, before = lax.scan(advance, initial, elements, reverse=reverse_dir)
    return (before, totals)

def attention_variant(queries, projected_keys, values, decay_gate_logits, decay_gate_bias, extra_log_decay, document_index, block_length):
    head_number = extra_log_decay.shape[1]
    row_number = queries.shape[0]
    blocks = row_number // block_length
    key_channels = queries.shape[1] // head_number
    val_dim = values.shape[1] // head_number
    query_f = queries.astype(jnp.float32).reshape(blocks, block_length, head_number, key_channels) * key_channels ** (-0.5)
    key_f = projected_keys.astype(jnp.float32).reshape(blocks, block_length, head_number, key_channels)
    value_b = values.reshape(blocks, block_length, head_number, val_dim)
    decay_logarithm = jax.nn.log_sigmoid(decay_gate_logits.astype(jnp.float32) + decay_gate_bias) / TAU
    decay_logarithm = decay_logarithm.reshape(row_number, head_number, key_channels) + extra_log_decay[:, :, None]
    cumulative = jnp.cumsum(decay_logarithm.reshape(blocks, block_length, head_number, key_channels), axis=1)
    document_float = document_index.astype(jnp.float32).reshape(blocks, block_length)
    middle = cumulative[:, block_length // 2 - 1:block_length // 2]
    rising = jnp.exp(cumulative - middle)
    falling = jnp.exp(middle - cumulative)
    forward = jnp.einsum('bihc,bjhc->bhij', (query_f * rising).astype(jnp.bfloat16), (key_f * falling).astype(jnp.bfloat16), preferred_element_type=jnp.float32)
    backward = jnp.einsum('bihc,bjhc->bhij', (query_f * falling).astype(jnp.bfloat16), (key_f * rising).astype(jnp.bfloat16), preferred_element_type=jnp.float32)
    offsets = jnp.arange(block_length)
    same_doc = (document_float[:, :, None] == document_float[:, None, :])[:, None]
    below_mask = offsets[None, :] <= offsets[:, None]
    above_mask = offsets[None, :] >= offsets[:, None]
    scores = jnp.where(same_doc & below_mask, forward, 0.0) + jnp.where(same_doc & above_mask, backward, 0.0)
    within_block = jnp.einsum('bhij,bjhv->bihv', scores.astype(jnp.bfloat16), value_b, preferred_element_type=jnp.float32)
    block_end = cumulative[:, block_length - 1]
    first_doc = document_float[:, 0]
    last_doc = document_float[:, block_length - 1]
    through = jnp.exp(block_end) * (first_doc == last_doc).astype(jnp.float32)[:, None, None]
    tail_mask = (document_float == last_doc[:, None]).astype(jnp.float32)[:, :, None, None]
    head_mask = (document_float == first_doc[:, None]).astype(jnp.float32)[:, :, None, None]
    tail_keys = (key_f * jnp.exp(block_end[:, None] - cumulative) * tail_mask).astype(jnp.bfloat16)
    head_keys = (key_f * jnp.exp(cumulative) * head_mask).astype(jnp.bfloat16)
    fwd_state = jnp.einsum('bjhc,bjhv->bhcv', tail_keys, value_b, preferred_element_type=jnp.float32)
    bwd_state = jnp.einsum('bjhc,bjhv->bhcv', head_keys, value_b, preferred_element_type=jnp.float32)
    forward_elements = (through, fwd_state, first_doc, last_doc)
    backward_elements = (through, bwd_state, last_doc, first_doc)
    forward_query = query_f * jnp.exp(cumulative)
    backward_query = query_f * jnp.exp(block_end[:, None] - cumulative)
    return (within_block, forward_elements, backward_elements, forward_query, backward_query, document_float)

def carried(inflow, factor, document_float):
    hit_mask = (document_float == inflow[3][:, None]).astype(jnp.float32)[:, :, None, None]
    return jnp.einsum('bihc,bhcv->bihv', factor, inflow[1], precision=HIGH) * hit_mask

def head_mix(within_block, fwd_in, bwd_in, forward_query, backward_query, document_float, output_gate, head_norm_gain, head_number):
    total_out = within_block + carried(fwd_in, forward_query, document_float) + carried(bwd_in, backward_query, document_float)
    row_number = output_gate.shape[0]
    total_out = total_out.reshape(row_number, head_number, -1)
    scaled = total_out * lax.rsqrt(lax.optimization_barrier(jnp.mean(total_out * total_out, axis=-1, keepdims=True)) + EPS)
    scaled = scaled * head_norm_gain.astype(jnp.float32)
    return (scaled.reshape(row_number, -1) * jax.nn.silu(output_gate.astype(jnp.float32))).astype(jnp.bfloat16)

def row_norm(rows_f, gain):
    factor = lax.rsqrt(lax.optimization_barrier(jnp.mean(rows_f * rows_f, axis=-1, keepdims=True)) + EPS)
    return (rows_f * factor * gain.astype(jnp.float32)).astype(jnp.bfloat16)

def reference(stream, queries, projected_keys, values, decay_gate_logits, decay_gate_bias, extra_log_decay, document_index, output_gate, head_norm_gain, output_weight, feedforward_norm_gain, gate_weight, up_weight, down_weight):
    head_number = extra_log_decay.shape[1]
    key_channels = queries.shape[1] // head_number
    val_dim = values.shape[1] // head_number
    within_block, forward_elements, backward_elements, forward_query, backward_query, document_float = attention_variant(queries, projected_keys, values, decay_gate_logits, decay_gate_bias, extra_log_decay, document_index, BLOCK_LENGTH)
    initial = neutral(head_number, key_channels, val_dim)
    fwd_in = block_prefix(forward_elements, initial, False)[0]
    bwd_in = block_prefix(backward_elements, initial, True)[0]
    head_mixed = head_mix(within_block, fwd_in, bwd_in, forward_query, backward_query, document_float, output_gate, head_norm_gain, head_number)
    col_group = values.shape[1] // N_TP
    attended = jnp.zeros(stream.shape, jnp.float32)
    for group_idx in range(N_TP):
        lower_col = group_idx * col_group
        partial_value = jnp.dot(head_mixed[:, lower_col:lower_col + col_group], output_weight[lower_col:lower_col + col_group], preferred_element_type=jnp.float32)
        attended = attended + lax.optimization_barrier(partial_value.astype(jnp.bfloat16)).astype(jnp.float32)
    resid = stream.astype(jnp.float32) + attended
    normed = row_norm(resid, feedforward_norm_gain)
    unit_group = gate_weight.shape[1] // N_TP
    mlp_out = jnp.zeros(stream.shape, jnp.float32)
    for group_idx in range(N_TP):
        lower_unit = group_idx * unit_group
        gate_act = jnp.dot(normed, gate_weight[:, lower_unit:lower_unit + unit_group], preferred_element_type=jnp.float32)
        up_act = jnp.dot(normed, up_weight[:, lower_unit:lower_unit + unit_group], preferred_element_type=jnp.float32)
        hidden = (jax.nn.silu(gate_act) * up_act).astype(jnp.bfloat16)
        partial_value = jnp.dot(hidden, down_weight[lower_unit:lower_unit + unit_group], preferred_element_type=jnp.float32)
        mlp_out = mlp_out + lax.optimization_barrier(partial_value.astype(jnp.bfloat16)).astype(jnp.float32)
    return (resid + mlp_out).astype(jnp.bfloat16)
```

```python
import functools
import jax
import jax.numpy as jnp
from jax import lax
from jax.experimental import pallas as pl
from jax.experimental.pallas import tpu as pltpu
from jax.sharding import Mesh
from jax.sharding import PartitionSpec as P

SP = ("sp_0", "sp_1", "sp_2")
SP_TP = ("sp_0", "sp_1", "sp_2", "tp")
MESH = pl.DeviceIdType.MESH
F32 = jnp.float32
BF16 = jnp.bfloat16
TAU = 16.0
EPS = 1e-06
BL = 64
GR = 256
DK = 128
DV = 256
NZ, NY = 4, 4
NCHIP = NZ * NY


def nt_dot(a, b):
    return lax.dot_general(a, b, (((1,), (1,)), ((), ())), preferred_element_type=F32)


def tn_dot(a, b):
    return lax.dot_general(a, b, (((0,), (0,)), ((), ())), preferred_element_type=F32)


def nn_dot(a, b):
    return lax.dot_general(a, b, (((1,), (0,)), ((), ())), preferred_element_type=F32)


def attention_kernel(
    q_ref, k_ref, v_ref, lg_ref, bias_ref, aux_ref, docrow_ref, gate_ref, gain_ref,
    mixed_ref,
    cum_ref, glob_ref, blk_ref, states_ref, before_ref, run_ref, local_ref,
    own_t, own_e, part_t, part_e, chip_t, chip_e, recv_t, recv_e, mine_c, send_c, part_c, sum_ref,
    core_send, core_recv, t_send, t_recv, e_send, e_recv,
):
    rows = q_ref.shape[0]
    blocks = rows // BL
    groups = rows // GR
    per = GR // BL
    z, y = lax.axis_index("sp_0"), lax.axis_index("sp_1")
    core, x = lax.axis_index("sp_2"), lax.axis_index("tp")
    chip = z * NY + y
    scale = DK ** (-0.5)

    def chip_peer(k):
        other = lax.rem(chip + k, NCHIP)
        return other, (other // NY, lax.rem(other, NY), core, x)

    partner = (z, y, 1 - core, x)

    recv_t[pl.ds(chip, 1)] = jnp.zeros((1, DV, DK), BF16)

    barrier = pltpu.get_barrier_semaphore()
    pl.semaphore_signal(barrier, inc=1, device_id=partner, device_id_type=MESH)
    for k in range(1, NCHIP):
        pl.semaphore_signal(barrier, inc=1, device_id=chip_peer(k)[1], device_id_type=MESH)

    ri = lax.broadcasted_iota(jnp.int32, (GR, GR), 0)
    ci = lax.broadcasted_iota(jnp.int32, (GR, GR), 1)

    def first(g, base):
        at = pl.multiple_of(g * GR, GR)
        same_block = (ri & (GR - BL)) == (ci & (GR - BL))
        tri = jnp.where(same_block & (ci <= ri), 1.0, 0.0).astype(BF16)
        logits = lg_ref[pl.ds(at, GR), :].astype(F32) + bias_ref[...]
        ld = (jnp.minimum(logits, 0.0) - jnp.log1p(jnp.exp(-jnp.abs(logits)))) / TAU
        extra0 = jnp.broadcast_to(aux_ref[pl.ds(at, GR), 0:1], (GR, DK))
        extra1 = jnp.broadcast_to(aux_ref[pl.ds(at, GR), 1:2], (GR, DK))
        ld = ld + jnp.concatenate([extra0, extra1], axis=1)
        hi = ld.astype(BF16)
        rest = ld - hi.astype(F32)
        mid = rest.astype(BF16)
        low = (rest - mid.astype(F32)).astype(BF16)
        cum = nn_dot(tri, hi) + nn_dot(tri, mid) + nn_dot(tri, low)
        cum_ref[pl.ds(at, GR), :] = cum
        cum3 = cum.reshape(per, BL, 2 * DK)
        ends = cum3[:, BL - 1 : BL, :]
        off, offs = base, []
        for b in range(per):
            offs.append(off)
            blk_ref[pl.ds(g * per + b, 1)] = ends[b : b + 1]
            off = off + ends[b]
        for b in range(per):
            glob_ref[pl.ds(pl.multiple_of(at + b * BL, BL), BL), :] = cum3[b] + offs[b]
        doc = aux_ref[pl.ds(at, GR), 2:3].reshape(per, BL, 1)
        tail_mask = jnp.where(doc == doc[:, BL - 1 : BL], 1.0, 0.0)
        head_mask = jnp.where(doc == doc[:, 0:1], 1.0, 0.0)
        kf = k_ref[pl.ds(at, GR), :].astype(F32).reshape(per, BL, 2 * DK)
        tail = (kf * jnp.exp(ends - cum3) * tail_mask).astype(BF16)
        head = (kf * jnp.exp(cum3) * head_mask).astype(BF16)
        for b in range(per):
            for h in range(2):
                keys = jnp.concatenate(
                    [tail[b][:, h * DK : (h + 1) * DK], head[b][:, h * DK : (h + 1) * DK]], axis=1
                )
                vals = v_ref[pl.ds(pl.multiple_of(at + b * BL, BL), BL), h * DV : (h + 1) * DV]
                states_ref[pl.ds((g * per + b) * 2 + h, 1)] = tn_dot(vals, keys)[None]
        return off

    total = lax.fori_loop(0, groups, first, jnp.zeros((1, 2 * DK), F32))
    sum_ref[...] = total

    run_ref[...] = jnp.zeros_like(run_ref)

    def doc_at(r):
        return aux_ref[pl.ds(r, 1), 2:3]

    def step(b, _):
        lo = jnp.maximum(b * BL - 1, 0)
        keep = jnp.where(doc_at(lo) == doc_at(b * BL + BL - 1), 1.0, 0.0)
        decay = jnp.exp(blk_ref[pl.ds(b, 1)][0]) * keep
        r = blocks - 1 - b
        hi = jnp.minimum(r * BL + BL, rows - 1)
        keep_b = jnp.where(doc_at(hi) == doc_at(r * BL), 1.0, 0.0)
        decay_b = jnp.exp(blk_ref[pl.ds(r, 1)][0]) * keep_b
        for h in range(2):
            fw = run_ref[h, :, :DK]
            before_ref[pl.ds(b * 2 + h, 1), :, :DK] = fw.astype(BF16)[None]
            run_ref[h, :, :DK] = fw * decay[:, h * DK : (h + 1) * DK] + states_ref[b * 2 + h, :, :DK]
            bw = run_ref[h, :, DK:]
            before_ref[pl.ds(r * 2 + h, 1), :, DK:] = bw.astype(BF16)[None]
            run_ref[h, :, DK:] = bw * decay_b[:, h * DK : (h + 1) * DK] + states_ref[r * 2 + h, :, DK:]
        return 0

    lax.fori_loop(0, blocks, step, 0)
    first_doc = jnp.broadcast_to(doc_at(0), (1, DK))
    last_doc = jnp.broadcast_to(doc_at(rows - 1), (1, DK))
    for h in range(2):
        own_t[h, :DV] = run_ref[h, :, :DK].astype(BF16)
        own_t[h, DV:] = run_ref[h, :, DK:].astype(BF16)
        own_e[h, 0:1] = total[:, h * DK : (h + 1) * DK]
        own_e[h, 1:2] = first_doc
        own_e[h, 2:3] = last_doc
        own_e[h, 3:8] = jnp.zeros((5, DK), F32)

    pl.semaphore_wait(barrier, NCHIP)
    swap_t = pltpu.make_async_remote_copy(
        own_t.at[1 - core], part_t, core_send.at[0], core_recv.at[0],
        device_id=partner, device_id_type=MESH)
    swap_e = pltpu.make_async_remote_copy(
        own_e.at[1 - core], part_e, core_send.at[1], core_recv.at[1],
        device_id=partner, device_id_type=MESH)
    swap_t.start()
    swap_e.start()
    swap_t.wait()
    swap_e.wait()
    is0 = core == 0
    mine_e = own_e[pl.ds(core, 1)][0]
    other_e = part_e[...]
    e0 = jnp.where(is0, mine_e, other_e)
    e1 = jnp.where(is0, other_e, mine_e)
    mine_t = own_t[pl.ds(core, 1)][0].astype(F32)
    other_t = part_t[...].astype(F32)
    t0 = jnp.where(is0, mine_t, other_t)
    t1 = jnp.where(is0, other_t, mine_t)
    through1 = jnp.exp(e1[0:1]) * jnp.where(e0[2:3] == e1[2:3], 1.0, 0.0)
    through0 = jnp.exp(e0[0:1]) * jnp.where(e1[1:2] == e0[1:2], 1.0, 0.0)
    chip_t[0] = (t1[:DV] + through1 * t0[:DV]).astype(BF16)
    chip_t[1] = (t0[DV:] + through0 * t1[DV:]).astype(BF16)
    chip_row = jnp.concatenate(
        [e0[0:1] + e1[0:1], e0[1:2], e1[2:3], jnp.zeros((5, DK), F32)], axis=0)
    chip_e[...] = chip_row
    recv_e[pl.ds(chip, 1)] = chip_row[None]

    sends = []
    for k in range(1, NCHIP):
        other, target = chip_peer(k)
        back = jnp.where(other > chip, 0, 1)
        sends.append(pltpu.make_async_remote_copy(
            chip_e, recv_e.at[chip], e_send.at[k], e_recv.at[k],
            device_id=target, device_id_type=MESH))
        sends.append(pltpu.make_async_remote_copy(
            chip_t.at[back], recv_t.at[chip], t_send.at[k], t_recv.at[k],
            device_id=target, device_id_type=MESH))
    for s in sends:
        s.start()

    def inside(g, _):
        at = pl.multiple_of(g * GR, GR)
        same_block = (ri & (GR - BL)) == (ci & (GR - BL))
        doc = aux_ref[pl.ds(at, GR), 2:3]
        same = same_block & (doc == docrow_ref[pl.ds(g, 1), :])
        below = same & (ci <= ri)
        above = same & (ci >= ri)
        cum3 = cum_ref[pl.ds(at, GR), :].reshape(per, BL, 2 * DK)
        middle = cum3[:, BL // 2 - 1 : BL // 2]
        ends = cum3[:, BL - 1 : BL]
        rising = jnp.exp(cum3 - middle)
        falling = jnp.exp(middle - cum3)
        qf = q_ref[pl.ds(at, GR), :].astype(F32).reshape(per, BL, 2 * DK) * scale
        kf = k_ref[pl.ds(at, GR), :].astype(F32).reshape(per, BL, 2 * DK)
        q_rise = (qf * rising).astype(BF16).reshape(GR, 2 * DK)
        q_fall = (qf * falling).astype(BF16).reshape(GR, 2 * DK)
        k_rise = (kf * rising).astype(BF16).reshape(GR, 2 * DK)
        k_fall = (kf * falling).astype(BF16).reshape(GR, 2 * DK)
        q_fwd = qf * jnp.exp(cum3)
        q_bwd = qf * jnp.exp(ends - cum3)
        for h in range(2):
            c = slice(h * DK, (h + 1) * DK)
            fw = nt_dot(q_rise[:, c], k_fall[:, c])
            bw = nt_dot(q_fall[:, c], k_rise[:, c])
            scores = jnp.where(below, fw, 0.0) + jnp.where(above, bw, 0.0)
            vals = v_ref[pl.ds(at, GR), h * DV : (h + 1) * DV]
            local_ref[pl.ds(at, GR), h * DV : (h + 1) * DV] = nn_dot(scores.astype(BF16), vals)
        for b in range(per):
            start = at + b * BL
            prev = doc_at(jnp.maximum(start - 1, 0))
            following = doc_at(jnp.minimum(start + BL, rows - 1))
            rows_doc = doc[b * BL : (b + 1) * BL]
            hit_f = jnp.where(rows_doc == prev, 1.0, 0.0)
            hit_b = jnp.where(rows_doc == following, 1.0, 0.0)
            for h in range(2):
                c = slice(h * DK, (h + 1) * DK)
                both = jnp.concatenate([q_fwd[b][:, c] * hit_f, q_bwd[b][:, c] * hit_b], axis=1)
                here = pl.ds(pl.multiple_of(start, BL), BL)
                local_ref[here, h * DV : (h + 1) * DV] += nt_dot(
                    both.astype(BF16), before_ref[(g * per + b) * 2 + h])
        return 0

    lax.fori_loop(0, groups, inside, 0)

    for s in sends:
        s.wait()
    run_ref[0] = jnp.zeros_like(run_ref[0])

    def earlier(j, _):
        e = recv_e[j]
        p = recv_e[jnp.maximum(j - 1, 0)]
        keep = jnp.exp(e[0:1]) * jnp.where(e[2:3] == p[2:3], 1.0, 0.0)
        run_ref[0, :, :DK] = recv_t[j].astype(F32) + run_ref[0, :, :DK] * keep
        return 0

    def later(i, _):
        j = NCHIP - 1 - i
        e = recv_e[j]
        p = recv_e[jnp.minimum(j + 1, NCHIP - 1)]
        keep = jnp.exp(e[0:1]) * jnp.where(e[1:2] == p[1:2], 1.0, 0.0)
        run_ref[0, :, DK:] = recv_t[j].astype(F32) + run_ref[0, :, DK:] * keep
        return 0

    lax.fori_loop(0, chip, earlier, 0)
    lax.fori_loop(0, NCHIP - 1 - chip, later, 0)
    cf, cb = run_ref[0, :, :DK], run_ref[0, :, DK:]
    before_doc = jnp.where(chip > 0, recv_e[jnp.maximum(chip - 1, 0)][2:3], -1.0)
    after_doc = jnp.where(
        chip < NCHIP - 1, recv_e[jnp.minimum(chip + 1, NCHIP - 1)][1:2], -1.0)
    pass0 = jnp.exp(e0[0:1]) * jnp.where(before_doc == e0[2:3], 1.0, 0.0)
    pass1 = jnp.exp(e1[0:1]) * jnp.where(after_doc == e1[1:2], 1.0, 0.0)
    mine_t = own_t[pl.ds(core, 1)][0].astype(F32)
    other_t = part_t[...].astype(F32)
    t0f = jnp.where(is0, mine_t[:DV], other_t[:DV])
    t1b = jnp.where(is0, other_t[DV:], mine_t[DV:])
    c0 = jnp.concatenate([cf, t1b + pass1 * cb], axis=1)
    c1 = jnp.concatenate([t0f + pass0 * cf, cb], axis=1)
    mine_c[...] = jnp.where(is0, c0, c1).astype(BF16)
    send_c[...] = jnp.where(is0, c1, c0).astype(BF16)
    swap_c = pltpu.make_async_remote_copy(
        send_c, part_c, core_send.at[2], core_recv.at[2],
        device_id=partner, device_id_type=MESH)
    swap_c.start()
    enter_f = jnp.where(is0, before_doc, e0[2:3])[:, 0:1]
    enter_b = jnp.where(is0, e1[1:2], after_doc)[:, 0:1]
    swap_c.wait()

    def last(g, _):
        at = pl.multiple_of(g * GR, GR)
        doc = aux_ref[pl.ds(at, GR), 2:3]
        hit_f = jnp.where(doc == enter_f, 1.0, 0.0)
        hit_b = jnp.where(doc == enter_b, 1.0, 0.0)
        glob = glob_ref[pl.ds(at, GR), :]
        qf = q_ref[pl.ds(at, GR), :].astype(F32) * scale
        q_fwd = (qf * jnp.exp(glob) * hit_f).astype(BF16)
        q_bwd = (qf * jnp.exp(sum_ref[...] - glob) * hit_b).astype(BF16)
        gain = gain_ref[...].astype(F32)
        for h in range(2):
            c = slice(h * DK, (h + 1) * DK)
            both = jnp.concatenate([q_fwd[:, c], q_bwd[:, c]], axis=1)
            carry = jnp.where(h == core, mine_c[...], part_c[...])
            out = local_ref[pl.ds(at, GR), h * DV : (h + 1) * DV] + nt_dot(both, carry)
            out = out * lax.rsqrt(jnp.mean(out * out, axis=-1, keepdims=True) + EPS) * gain
            u = gate_ref[pl.ds(at, GR), h * DV : (h + 1) * DV].astype(F32)
            mixed_ref[pl.ds(at, GR), h * DV : (h + 1) * DV] = (
                out * (u / (1.0 + jnp.exp(-u)))).astype(BF16)
        return 0

    lax.fori_loop(0, groups, last, 0)


def attention(q, k, v, lg, bias, extra, doc, gate, gain):
    rows = q.shape[0]
    doc_f = doc.astype(F32)
    aux = jnp.concatenate([extra, doc_f[:, None]], axis=1)
    docrow = doc_f.reshape(rows // GR, GR)
    vm = pl.BlockSpec(memory_space=pltpu.VMEM)
    blocks = rows // BL
    return pl.pallas_call(
        attention_kernel,
        out_shape=jax.ShapeDtypeStruct((rows, 2 * DV), BF16),
        in_specs=[vm] * 9,
        out_specs=vm,
        scratch_shapes=[
            pltpu.VMEM((rows, 2 * DK), F32),
            pltpu.VMEM((rows, 2 * DK), F32),
            pltpu.VMEM((blocks, 1, 2 * DK), F32),
            pltpu.VMEM((blocks * 2, DV, 2 * DK), F32),
            pltpu.VMEM((blocks * 2, DV, 2 * DK), BF16),
            pltpu.VMEM((2, DV, 2 * DK), F32),
            pltpu.VMEM((rows, 2 * DV), F32),
            pltpu.VMEM((2, 2 * DV, DK), BF16),
            pltpu.VMEM((2, 8, DK), F32),
            pltpu.VMEM((2 * DV, DK), BF16),
            pltpu.VMEM((8, DK), F32),
            pltpu.VMEM((2, DV, DK), BF16),
            pltpu.VMEM((8, DK), F32),
            pltpu.VMEM((NCHIP, DV, DK), BF16),
            pltpu.VMEM((NCHIP, 8, DK), F32),
            pltpu.VMEM((DV, 2 * DK), BF16),
            pltpu.VMEM((DV, 2 * DK), BF16),
            pltpu.VMEM((DV, 2 * DK), BF16),
            pltpu.VMEM((1, 2 * DK), F32),
            pltpu.SemaphoreType.DMA((3,)),
            pltpu.SemaphoreType.DMA((3,)),
            pltpu.SemaphoreType.DMA((NCHIP,)),
            pltpu.SemaphoreType.DMA((NCHIP,)),
            pltpu.SemaphoreType.DMA((NCHIP,)),
            pltpu.SemaphoreType.DMA((NCHIP,)),
        ],
        compiler_params=pltpu.CompilerParams(
            collective_id=0, has_side_effects=True, vmem_limit_bytes=48 * 2**20),
        cost_estimate=pl.CostEstimate(flops=3_000_000_000, bytes_accessed=8_000_000, transcendentals=0),
        name="attention",
    )(q, k, v, lg, bias.reshape(1, -1), aux, docrow, gate, gain.reshape(1, -1))


def row_norm(rows_f, gain):
    factor = lax.rsqrt(jnp.mean(rows_f * rows_f, axis=-1, keepdims=True) + EPS)
    return (rows_f * factor * gain.astype(F32)).astype(BF16)


def per_device(
    stream, queries, projected_keys, values, decay_gate_logits, decay_gate_bias, extra_log_decay,
    document_index, output_gate, head_norm_gain, output_weight, feedforward_norm_gain,
    gate_weight, up_weight, down_weight,
):
    both = lax.all_gather(jnp.concatenate([gate_weight, up_weight], axis=1), SP, axis=0, tiled=True)
    width = gate_weight.shape[1]
    whole_gate, whole_up = both[:, :width], both[:, width:]
    down = lax.all_gather(down_weight, SP)
    whole_down = jnp.moveaxis(down, 0, 1).reshape(down_weight.shape[0], -1)
    head_mixed = attention(
        queries, projected_keys, values, decay_gate_logits, decay_gate_bias, extra_log_decay,
        document_index, output_gate, head_norm_gain)
    tp_rows = stream.shape[0] // lax.axis_size("tp")
    tp_start = lax.axis_index("tp") * tp_rows
    partial = jnp.dot(head_mixed, output_weight, preferred_element_type=F32).astype(BF16)
    attended = lax.psum(partial, "tp").astype(F32)
    resid_all = stream.astype(F32) + attended
    normed = row_norm(resid_all, feedforward_norm_gain)
    resid_own = lax.dynamic_slice_in_dim(resid_all, tp_start, tp_rows, 0)
    gate_act = jnp.dot(normed, whole_gate, preferred_element_type=F32)
    up_act = jnp.dot(normed, whole_up, preferred_element_type=F32)
    hidden = (jax.nn.silu(gate_act) * up_act).astype(BF16)
    partial = jnp.dot(hidden, whole_down, preferred_element_type=F32).astype(BF16)
    tiles = partial.reshape(lax.axis_size("tp"), tp_rows, -1)
    arrived = lax.all_to_all(tiles, "tp", split_axis=0, concat_axis=0, tiled=True)
    return (resid_own + arrived.astype(F32).sum(axis=0)).astype(BF16)


def solution(mesh):
    torus = Mesh(mesh.devices.reshape(4, 4, 2, mesh.shape["tp"]), ("sp_0", "sp_1", "sp_2", "tp"))
    placed = (
        P(SP, None), P(SP, "tp"), P(SP, "tp"), P(SP, "tp"), P(SP, "tp"), P("tp"), P(SP, "tp"),
        P(SP), P(SP, "tp"), P(), P("tp", None), P(), P(SP, "tp"), P(SP, "tp"), P("tp", SP),
    )
    return jax.shard_map(
        per_device, mesh=torus, in_specs=placed, out_specs=P(SP_TP, None), check_vma=False
    )
```

```python
import functools
import jax
import jax.numpy as jnp
from jax import lax
from jax.experimental import pallas as pl
from jax.experimental.pallas import tpu as pltpu
from jax.sharding import Mesh
from jax.sharding import PartitionSpec as P

SP = ("sp_0", "sp_1", "sp_2")
SP_TP = ("sp_0", "sp_1", "sp_2", "tp")
MESH = pl.DeviceIdType.MESH
F32 = jnp.float32
BF16 = jnp.bfloat16
TAU = 16.0
EPS = 1e-06
BL = 64
GR = 256
DK = 128
DV = 256
NZ, NY = 4, 4
NCHIP = NZ * NY


def nt_dot(a, b):
    return lax.dot_general(a, b, (((1,), (1,)), ((), ())), preferred_element_type=F32)


def tn_dot(a, b):
    return lax.dot_general(a, b, (((0,), (0,)), ((), ())), preferred_element_type=F32)


def nn_dot(a, b):
    return lax.dot_general(a, b, (((1,), (0,)), ((), ())), preferred_element_type=F32)


def attention_kernel(
    q_ref, k_ref, v_ref, lg_ref, bias_ref, aux_ref, docrow_ref, gate_ref, gain_ref,
    mixed_ref,
    cum_ref, glob_ref, blk_ref, states_ref, before_ref, run_ref, local_ref,
    own_t, own_e, part_t, part_e, chip_t, chip_e, recv_t, recv_e, mine_c, send_c, part_c, sum_ref,
    core_send, core_recv, t_send, t_recv, e_send, e_recv,
):
    rows = q_ref.shape[0]
    blocks = rows // BL
    groups = rows // GR
    per = GR // BL
    z, y = lax.axis_index("sp_0"), lax.axis_index("sp_1")
    core, x = lax.axis_index("sp_2"), lax.axis_index("tp")
    chip = z * NY + y
    scale = DK ** (-0.5)

    def chip_peer(k):
        other = lax.rem(chip + k, NCHIP)
        return other, (other // NY, lax.rem(other, NY), core, x)

    partner = (z, y, 1 - core, x)

    recv_t[pl.ds(chip, 1)] = jnp.zeros((1, DV, DK), BF16)

    barrier = pltpu.get_barrier_semaphore()
    pl.semaphore_signal(barrier, inc=1, device_id=partner, device_id_type=MESH)
    for k in range(1, NCHIP):
        pl.semaphore_signal(barrier, inc=1, device_id=chip_peer(k)[1], device_id_type=MESH)

    ri = lax.broadcasted_iota(jnp.int32, (GR, GR), 0)
    ci = lax.broadcasted_iota(jnp.int32, (GR, GR), 1)

    def first(g, base):
        at = pl.multiple_of(g * GR, GR)
        same_block = (ri & (GR - BL)) == (ci & (GR - BL))
        tri = jnp.where(same_block & (ci <= ri), 1.0, 0.0).astype(BF16)
        logits = lg_ref[pl.ds(at, GR), :].astype(F32) + bias_ref[...]
        ld = (jnp.minimum(logits, 0.0) - jnp.log1p(jnp.exp(-jnp.abs(logits)))) / TAU
        extra0 = jnp.broadcast_to(aux_ref[pl.ds(at, GR), 0:1], (GR, DK))
        extra1 = jnp.broadcast_to(aux_ref[pl.ds(at, GR), 1:2], (GR, DK))
        ld = ld + jnp.concatenate([extra0, extra1], axis=1)
        hi = ld.astype(BF16)
        rest = ld - hi.astype(F32)
        mid = rest.astype(BF16)
        low = (rest - mid.astype(F32)).astype(BF16)
        cum = nn_dot(tri, hi) + nn_dot(tri, mid) + nn_dot(tri, low)
        cum_ref[pl.ds(at, GR), :] = cum
        cum3 = cum.reshape(per, BL, 2 * DK)
        ends = cum3[:, BL - 1 : BL, :]
        off, offs = base, []
        for b in range(per):
            offs.append(off)
            blk_ref[pl.ds(g * per + b, 1)] = ends[b : b + 1]
            off = off + ends[b]
        for b in range(per):
            glob_ref[pl.ds(pl.multiple_of(at + b * BL, BL), BL), :] = cum3[b] + offs[b]
        doc = aux_ref[pl.ds(at, GR), 2:3].reshape(per, BL, 1)
        tail_mask = jnp.where(doc == doc[:, BL - 1 : BL], 1.0, 0.0)
        head_mask = jnp.where(doc == doc[:, 0:1], 1.0, 0.0)
        kf = k_ref[pl.ds(at, GR), :].astype(F32).reshape(per, BL, 2 * DK)
        tail = (kf * jnp.exp(ends - cum3) * tail_mask).astype(BF16)
        head = (kf * jnp.exp(cum3) * head_mask).astype(BF16)
        for b in range(per):
            for h in range(2):
                keys = jnp.concatenate(
                    [tail[b][:, h * DK : (h + 1) * DK], head[b][:, h * DK : (h + 1) * DK]], axis=1
                )
                vals = v_ref[pl.ds(pl.multiple_of(at + b * BL, BL), BL), h * DV : (h + 1) * DV]
                states_ref[pl.ds((g * per + b) * 2 + h, 1)] = tn_dot(vals, keys)[None]
        return off

    total = lax.fori_loop(0, groups, first, jnp.zeros((1, 2 * DK), F32))
    sum_ref[...] = total

    run_ref[...] = jnp.zeros_like(run_ref)

    def doc_at(r):
        return aux_ref[pl.ds(r, 1), 2:3]

    def step(b, _):
        lo = jnp.maximum(b * BL - 1, 0)
        keep = jnp.where(doc_at(lo) == doc_at(b * BL + BL - 1), 1.0, 0.0)
        decay = jnp.exp(blk_ref[pl.ds(b, 1)][0]) * keep
        r = blocks - 1 - b
        hi = jnp.minimum(r * BL + BL, rows - 1)
        keep_b = jnp.where(doc_at(hi) == doc_at(r * BL), 1.0, 0.0)
        decay_b = jnp.exp(blk_ref[pl.ds(r, 1)][0]) * keep_b
        for h in range(2):
            fw = run_ref[h, :, :DK]
            before_ref[pl.ds(b * 2 + h, 1), :, :DK] = fw.astype(BF16)[None]
            run_ref[h, :, :DK] = fw * decay[:, h * DK : (h + 1) * DK] + states_ref[b * 2 + h, :, :DK]
            bw = run_ref[h, :, DK:]
            before_ref[pl.ds(r * 2 + h, 1), :, DK:] = bw.astype(BF16)[None]
            run_ref[h, :, DK:] = bw * decay_b[:, h * DK : (h + 1) * DK] + states_ref[r * 2 + h, :, DK:]
        return 0

    lax.fori_loop(0, blocks, step, 0)
    first_doc = jnp.broadcast_to(doc_at(0), (1, DK))
    last_doc = jnp.broadcast_to(doc_at(rows - 1), (1, DK))
    for h in range(2):
        own_t[h, :DV] = run_ref[h, :, :DK].astype(BF16)
        own_t[h, DV:] = run_ref[h, :, DK:].astype(BF16)
        own_e[h, 0:1] = total[:, h * DK : (h + 1) * DK]
        own_e[h, 1:2] = first_doc
        own_e[h, 2:3] = last_doc
        own_e[h, 3:8] = jnp.zeros((5, DK), F32)

    pl.semaphore_wait(barrier, NCHIP)
    swap_t = pltpu.make_async_remote_copy(
        own_t.at[1 - core], part_t, core_send.at[0], core_recv.at[0],
        device_id=partner, device_id_type=MESH)
    swap_e = pltpu.make_async_remote_copy(
        own_e.at[1 - core], part_e, core_send.at[1], core_recv.at[1],
        device_id=partner, device_id_type=MESH)
    swap_t.start()
    swap_e.start()
    swap_t.wait()
    swap_e.wait()
    is0 = core == 0
    mine_e = own_e[pl.ds(core, 1)][0]
    other_e = part_e[...]
    e0 = jnp.where(is0, mine_e, other_e)
    e1 = jnp.where(is0, other_e, mine_e)
    mine_t = own_t[pl.ds(core, 1)][0].astype(F32)
    other_t = part_t[...].astype(F32)
    t0 = jnp.where(is0, mine_t, other_t)
    t1 = jnp.where(is0, other_t, mine_t)
    through1 = jnp.exp(e1[0:1]) * jnp.where(e0[2:3] == e1[2:3], 1.0, 0.0)
    through0 = jnp.exp(e0[0:1]) * jnp.where(e1[1:2] == e0[1:2], 1.0, 0.0)
    chip_t[0] = (t1[:DV] + through1 * t0[:DV]).astype(BF16)
    chip_t[1] = (t0[DV:] + through0 * t1[DV:]).astype(BF16)
    chip_row = jnp.concatenate(
        [e0[0:1] + e1[0:1], e0[1:2], e1[2:3], jnp.zeros((5, DK), F32)], axis=0)
    chip_e[...] = chip_row
    recv_e[pl.ds(chip, 1)] = chip_row[None]

    sends = []
    for k in range(1, NCHIP):
        other, target = chip_peer(k)
        back = jnp.where(other > chip, 0, 1)
        sends.append(pltpu.make_async_remote_copy(
            chip_e, recv_e.at[chip], e_send.at[k], e_recv.at[k],
            device_id=target, device_id_type=MESH))
        sends.append(pltpu.make_async_remote_copy(
            chip_t.at[back], recv_t.at[chip], t_send.at[k], t_recv.at[k],
            device_id=target, device_id_type=MESH))
    for s in sends:
        s.start()

    def inside(g, _):
        at = pl.multiple_of(g * GR, GR)
        same_block = (ri & (GR - BL)) == (ci & (GR - BL))
        doc = aux_ref[pl.ds(at, GR), 2:3]
        same = same_block & (doc == docrow_ref[pl.ds(g, 1), :])
        below = same & (ci <= ri)
        above = same & (ci >= ri)
        cum3 = cum_ref[pl.ds(at, GR), :].reshape(per, BL, 2 * DK)
        middle = cum3[:, BL // 2 - 1 : BL // 2]
        ends = cum3[:, BL - 1 : BL]
        rising = jnp.exp(cum3 - middle)
        falling = jnp.exp(middle - cum3)
        qf = q_ref[pl.ds(at, GR), :].astype(F32).reshape(per, BL, 2 * DK) * scale
        kf = k_ref[pl.ds(at, GR), :].astype(F32).reshape(per, BL, 2 * DK)
        q_rise = (qf * rising).astype(BF16).reshape(GR, 2 * DK)
        q_fall = (qf * falling).astype(BF16).reshape(GR, 2 * DK)
        k_rise = (kf * rising).astype(BF16).reshape(GR, 2 * DK)
        k_fall = (kf * falling).astype(BF16).reshape(GR, 2 * DK)
        q_fwd = qf * jnp.exp(cum3)
        q_bwd = qf * jnp.exp(ends - cum3)
        for h in range(2):
            c = slice(h * DK, (h + 1) * DK)
            fw = nt_dot(q_rise[:, c], k_fall[:, c])
            bw = nt_dot(q_fall[:, c], k_rise[:, c])
            scores = jnp.where(below, fw, 0.0) + jnp.where(above, bw, 0.0)
            vals = v_ref[pl.ds(at, GR), h * DV : (h + 1) * DV]
            local_ref[pl.ds(at, GR), h * DV : (h + 1) * DV] = nn_dot(scores.astype(BF16), vals)
        for b in range(per):
            start = at + b * BL
            prev = doc_at(jnp.maximum(start - 1, 0))
            following = doc_at(jnp.minimum(start + BL, rows - 1))
            rows_doc = doc[b * BL : (b + 1) * BL]
            hit_f = jnp.where(rows_doc == prev, 1.0, 0.0)
            hit_b = jnp.where(rows_doc == following, 1.0, 0.0)
            for h in range(2):
                c = slice(h * DK, (h + 1) * DK)
                both = jnp.concatenate([q_fwd[b][:, c] * hit_f, q_bwd[b][:, c] * hit_b], axis=1)
                here = pl.ds(pl.multiple_of(start, BL), BL)
                local_ref[here, h * DV : (h + 1) * DV] += nt_dot(
                    both.astype(BF16), before_ref[(g * per + b) * 2 + h])
        return 0

    lax.fori_loop(0, groups, inside, 0)

    for s in sends:
        s.wait()
    run_ref[0] = jnp.zeros_like(run_ref[0])

    def earlier(j, _):
        e = recv_e[j]
        p = recv_e[jnp.maximum(j - 1, 0)]
        keep = jnp.exp(e[0:1]) * jnp.where(e[2:3] == p[2:3], 1.0, 0.0)
        run_ref[0, :, :DK] = recv_t[j].astype(F32) + run_ref[0, :, :DK] * keep
        return 0

    def later(i, _):
        j = NCHIP - 1 - i
        e = recv_e[j]
        p = recv_e[jnp.minimum(j + 1, NCHIP - 1)]
        keep = jnp.exp(e[0:1]) * jnp.where(e[1:2] == p[1:2], 1.0, 0.0)
        run_ref[0, :, DK:] = recv_t[j].astype(F32) + run_ref[0, :, DK:] * keep
        return 0

    lax.fori_loop(0, chip, earlier, 0)
    lax.fori_loop(0, NCHIP - 1 - chip, later, 0)
    cf, cb = run_ref[0, :, :DK], run_ref[0, :, DK:]
    before_doc = jnp.where(chip > 0, recv_e[jnp.maximum(chip - 1, 0)][2:3], -1.0)
    after_doc = jnp.where(
        chip < NCHIP - 1, recv_e[jnp.minimum(chip + 1, NCHIP - 1)][1:2], -1.0)
    pass0 = jnp.exp(e0[0:1]) * jnp.where(before_doc == e0[2:3], 1.0, 0.0)
    pass1 = jnp.exp(e1[0:1]) * jnp.where(after_doc == e1[1:2], 1.0, 0.0)
    mine_t = own_t[pl.ds(core, 1)][0].astype(F32)
    other_t = part_t[...].astype(F32)
    t0f = jnp.where(is0, mine_t[:DV], other_t[:DV])
    t1b = jnp.where(is0, other_t[DV:], mine_t[DV:])
    c0 = jnp.concatenate([cf, t1b + pass1 * cb], axis=1)
    c1 = jnp.concatenate([t0f + pass0 * cf, cb], axis=1)
    mine_c[...] = jnp.where(is0, c0, c1).astype(BF16)
    send_c[...] = jnp.where(is0, c1, c0).astype(BF16)
    swap_c = pltpu.make_async_remote_copy(
        send_c, part_c, core_send.at[2], core_recv.at[2],
        device_id=partner, device_id_type=MESH)
    swap_c.start()
    enter_f = jnp.where(is0, before_doc, e0[2:3])[:, 0:1]
    enter_b = jnp.where(is0, e1[1:2], after_doc)[:, 0:1]
    swap_c.wait()

    def last(g, _):
        at = pl.multiple_of(g * GR, GR)
        doc = aux_ref[pl.ds(at, GR), 2:3]
        hit_f = jnp.where(doc == enter_f, 1.0, 0.0)
        hit_b = jnp.where(doc == enter_b, 1.0, 0.0)
        glob = glob_ref[pl.ds(at, GR), :]
        qf = q_ref[pl.ds(at, GR), :].astype(F32) * scale
        q_fwd = (qf * jnp.exp(glob) * hit_f).astype(BF16)
        q_bwd = (qf * jnp.exp(sum_ref[...] - glob) * hit_b).astype(BF16)
        gain = gain_ref[...].astype(F32)
        for h in range(2):
            c = slice(h * DK, (h + 1) * DK)
            both = jnp.concatenate([q_fwd[:, c], q_bwd[:, c]], axis=1)
            carry = jnp.where(h == core, mine_c[...], part_c[...])
            out = local_ref[pl.ds(at, GR), h * DV : (h + 1) * DV] + nt_dot(both, carry)
            out = out * lax.rsqrt(jnp.mean(out * out, axis=-1, keepdims=True) + EPS) * gain
            u = gate_ref[pl.ds(at, GR), h * DV : (h + 1) * DV].astype(F32)
            mixed_ref[pl.ds(at, GR), h * DV : (h + 1) * DV] = (
                out * (u / (1.0 + jnp.exp(-u)))).astype(BF16)
        return 0

    lax.fori_loop(0, groups, last, 0)


def attention(q, k, v, lg, bias, extra, doc, gate, gain):
    rows = q.shape[0]
    doc_f = doc.astype(F32)
    aux = jnp.concatenate([extra, doc_f[:, None]], axis=1)
    docrow = doc_f.reshape(rows // GR, GR)
    vm = pl.BlockSpec(memory_space=pltpu.VMEM)
    blocks = rows // BL
    return pl.pallas_call(
        attention_kernel,
        out_shape=jax.ShapeDtypeStruct((rows, 2 * DV), BF16),
        in_specs=[vm] * 9,
        out_specs=vm,
        scratch_shapes=[
            pltpu.VMEM((rows, 2 * DK), F32),
            pltpu.VMEM((rows, 2 * DK), F32),
            pltpu.VMEM((blocks, 1, 2 * DK), F32),
            pltpu.VMEM((blocks * 2, DV, 2 * DK), F32),
            pltpu.VMEM((blocks * 2, DV, 2 * DK), BF16),
            pltpu.VMEM((2, DV, 2 * DK), F32),
            pltpu.VMEM((rows, 2 * DV), F32),
            pltpu.VMEM((2, 2 * DV, DK), BF16),
            pltpu.VMEM((2, 8, DK), F32),
            pltpu.VMEM((2 * DV, DK), BF16),
            pltpu.VMEM((8, DK), F32),
            pltpu.VMEM((2, DV, DK), BF16),
            pltpu.VMEM((8, DK), F32),
            pltpu.VMEM((NCHIP, DV, DK), BF16),
            pltpu.VMEM((NCHIP, 8, DK), F32),
            pltpu.VMEM((DV, 2 * DK), BF16),
            pltpu.VMEM((DV, 2 * DK), BF16),
            pltpu.VMEM((DV, 2 * DK), BF16),
            pltpu.VMEM((1, 2 * DK), F32),
            pltpu.SemaphoreType.DMA((3,)),
            pltpu.SemaphoreType.DMA((3,)),
            pltpu.SemaphoreType.DMA((NCHIP,)),
            pltpu.SemaphoreType.DMA((NCHIP,)),
            pltpu.SemaphoreType.DMA((NCHIP,)),
            pltpu.SemaphoreType.DMA((NCHIP,)),
        ],
        compiler_params=pltpu.CompilerParams(
            collective_id=0, has_side_effects=True, vmem_limit_bytes=48 * 2**20),
        cost_estimate=pl.CostEstimate(flops=3_000_000_000, bytes_accessed=8_000_000, transcendentals=0),
        name="attention",
    )(q, k, v, lg, bias.reshape(1, -1), aux, docrow, gate, gain.reshape(1, -1))


def ffn_kernel(
    mixed_ref, stream_ref, wo_ref, w_ref, gain_ref,
    out_ref,
    hm, st, wo_v, w_v, resid, keep, normed, hidden, s2, s1, s3, ra, rb, rl, rr,
    local_sem, own_rs, own_ls, fwd_rs, fwd_ls, left_in, right_in, opp_l, opp_r,
    rs_send, rs_recv,
):
    z, y, core = lax.axis_index("sp_0"), lax.axis_index("sp_1"), lax.axis_index("sp_2")
    me = lax.axis_index("tp")
    n = 4
    q_rows = GR
    half = q_rows // 2
    d = out_ref.shape[1]
    units = hidden.shape[1]
    ix_r, ix_l = lax.rem(me + 1, n), lax.rem(me + n - 1, n)
    right, left = (z, y, core, ix_r), (z, y, core, ix_l)

    own = pltpu.make_async_copy(mixed_ref, hm.at[me], local_sem.at[0])
    load_wo = pltpu.make_async_copy(wo_ref, wo_v, local_sem.at[1])
    load_st = pltpu.make_async_copy(stream_ref, st, local_sem.at[2])
    load_w = pltpu.make_async_copy(w_ref, w_v, local_sem.at[3])
    own.start()
    load_wo.start()
    load_st.start()
    load_w.start()
    barrier = pltpu.get_barrier_semaphore()
    pl.semaphore_signal(barrier, inc=1, device_id=right, device_id_type=MESH)
    pl.semaphore_signal(barrier, inc=1, device_id=left, device_id_type=MESH)
    pl.semaphore_wait(barrier, 2)
    own.wait()

    def piece(slot, r, part):
        return hm.at[slot, pl.ds(pl.multiple_of(r * q_rows + part * half, half), half)]

    def remote(ref, send, recv, target, dst=None):
        return pltpu.make_async_remote_copy(
            ref, ref if dst is None else dst, send, recv, device_id=target, device_id_type=MESH)

    def own_right(r, p):
        return remote(piece(me, r, p), own_rs.at[r * 2 + p], left_in.at[r * 2 + p], right)

    def own_left(r, p):
        return remote(piece(me, r, p), own_ls.at[r * 2 + p], right_in.at[r * 2 + p], left)

    def fwd_right(r):
        return remote(piece(ix_l, r, 0), fwd_rs.at[r], opp_l.at[r], right)

    def fwd_left(r):
        return remote(piece(ix_r, r, 1), fwd_ls.at[r], opp_r.at[r], left)

    def came_left(r, p):
        return remote(piece(ix_l, r, p), own_rs.at[r * 2 + p], left_in.at[r * 2 + p], right)

    def came_right(r, p):
        return remote(piece(ix_r, r, p), own_ls.at[r * 2 + p], right_in.at[r * 2 + p], left)

    opposite = lax.rem(me + 2, n)

    def came_opp_l(r):
        return remote(piece(opposite, r, 0), fwd_rs.at[r], opp_l.at[r], right)

    def came_opp_r(r):
        return remote(piece(opposite, r, 1), fwd_ls.at[r], opp_r.at[r], left)

    def send_own(r):
        own_right(r, 0).start()
        own_left(r, 1).start()
        own_right(r, 1).start()
        own_left(r, 0).start()

    def pump(r):
        came_left(r, 0).wait_recv()
        fwd_right(r).start()
        came_right(r, 1).wait_recv()
        fwd_left(r).start()

    send_own(0)
    pump(0)
    send_own(1)
    load_wo.wait()
    load_st.wait()

    dh = d // 2
    to_r_a = remote(s2.at[:, pl.ds(0, dh)], rs_send.at[0], rs_recv.at[0], right, ra)
    to_l_b = remote(s2.at[:, pl.ds(dh, dh)], rs_send.at[1], rs_recv.at[1], left, rb)
    to_r = remote(s1, rs_send.at[2], rs_recv.at[2], right, rl)
    to_l = remote(s3, rs_send.at[3], rs_recv.at[3], left, rr)

    def pass_on(role):
        @pl.when(role == 1)
        def _():
            to_r_a.wait_recv()
            s1[:, :dh] = (s1[:, :dh].astype(F32) + ra[...].astype(F32)).astype(BF16)
            to_r.start()

        @pl.when(role == 3)
        def _():
            to_l_b.wait_recv()
            s3[:, dh:] = (s3[:, dh:].astype(F32) + rb[...].astype(F32)).astype(BF16)
            to_l.start()

    def quarter(q, _):
        role = lax.rem(q - me + n, n)
        at = pl.multiple_of(q * q_rows, q_rows)
        rows = pl.ds(at, q_rows)
        came_left(q, 1).wait_recv()
        came_right(q, 0).wait_recv()
        came_opp_l(q).wait_recv()
        came_opp_r(q).wait_recv()

        def project(j, total):
            cols = pl.ds(pl.multiple_of(j * 512, 512), 512)
            acc = st[rows, cols].astype(F32)
            for k in range(n):
                acc = acc + nn_dot(hm[k, rows, :], wo_v[k * 512 : (k + 1) * 512, cols])
            resid[:, cols] = acc
            return total + jnp.sum(acc * acc, axis=-1, keepdims=True)

        squares = lax.fori_loop(0, d // 512, project, jnp.zeros((q_rows, 1), F32))

        @pl.when(q < n - 1)
        def _():
            pump(q + 1)

        @pl.when(q < n - 2)
        def _():
            send_own(q + 2)

        @pl.when(q == 0)
        def _():
            load_w.wait()

        factor = lax.rsqrt(squares / d + EPS)
        normed[...] = (resid[...] * factor * gain_ref[...].astype(F32)).astype(BF16)

        @pl.when(role == 0)
        def _():
            keep[...] = resid[...]

        def gate_up(j, _):
            both = nn_dot(normed[...], w_v[:, pl.ds(pl.multiple_of(j * 256, 256), 256)])
            g, u = both[:, :128], both[:, 128:]
            hidden[:, pl.ds(pl.multiple_of(j * 128, 128), 128)] = (
                g / (1.0 + jnp.exp(-g)) * u).astype(BF16)
            return 0

        lax.fori_loop(0, units // 128, gate_up, 0)

        @pl.when(q > 0)
        def _():
            pass_on(lax.rem(q - 1 - me + n, n))

        def down(j, _):
            at_col = pl.multiple_of(j * 256, 256)
            cols = pl.ds(at_col, 256)
            part = nt_dot(hidden[...], w_v[cols, 2 * units : 3 * units]).astype(BF16)

            @pl.when(role == 0)
            def _():
                keep[:, cols] = keep[:, cols] + part.astype(F32)

            @pl.when(role == 1)
            def _():
                s1[:, cols] = part

            @pl.when(role == 2)
            def _():
                s2[:, cols] = part

            @pl.when(role == 3)
            def _():
                s3[:, cols] = part

            return 0

        lax.fori_loop(0, d // 256, down, 0)

        @pl.when(role == 2)
        def _():
            to_r_a.start()
            to_l_b.start()

        return 0

    lax.fori_loop(0, n, quarter, 0)
    pass_on(lax.rem(n - 1 - me + n, n))
    to_r.wait_recv()
    to_l.wait_recv()
    out_ref[...] = (keep[...] + rl[...].astype(F32) + rr[...].astype(F32)).astype(BF16)

    for r in range(n):
        for p in range(2):
            own_right(r, p).wait_send()
            own_left(r, p).wait_send()
        fwd_right(r).wait_send()
        fwd_left(r).wait_send()
    to_r_a.wait_send()
    to_l_b.wait_send()
    to_r.wait_send()
    to_l.wait_send()


def feed_forward(mixed, stream, wo, w, gain):
    rows, d = stream.shape
    units = w.shape[1] // 3
    vm = pl.BlockSpec(memory_space=pltpu.VMEM)
    hbm = pl.BlockSpec(memory_space=pl.ANY)
    dma = pltpu.SemaphoreType.DMA
    return pl.pallas_call(
        ffn_kernel,
        out_shape=jax.ShapeDtypeStruct((GR, d), BF16),
        in_specs=[hbm, hbm, hbm, hbm, vm],
        out_specs=vm,
        scratch_shapes=[
            pltpu.VMEM((4, rows, mixed.shape[1]), BF16),
            pltpu.VMEM((rows, d), BF16),
            pltpu.VMEM(wo.shape, BF16),
            pltpu.VMEM(w.shape, BF16),
            pltpu.VMEM((GR, d), F32),
            pltpu.VMEM((GR, d), F32),
            pltpu.VMEM((GR, d), BF16),
            pltpu.VMEM((GR, units), BF16),
            pltpu.VMEM((GR, d), BF16),
            pltpu.VMEM((GR, d), BF16),
            pltpu.VMEM((GR, d), BF16),
            pltpu.VMEM((GR, d // 2), BF16),
            pltpu.VMEM((GR, d // 2), BF16),
            pltpu.VMEM((GR, d), BF16),
            pltpu.VMEM((GR, d), BF16),
            dma((4,)), dma((8,)), dma((8,)), dma((4,)), dma((4,)),
            dma((8,)), dma((8,)), dma((4,)), dma((4,)), dma((4,)), dma((4,)),
        ],
        compiler_params=pltpu.CompilerParams(
            collective_id=1, has_side_effects=True, vmem_limit_bytes=60 * 2**20),
        cost_estimate=pl.CostEstimate(
            flops=26_000_000_000, bytes_accessed=32_000_000, transcendentals=0),
        name="feed_forward",
    )(mixed, stream, wo, w, gain.reshape(1, -1))


def per_device(
    stream, queries, projected_keys, values, decay_gate_logits, decay_gate_bias, extra_log_decay,
    document_index, output_gate, head_norm_gain, output_weight, feedforward_norm_gain,
    gate_weight, up_weight, down_weight,
):
    own_rows, units = gate_weight.shape
    pair = jnp.stack(
        [gate_weight.reshape(own_rows, -1, 128), up_weight.reshape(own_rows, -1, 128)], axis=2)
    shard = jnp.concatenate([pair.reshape(own_rows, 2 * units), down_weight.T], axis=1)
    weights = lax.all_gather(shard, SP, axis=0, tiled=True)
    whole_out = lax.all_gather(output_weight, "tp", axis=0, tiled=True)
    head_mixed = attention(
        queries, projected_keys, values, decay_gate_logits, decay_gate_bias, extra_log_decay,
        document_index, output_gate, head_norm_gain)
    return feed_forward(head_mixed, stream, whole_out, weights, feedforward_norm_gain)


def solution(mesh):
    torus = Mesh(mesh.devices.reshape(4, 4, 2, mesh.shape["tp"]), ("sp_0", "sp_1", "sp_2", "tp"))
    placed = (
        P(SP, None), P(SP, "tp"), P(SP, "tp"), P(SP, "tp"), P(SP, "tp"), P("tp"), P(SP, "tp"),
        P(SP), P(SP, "tp"), P(), P("tp", None), P(), P(SP, "tp"), P(SP, "tp"), P("tp", SP),
    )
    return jax.shard_map(
        per_device, mesh=torus, in_specs=placed, out_specs=P(SP_TP, None), check_vma=False
    )
```

```python
import functools
import jax
import jax.numpy as jnp
from jax import lax
from jax.experimental import pallas as pl
from jax.experimental.pallas import tpu as pltpu
from jax.sharding import Mesh
from jax.sharding import PartitionSpec as P

SP = ("sp_0", "sp_1", "sp_2")
SP_TP = ("sp_0", "sp_1", "sp_2", "tp")
MESH = pl.DeviceIdType.MESH
F32 = jnp.float32
BF16 = jnp.bfloat16
TAU = 16.0
EPS = 1e-06
BL = 64
GR = 256
DK = 128
DV = 256
NZ, NY = 4, 4
NCHIP = NZ * NY


def nt_dot(a, b):
    return lax.dot_general(a, b, (((1,), (1,)), ((), ())), preferred_element_type=F32)


def tn_dot(a, b):
    return lax.dot_general(a, b, (((0,), (0,)), ((), ())), preferred_element_type=F32)


def nn_dot(a, b):
    return lax.dot_general(a, b, (((1,), (0,)), ((), ())), preferred_element_type=F32)


def attention_kernel(
    q_ref, k_ref, v_ref, lg_ref, bias_ref, aux_ref, docrow_ref, gate_ref, gain_ref,
    mixed_ref,
    cum_ref, glob_ref, blk_ref, states_ref, before_ref, run_ref, local_ref,
    own_t, own_e, part_t, part_e, chip_t, chip_e, recv_t, recv_e, mine_c, send_c, part_c, sum_ref,
    core_send, core_recv, t_send, t_recv, e_send, e_recv,
):
    rows = q_ref.shape[0]
    blocks = rows // BL
    groups = rows // GR
    per = GR // BL
    z, y = lax.axis_index("sp_0"), lax.axis_index("sp_1")
    core, x = lax.axis_index("sp_2"), lax.axis_index("tp")
    chip = z * NY + y
    scale = DK ** (-0.5)

    def chip_peer(k):
        other = lax.rem(chip + k, NCHIP)
        return other, (other // NY, lax.rem(other, NY), core, x)

    partner = (z, y, 1 - core, x)

    recv_t[pl.ds(chip, 1)] = jnp.zeros((1, DV, DK), BF16)

    barrier = pltpu.get_barrier_semaphore()
    pl.semaphore_signal(barrier, inc=1, device_id=partner, device_id_type=MESH)
    for k in range(1, NCHIP):
        pl.semaphore_signal(barrier, inc=1, device_id=chip_peer(k)[1], device_id_type=MESH)

    ri = lax.broadcasted_iota(jnp.int32, (GR, GR), 0)
    ci = lax.broadcasted_iota(jnp.int32, (GR, GR), 1)

    def first(g, base):
        at = pl.multiple_of(g * GR, GR)
        same_block = (ri & (GR - BL)) == (ci & (GR - BL))
        tri = jnp.where(same_block & (ci <= ri), 1.0, 0.0).astype(BF16)
        logits = lg_ref[pl.ds(at, GR), :].astype(F32) + bias_ref[...]
        ld = (jnp.minimum(logits, 0.0) - jnp.log1p(jnp.exp(-jnp.abs(logits)))) / TAU
        extra0 = jnp.broadcast_to(aux_ref[pl.ds(at, GR), 0:1], (GR, DK))
        extra1 = jnp.broadcast_to(aux_ref[pl.ds(at, GR), 1:2], (GR, DK))
        ld = ld + jnp.concatenate([extra0, extra1], axis=1)
        hi = ld.astype(BF16)
        rest = ld - hi.astype(F32)
        mid = rest.astype(BF16)
        low = (rest - mid.astype(F32)).astype(BF16)
        cum = nn_dot(tri, hi) + nn_dot(tri, mid) + nn_dot(tri, low)
        cum_ref[pl.ds(at, GR), :] = cum
        cum3 = cum.reshape(per, BL, 2 * DK)
        ends = cum3[:, BL - 1 : BL, :]
        off, offs = base, []
        for b in range(per):
            offs.append(off)
            blk_ref[pl.ds(g * per + b, 1)] = ends[b : b + 1]
            off = off + ends[b]
        for b in range(per):
            glob_ref[pl.ds(pl.multiple_of(at + b * BL, BL), BL), :] = cum3[b] + offs[b]
        doc = aux_ref[pl.ds(at, GR), 2:3].reshape(per, BL, 1)
        tail_mask = jnp.where(doc == doc[:, BL - 1 : BL], 1.0, 0.0)
        head_mask = jnp.where(doc == doc[:, 0:1], 1.0, 0.0)
        kf = k_ref[pl.ds(at, GR), :].astype(F32).reshape(per, BL, 2 * DK)
        tail = (kf * jnp.exp(ends - cum3) * tail_mask).astype(BF16)
        head = (kf * jnp.exp(cum3) * head_mask).astype(BF16)
        for b in range(per):
            for h in range(2):
                keys = jnp.concatenate(
                    [tail[b][:, h * DK : (h + 1) * DK], head[b][:, h * DK : (h + 1) * DK]], axis=1
                )
                vals = v_ref[pl.ds(pl.multiple_of(at + b * BL, BL), BL), h * DV : (h + 1) * DV]
                states_ref[pl.ds((g * per + b) * 2 + h, 1)] = tn_dot(vals, keys)[None]
        return off

    total = lax.fori_loop(0, groups, first, jnp.zeros((1, 2 * DK), F32))
    sum_ref[...] = total

    run_ref[...] = jnp.zeros_like(run_ref)

    def doc_at(r):
        return aux_ref[pl.ds(r, 1), 2:3]

    def step(b, _):
        lo = jnp.maximum(b * BL - 1, 0)
        keep = jnp.where(doc_at(lo) == doc_at(b * BL + BL - 1), 1.0, 0.0)
        decay = jnp.exp(blk_ref[pl.ds(b, 1)][0]) * keep
        r = blocks - 1 - b
        hi = jnp.minimum(r * BL + BL, rows - 1)
        keep_b = jnp.where(doc_at(hi) == doc_at(r * BL), 1.0, 0.0)
        decay_b = jnp.exp(blk_ref[pl.ds(r, 1)][0]) * keep_b
        for h in range(2):
            fw = run_ref[h, :, :DK]
            before_ref[pl.ds(b * 2 + h, 1), :, :DK] = fw.astype(BF16)[None]
            run_ref[h, :, :DK] = fw * decay[:, h * DK : (h + 1) * DK] + states_ref[b * 2 + h, :, :DK]
            bw = run_ref[h, :, DK:]
            before_ref[pl.ds(r * 2 + h, 1), :, DK:] = bw.astype(BF16)[None]
            run_ref[h, :, DK:] = bw * decay_b[:, h * DK : (h + 1) * DK] + states_ref[r * 2 + h, :, DK:]
        return 0

    lax.fori_loop(0, blocks, step, 0)
    first_doc = jnp.broadcast_to(doc_at(0), (1, DK))
    last_doc = jnp.broadcast_to(doc_at(rows - 1), (1, DK))
    for h in range(2):
        own_t[h, :DV] = run_ref[h, :, :DK].astype(BF16)
        own_t[h, DV:] = run_ref[h, :, DK:].astype(BF16)
        own_e[h, 0:1] = total[:, h * DK : (h + 1) * DK]
        own_e[h, 1:2] = first_doc
        own_e[h, 2:3] = last_doc
        own_e[h, 3:8] = jnp.zeros((5, DK), F32)

    pl.semaphore_wait(barrier, NCHIP)
    swap_t = pltpu.make_async_remote_copy(
        own_t.at[1 - core], part_t, core_send.at[0], core_recv.at[0],
        device_id=partner, device_id_type=MESH)
    swap_e = pltpu.make_async_remote_copy(
        own_e.at[1 - core], part_e, core_send.at[1], core_recv.at[1],
        device_id=partner, device_id_type=MESH)
    swap_t.start()
    swap_e.start()
    swap_t.wait()
    swap_e.wait()
    is0 = core == 0
    mine_e = own_e[pl.ds(core, 1)][0]
    other_e = part_e[...]
    e0 = jnp.where(is0, mine_e, other_e)
    e1 = jnp.where(is0, other_e, mine_e)
    mine_t = own_t[pl.ds(core, 1)][0].astype(F32)
    other_t = part_t[...].astype(F32)
    t0 = jnp.where(is0, mine_t, other_t)
    t1 = jnp.where(is0, other_t, mine_t)
    through1 = jnp.exp(e1[0:1]) * jnp.where(e0[2:3] == e1[2:3], 1.0, 0.0)
    through0 = jnp.exp(e0[0:1]) * jnp.where(e1[1:2] == e0[1:2], 1.0, 0.0)
    chip_t[0] = (t1[:DV] + through1 * t0[:DV]).astype(BF16)
    chip_t[1] = (t0[DV:] + through0 * t1[DV:]).astype(BF16)
    chip_row = jnp.concatenate(
        [e0[0:1] + e1[0:1], e0[1:2], e1[2:3], jnp.zeros((5, DK), F32)], axis=0)
    chip_e[...] = chip_row
    recv_e[pl.ds(chip, 1)] = chip_row[None]

    sends = []
    for k in range(1, NCHIP):
        other, target = chip_peer(k)
        back = jnp.where(other > chip, 0, 1)
        sends.append(pltpu.make_async_remote_copy(
            chip_e, recv_e.at[chip], e_send.at[k], e_recv.at[k],
            device_id=target, device_id_type=MESH))
        sends.append(pltpu.make_async_remote_copy(
            chip_t.at[back], recv_t.at[chip], t_send.at[k], t_recv.at[k],
            device_id=target, device_id_type=MESH))
    for s in sends:
        s.start()

    def inside(g, _):
        at = pl.multiple_of(g * GR, GR)
        same_block = (ri & (GR - BL)) == (ci & (GR - BL))
        doc = aux_ref[pl.ds(at, GR), 2:3]
        same = same_block & (doc == docrow_ref[pl.ds(g, 1), :])
        below = same & (ci <= ri)
        above = same & (ci >= ri)
        cum3 = cum_ref[pl.ds(at, GR), :].reshape(per, BL, 2 * DK)
        middle = cum3[:, BL // 2 - 1 : BL // 2]
        ends = cum3[:, BL - 1 : BL]
        rising = jnp.exp(cum3 - middle)
        falling = jnp.exp(middle - cum3)
        qf = q_ref[pl.ds(at, GR), :].astype(F32).reshape(per, BL, 2 * DK) * scale
        kf = k_ref[pl.ds(at, GR), :].astype(F32).reshape(per, BL, 2 * DK)
        q_rise = (qf * rising).astype(BF16).reshape(GR, 2 * DK)
        q_fall = (qf * falling).astype(BF16).reshape(GR, 2 * DK)
        k_rise = (kf * rising).astype(BF16).reshape(GR, 2 * DK)
        k_fall = (kf * falling).astype(BF16).reshape(GR, 2 * DK)
        q_fwd = qf * jnp.exp(cum3)
        q_bwd = qf * jnp.exp(ends - cum3)
        for h in range(2):
            c = slice(h * DK, (h + 1) * DK)
            fw = nt_dot(q_rise[:, c], k_fall[:, c])
            bw = nt_dot(q_fall[:, c], k_rise[:, c])
            scores = jnp.where(below, fw, 0.0) + jnp.where(above, bw, 0.0)
            vals = v_ref[pl.ds(at, GR), h * DV : (h + 1) * DV]
            local_ref[pl.ds(at, GR), h * DV : (h + 1) * DV] = nn_dot(scores.astype(BF16), vals)
        for b in range(per):
            start = at + b * BL
            prev = doc_at(jnp.maximum(start - 1, 0))
            following = doc_at(jnp.minimum(start + BL, rows - 1))
            rows_doc = doc[b * BL : (b + 1) * BL]
            hit_f = jnp.where(rows_doc == prev, 1.0, 0.0)
            hit_b = jnp.where(rows_doc == following, 1.0, 0.0)
            for h in range(2):
                c = slice(h * DK, (h + 1) * DK)
                both = jnp.concatenate([q_fwd[b][:, c] * hit_f, q_bwd[b][:, c] * hit_b], axis=1)
                here = pl.ds(pl.multiple_of(start, BL), BL)
                local_ref[here, h * DV : (h + 1) * DV] += nt_dot(
                    both.astype(BF16), before_ref[(g * per + b) * 2 + h])
        return 0

    lax.fori_loop(0, groups, inside, 0)

    for s in sends:
        s.wait()
    run_ref[0] = jnp.zeros_like(run_ref[0])

    def earlier(j, _):
        e = recv_e[j]
        p = recv_e[jnp.maximum(j - 1, 0)]
        keep = jnp.exp(e[0:1]) * jnp.where(e[2:3] == p[2:3], 1.0, 0.0)
        run_ref[0, :, :DK] = recv_t[j].astype(F32) + run_ref[0, :, :DK] * keep
        return 0

    def later(i, _):
        j = NCHIP - 1 - i
        e = recv_e[j]
        p = recv_e[jnp.minimum(j + 1, NCHIP - 1)]
        keep = jnp.exp(e[0:1]) * jnp.where(e[1:2] == p[1:2], 1.0, 0.0)
        run_ref[0, :, DK:] = recv_t[j].astype(F32) + run_ref[0, :, DK:] * keep
        return 0

    lax.fori_loop(0, chip, earlier, 0)
    lax.fori_loop(0, NCHIP - 1 - chip, later, 0)
    cf, cb = run_ref[0, :, :DK], run_ref[0, :, DK:]
    before_doc = jnp.where(chip > 0, recv_e[jnp.maximum(chip - 1, 0)][2:3], -1.0)
    after_doc = jnp.where(
        chip < NCHIP - 1, recv_e[jnp.minimum(chip + 1, NCHIP - 1)][1:2], -1.0)
    pass0 = jnp.exp(e0[0:1]) * jnp.where(before_doc == e0[2:3], 1.0, 0.0)
    pass1 = jnp.exp(e1[0:1]) * jnp.where(after_doc == e1[1:2], 1.0, 0.0)
    mine_t = own_t[pl.ds(core, 1)][0].astype(F32)
    other_t = part_t[...].astype(F32)
    t0f = jnp.where(is0, mine_t[:DV], other_t[:DV])
    t1b = jnp.where(is0, other_t[DV:], mine_t[DV:])
    c0 = jnp.concatenate([cf, t1b + pass1 * cb], axis=1)
    c1 = jnp.concatenate([t0f + pass0 * cf, cb], axis=1)
    mine_c[...] = jnp.where(is0, c0, c1).astype(BF16)
    send_c[...] = jnp.where(is0, c1, c0).astype(BF16)
    swap_c = pltpu.make_async_remote_copy(
        send_c, part_c, core_send.at[2], core_recv.at[2],
        device_id=partner, device_id_type=MESH)
    swap_c.start()
    enter_f = jnp.where(is0, before_doc, e0[2:3])[:, 0:1]
    enter_b = jnp.where(is0, e1[1:2], after_doc)[:, 0:1]
    swap_c.wait()

    def last(g, _):
        at = pl.multiple_of(g * GR, GR)
        doc = aux_ref[pl.ds(at, GR), 2:3]
        hit_f = jnp.where(doc == enter_f, 1.0, 0.0)
        hit_b = jnp.where(doc == enter_b, 1.0, 0.0)
        glob = glob_ref[pl.ds(at, GR), :]
        qf = q_ref[pl.ds(at, GR), :].astype(F32) * scale
        q_fwd = (qf * jnp.exp(glob) * hit_f).astype(BF16)
        q_bwd = (qf * jnp.exp(sum_ref[...] - glob) * hit_b).astype(BF16)
        gain = gain_ref[...].astype(F32)
        for h in range(2):
            c = slice(h * DK, (h + 1) * DK)
            both = jnp.concatenate([q_fwd[:, c], q_bwd[:, c]], axis=1)
            carry = jnp.where(h == core, mine_c[...], part_c[...])
            out = local_ref[pl.ds(at, GR), h * DV : (h + 1) * DV] + nt_dot(both, carry)
            out = out * lax.rsqrt(jnp.mean(out * out, axis=-1, keepdims=True) + EPS) * gain
            u = gate_ref[pl.ds(at, GR), h * DV : (h + 1) * DV].astype(F32)
            mixed_ref[pl.ds(at, GR), h * DV : (h + 1) * DV] = (
                out * (u / (1.0 + jnp.exp(-u)))).astype(BF16)
        return 0

    lax.fori_loop(0, groups, last, 0)


def attention(q, k, v, lg, bias, extra, doc, gate, gain):
    rows = q.shape[0]
    doc_f = doc.astype(F32)
    aux = jnp.concatenate([extra, doc_f[:, None]], axis=1)
    docrow = doc_f.reshape(rows // GR, GR)
    vm = pl.BlockSpec(memory_space=pltpu.VMEM)
    blocks = rows // BL
    return pl.pallas_call(
        attention_kernel,
        out_shape=jax.ShapeDtypeStruct((rows, 2 * DV), BF16),
        in_specs=[vm] * 9,
        out_specs=vm,
        scratch_shapes=[
            pltpu.VMEM((rows, 2 * DK), F32),
            pltpu.VMEM((rows, 2 * DK), F32),
            pltpu.VMEM((blocks, 1, 2 * DK), F32),
            pltpu.VMEM((blocks * 2, DV, 2 * DK), F32),
            pltpu.VMEM((blocks * 2, DV, 2 * DK), BF16),
            pltpu.VMEM((2, DV, 2 * DK), F32),
            pltpu.VMEM((rows, 2 * DV), F32),
            pltpu.VMEM((2, 2 * DV, DK), BF16),
            pltpu.VMEM((2, 8, DK), F32),
            pltpu.VMEM((2 * DV, DK), BF16),
            pltpu.VMEM((8, DK), F32),
            pltpu.VMEM((2, DV, DK), BF16),
            pltpu.VMEM((8, DK), F32),
            pltpu.VMEM((NCHIP, DV, DK), BF16),
            pltpu.VMEM((NCHIP, 8, DK), F32),
            pltpu.VMEM((DV, 2 * DK), BF16),
            pltpu.VMEM((DV, 2 * DK), BF16),
            pltpu.VMEM((DV, 2 * DK), BF16),
            pltpu.VMEM((1, 2 * DK), F32),
            pltpu.SemaphoreType.DMA((3,)),
            pltpu.SemaphoreType.DMA((3,)),
            pltpu.SemaphoreType.DMA((NCHIP,)),
            pltpu.SemaphoreType.DMA((NCHIP,)),
            pltpu.SemaphoreType.DMA((NCHIP,)),
            pltpu.SemaphoreType.DMA((NCHIP,)),
        ],
        compiler_params=pltpu.CompilerParams(
            collective_id=0, has_side_effects=True, vmem_limit_bytes=48 * 2**20),
        cost_estimate=pl.CostEstimate(flops=3_000_000_000, bytes_accessed=8_000_000, transcendentals=0),
        name="attention",
    )(q, k, v, lg, bias.reshape(1, -1), aux, docrow, gate, gain.reshape(1, -1))


def ffn_kernel(
    mixed_ref, stream_ref, wo_ref, w_ref, gain_ref,
    out_ref,
    hm, st, wo_v, w_v, resid, normed, hidden, s2, s1, s3, ra, rb, rl, rr,
    local_sem, own_rs, own_ls, fwd_rs, fwd_ls, left_in, right_in, opp_l, opp_r,
    rs_send, rs_recv,
):
    z, y, core = lax.axis_index("sp_0"), lax.axis_index("sp_1"), lax.axis_index("sp_2")
    me = lax.axis_index("tp")
    n = 4
    q_rows = GR
    half = q_rows // 2
    d = out_ref.shape[1]
    units = hidden.shape[1]
    ix_r, ix_l = lax.rem(me + 1, n), lax.rem(me + n - 1, n)
    right, left = (z, y, core, ix_r), (z, y, core, ix_l)

    own = pltpu.make_async_copy(mixed_ref, hm.at[me], local_sem.at[0])
    load_wo = pltpu.make_async_copy(wo_ref, wo_v, local_sem.at[1])
    load_st = pltpu.make_async_copy(stream_ref, st, local_sem.at[2])
    load_w = pltpu.make_async_copy(w_ref, w_v, local_sem.at[3])
    own.start()
    load_wo.start()
    load_st.start()
    load_w.start()
    barrier = pltpu.get_barrier_semaphore()
    pl.semaphore_signal(barrier, inc=1, device_id=right, device_id_type=MESH)
    pl.semaphore_signal(barrier, inc=1, device_id=left, device_id_type=MESH)
    pl.semaphore_wait(barrier, 2)
    own.wait()

    def piece(slot, r, part):
        return hm.at[slot, pl.ds(pl.multiple_of(r * q_rows + part * half, half), half)]

    def remote(ref, send, recv, target, dst=None):
        return pltpu.make_async_remote_copy(
            ref, ref if dst is None else dst, send, recv, device_id=target, device_id_type=MESH)

    order = (2, 1, 3, 0)

    def quarter_of(owner, offset):
        return lax.rem(owner + offset, n)

    def wire(slot, quarter, part, send, recv, target):
        return remote(piece(slot, quarter, part), send, recv, target)

    to_right = (((3, 0), (3, 1), (0, 0)), ((2, 0), (2, 1)), ((0, 1), (1, 0)), ((1, 1),))
    to_left = (((1, 1), (1, 0), (0, 1)), ((0, 0), (3, 1)), ((2, 1), (2, 0)), ((3, 0),))

    def own_right(o, p):
        return wire(me, quarter_of(me, o), p, own_rs.at[o * 2 + p], left_in.at[o * 2 + p], right)

    def own_left(o, p):
        return wire(me, quarter_of(me, o), p, own_ls.at[o * 2 + p], right_in.at[o * 2 + p], left)

    def came_left(o, p):
        return wire(ix_l, quarter_of(ix_l, o), p, own_rs.at[o * 2 + p], left_in.at[o * 2 + p], right)

    def came_right(o, p):
        return wire(ix_r, quarter_of(ix_r, o), p, own_ls.at[o * 2 + p], right_in.at[o * 2 + p], left)

    def fwd_right(i):
        return wire(ix_l, quarter_of(ix_r, order[i]), 0, fwd_rs.at[i], opp_l.at[i], right)

    def fwd_left(i):
        return wire(ix_r, quarter_of(ix_l, order[i]), 1, fwd_ls.at[i], opp_r.at[i], left)

    opposite = lax.rem(me + 2, n)

    def came_opp_l(i):
        return wire(opposite, quarter_of(me, order[i]), 0, fwd_rs.at[i], opp_l.at[i], right)

    def came_opp_r(i):
        return wire(opposite, quarter_of(me, order[i]), 1, fwd_ls.at[i], opp_r.at[i], left)

    def send_own(i):
        for k in range(len(to_right[i])):
            own_right(*to_right[i][k]).start()
            own_left(*to_left[i][k]).start()

    seen = set()

    def arrived(side, o, p):
        if (side, o, p) not in seen:
            seen.add((side, o, p))
            (came_left if side == "l" else came_right)(o, p).wait_recv()

    def pump(i):
        arrived("l", (2 + order[i]) % n, 0)
        fwd_right(i).start()
        arrived("r", (n - 2 + order[i]) % n, 1)
        fwd_left(i).start()

    send_own(0)
    pump(0)
    send_own(1)
    load_wo.wait()
    load_st.wait()

    dh = d // 2
    to_r_a = remote(s2.at[:, pl.ds(0, dh)], rs_send.at[0], rs_recv.at[0], right, ra)
    to_l_b = remote(s2.at[:, pl.ds(dh, dh)], rs_send.at[1], rs_recv.at[1], left, rb)
    to_r = remote(s1, rs_send.at[2], rs_recv.at[2], right, rl)
    to_l = remote(s3, rs_send.at[3], rs_recv.at[3], left, rr)

    for i in range(n):
        q = quarter_of(me, order[i])
        at = pl.multiple_of(q * q_rows, q_rows)
        rows = pl.ds(at, q_rows)
        for p in range(2):
            arrived("l", (1 + order[i]) % n, p)
            arrived("r", (n - 1 + order[i]) % n, p)
        came_opp_l(i).wait_recv()
        came_opp_r(i).wait_recv()

        def project(j, total):
            cols = pl.ds(pl.multiple_of(j * 512, 512), 512)
            acc = st[rows, cols].astype(F32)
            for k in range(n):
                acc = acc + nn_dot(hm[k, rows, :], wo_v[k * 512 : (k + 1) * 512, cols])
            resid[:, cols] = acc
            return total + jnp.sum(acc * acc, axis=-1, keepdims=True)

        squares = lax.fori_loop(0, d // 512, project, jnp.zeros((q_rows, 1), F32))
        if i < n - 1:
            pump(i + 1)
        if i < n - 2:
            send_own(i + 2)
        if i == 0:
            load_w.wait()
        factor = lax.rsqrt(squares / d + EPS)
        normed[...] = (resid[...] * factor * gain_ref[...].astype(F32)).astype(BF16)

        def gate_up(j, _):
            both = nn_dot(normed[...], w_v[:, pl.ds(pl.multiple_of(j * 256, 256), 256)])
            g, u = both[:, :128], both[:, 128:]
            hidden[:, pl.ds(pl.multiple_of(j * 128, 128), 128)] = (
                g / (1.0 + jnp.exp(-g)) * u).astype(BF16)
            return 0

        lax.fori_loop(0, units // 128, gate_up, 0)
        target = (s2, s1, s3, resid)[i]

        def down(j, _):
            cols = pl.ds(pl.multiple_of(j * 256, 256), 256)
            part = nt_dot(hidden[...], w_v[cols, 2 * units : 3 * units]).astype(BF16)
            if i < n - 1:
                target[:, cols] = part
            else:
                target[:, cols] = target[:, cols] + part.astype(F32)
            return 0

        lax.fori_loop(0, d // 256, down, 0)
        if i == 0:
            to_r_a.start()
            to_l_b.start()
        if i == 2:
            to_r_a.wait_recv()
            s1[:, :dh] = (s1[:, :dh].astype(F32) + ra[...].astype(F32)).astype(BF16)
            to_r.start()
            to_l_b.wait_recv()
            s3[:, dh:] = (s3[:, dh:].astype(F32) + rb[...].astype(F32)).astype(BF16)
            to_l.start()

    to_r.wait_recv()
    to_l.wait_recv()
    out_ref[...] = (resid[...] + rl[...].astype(F32) + rr[...].astype(F32)).astype(BF16)

    for o in range(n):
        for p in range(2):
            own_right(o, p).wait_send()
            own_left(o, p).wait_send()
    for i in range(n):
        fwd_right(i).wait_send()
        fwd_left(i).wait_send()
    to_r_a.wait_send()
    to_l_b.wait_send()
    to_r.wait_send()
    to_l.wait_send()


def feed_forward(mixed, stream, wo, w, gain):
    rows, d = stream.shape
    units = w.shape[1] // 3
    vm = pl.BlockSpec(memory_space=pltpu.VMEM)
    hbm = pl.BlockSpec(memory_space=pl.ANY)
    dma = pltpu.SemaphoreType.DMA
    return pl.pallas_call(
        ffn_kernel,
        out_shape=jax.ShapeDtypeStruct((GR, d), BF16),
        in_specs=[hbm, hbm, hbm, hbm, vm],
        out_specs=vm,
        scratch_shapes=[
            pltpu.VMEM((4, rows, mixed.shape[1]), BF16),
            pltpu.VMEM((rows, d), BF16),
            pltpu.VMEM(wo.shape, BF16),
            pltpu.VMEM(w.shape, BF16),
            pltpu.VMEM((GR, d), F32),
            pltpu.VMEM((GR, d), BF16),
            pltpu.VMEM((GR, units), BF16),
            pltpu.VMEM((GR, d), BF16),
            pltpu.VMEM((GR, d), BF16),
            pltpu.VMEM((GR, d), BF16),
            pltpu.VMEM((GR, d // 2), BF16),
            pltpu.VMEM((GR, d // 2), BF16),
            pltpu.VMEM((GR, d), BF16),
            pltpu.VMEM((GR, d), BF16),
            dma((4,)), dma((8,)), dma((8,)), dma((4,)), dma((4,)),
            dma((8,)), dma((8,)), dma((4,)), dma((4,)), dma((4,)), dma((4,)),
        ],
        compiler_params=pltpu.CompilerParams(
            collective_id=1, has_side_effects=True, vmem_limit_bytes=60 * 2**20),
        cost_estimate=pl.CostEstimate(
            flops=26_000_000_000, bytes_accessed=32_000_000, transcendentals=0),
        name="feed_forward",
    )(mixed, stream, wo, w, gain.reshape(1, -1))


def per_device(
    stream, queries, projected_keys, values, decay_gate_logits, decay_gate_bias, extra_log_decay,
    document_index, output_gate, head_norm_gain, output_weight, feedforward_norm_gain,
    gate_weight, up_weight, down_weight,
):
    own_rows, units = gate_weight.shape
    pair = jnp.stack(
        [gate_weight.reshape(own_rows, -1, 128), up_weight.reshape(own_rows, -1, 128)], axis=2)
    shard = jnp.concatenate([pair.reshape(own_rows, 2 * units), down_weight.T], axis=1)
    weights = lax.all_gather(shard, SP, axis=0, tiled=True)
    whole_out = lax.all_gather(output_weight, "tp", axis=0, tiled=True)
    head_mixed = attention(
        queries, projected_keys, values, decay_gate_logits, decay_gate_bias, extra_log_decay,
        document_index, output_gate, head_norm_gain)
    return feed_forward(head_mixed, stream, whole_out, weights, feedforward_norm_gain)


def solution(mesh):
    torus = Mesh(mesh.devices.reshape(4, 4, 2, mesh.shape["tp"]), ("sp_0", "sp_1", "sp_2", "tp"))
    placed = (
        P(SP, None), P(SP, "tp"), P(SP, "tp"), P(SP, "tp"), P(SP, "tp"), P("tp"), P(SP, "tp"),
        P(SP), P(SP, "tp"), P(), P("tp", None), P(), P(SP, "tp"), P(SP, "tp"), P("tp", SP),
    )
    return jax.shard_map(
        per_device, mesh=torus, in_specs=placed, out_specs=P(SP_TP, None), check_vma=False
    )
```

```python
import functools
import jax
import jax.numpy as jnp
from jax import lax
from jax.experimental import pallas as pl
from jax.experimental.pallas import tpu as pltpu
from jax.sharding import Mesh
from jax.sharding import PartitionSpec as P

SP = ("sp_0", "sp_1", "sp_2")
SP_TP = ("sp_0", "sp_1", "sp_2", "tp")
MESH = pl.DeviceIdType.MESH
F32 = jnp.float32
BF16 = jnp.bfloat16
TAU = 16.0
EPS = 1e-06
BL = 64
GR = 256
DK = 128
DV = 256
NZ, NY = 4, 4
NCHIP = NZ * NY


def nt_dot(a, b):
    return lax.dot_general(a, b, (((1,), (1,)), ((), ())), preferred_element_type=F32)


def tn_dot(a, b):
    return lax.dot_general(a, b, (((0,), (0,)), ((), ())), preferred_element_type=F32)


def nn_dot(a, b):
    return lax.dot_general(a, b, (((1,), (0,)), ((), ())), preferred_element_type=F32)


def remote_copy(src, dst, send, recv, target):
    return pltpu.make_async_remote_copy(
        src, dst, send, recv, device_id=target, device_id_type=MESH)


class PlaneGather:
    SEMS = (40, 40, 32, 32, 1)

    def __init__(self, src, dst, sems):
        self.src, self.dst = src, dst
        self.send, self.recv, self.core_send, self.core_recv, self.local = sems
        self.at = {"z": lax.axis_index("sp_0"), "y": lax.axis_index("sp_1")}
        self.core, self.x = lax.axis_index("sp_2"), lax.axis_index("tp")
        self.rows = src.shape[0] // 2

    def shifted(self, moves):
        at = dict(self.at)
        for axis, k in moves:
            at[axis] = lax.rem(at[axis] + (k + 4), 4)
        return at["z"], at["y"]

    def chip_at(self, axis, k):
        z, y = self.shifted([(axis, k)])
        return z, y, self.core, self.x

    def piece(self, hf, ja, jb, sub=None):
        a, b = ("y", "z") if hf == 0 else ("z", "y")
        z, y = self.shifted([(a, ja), (b, jb)])
        row = ((z * NY + y) * 2 + self.core) * (2 * self.rows) + hf * self.rows
        size = self.rows
        if sub is not None:
            size = size // 2
            row = row + sub * size
        return self.dst.at[pl.ds(pl.multiple_of(row, 16), size)]

    def axis(self, hf, stage):
        return ("y", "z")[(hf + stage) % 2]

    OFFS = (0, -1, 1, 2)

    def hop(self, hf, stage, ja, way, forward):
        axis = self.axis(hf, stage)
        k = hf * 20 + (0 if stage == 0 else 4 + 4 * self.OFFS.index(ja)) + (0 if way > 0 else 1)
        k = k + (2 if forward else 0)
        target = self.chip_at(axis, way)
        if forward:
            sub = 0 if way > 0 else 1
            ref = self.piece(hf, -way, 0, sub) if stage == 0 else self.piece(hf, ja, -way, sub)
            src = ref
        else:
            ref = self.piece(hf, 0, 0) if stage == 0 else self.piece(hf, ja, 0)
            own = stage == 0 or ja == 0
            src = self.src.at[pl.ds(hf * self.rows, self.rows)] if own else ref
        return remote_copy(src, ref, self.send.at[k], self.recv.at[k], target)

    def landing(self, hf, stage, ja, way, forward):
        axis = self.axis(hf, stage)
        k = hf * 20 + (0 if stage == 0 else 4 + 4 * self.OFFS.index(ja)) + (0 if way > 0 else 1)
        k = k + (2 if forward else 0)
        back = 2 if forward else -way
        sub = (0 if way > 0 else 1) if forward else None
        ref = self.piece(hf, back, 0, sub) if stage == 0 else self.piece(hf, ja, back, sub)
        return remote_copy(ref, ref, self.send.at[k], self.recv.at[k], self.chip_at(axis, way))

    def hand(self, hf, ja, jb):
        p = hf * 16 + self.OFFS.index(ja) * 4 + self.OFFS.index(jb)
        ref = self.piece(hf, ja, jb)
        src = self.src.at[pl.ds(hf * self.rows, self.rows)] if ja == 0 and jb == 0 else ref
        partner = (self.at["z"], self.at["y"], 1 - self.core, self.x)
        return remote_copy(src, ref, self.core_send.at[p], self.core_recv.at[p], partner)

    def handed(self, hf, ja, jb):
        p = hf * 16 + self.OFFS.index(ja) * 4 + self.OFFS.index(jb)
        a, b = ("y", "z") if hf == 0 else ("z", "y")
        z, y = self.shifted([(a, ja), (b, jb)])
        row = ((z * NY + y) * 2 + 1 - self.core) * (2 * self.rows) + hf * self.rows
        ref = self.dst.at[pl.ds(pl.multiple_of(row, 16), self.rows)]
        partner = (self.at["z"], self.at["y"], 1 - self.core, self.x)
        return remote_copy(ref, ref, self.core_send.at[p], self.core_recv.at[p], partner)

    def keep(self):
        row = ((self.at["z"] * NY + self.at["y"]) * 2 + self.core) * (2 * self.rows)
        return pltpu.make_async_copy(
            self.src, self.dst.at[pl.ds(pl.multiple_of(row, 16), 2 * self.rows)], self.local.at[0])

    def start(self):
        for stage in range(2):
            for hf in range(2):
                for way in (1, -1):
                    self.hop(hf, stage, 0, way, False).start()
        for hf in range(2):
            self.hand(hf, 0, 0).start()
        self.keep().start()

    def second(self, hf, ja):
        for way in (1, -1):
            self.hop(hf, 1, ja, way, False).start()
        self.hand(hf, ja, 0).start()

    def near(self):
        for way in (1, -1):
            for hf in range(2):
                self.landing(hf, 0, 0, way, False).wait_recv()
                self.hop(hf, 0, 0, way, True).start()
                self.second(hf, -way)

    def far(self):
        for hf in range(2):
            for way in (1, -1):
                self.landing(hf, 0, 0, way, True).wait_recv()
            self.second(hf, 2)

    def column(self, ja):
        for way in (1, -1):
            for hf in range(2):
                self.landing(hf, 1, ja, way, False).wait_recv()
                self.hop(hf, 1, ja, way, True).start()
                self.hand(hf, ja, -way).start()

    def column_far(self, ja):
        for hf in range(2):
            for way in (1, -1):
                self.landing(hf, 1, ja, way, True).wait_recv()
            self.hand(hf, ja, 2).start()

    def finish(self):
        self.keep().wait()
        for hf in range(2):
            for ja in self.OFFS:
                for jb in self.OFFS:
                    self.handed(hf, ja, jb).wait_recv()

    def drain(self):
        for hf in range(2):
            for way in (1, -1):
                for forward in (False, True):
                    self.hop(hf, 0, 0, way, forward).wait_send()
                    for ja in self.OFFS:
                        self.hop(hf, 1, ja, way, forward).wait_send()
            for ja in self.OFFS:
                for jb in self.OFFS:
                    self.hand(hf, ja, jb).wait_send()


class RowGather:
    SEMS = (4, 4, 3, 3)

    def __init__(self, src, dst, sems):
        self.src, self.dst = src, dst
        self.send, self.recv, self.core_send, self.core_recv = sems
        self.z, self.y = lax.axis_index("sp_0"), lax.axis_index("sp_1")
        self.core, self.x = lax.axis_index("sp_2"), lax.axis_index("tp")
        self.rows = src.shape[0]

    def piece(self, k, core, sub=None):
        size = self.rows // 2
        row = lax.rem(self.x + (k + 4), 4) * self.rows + core * size
        if sub is not None:
            size = size // 2
            row = row + sub * size
        return self.dst.at[pl.ds(pl.multiple_of(row, 16), size)]

    def side(self, way):
        return (self.z, self.y, self.core, lax.rem(self.x + (way + 4), 4))

    def hop(self, way, forward):
        k = (0 if way > 0 else 1) + (2 if forward else 0)
        if forward:
            dst = self.piece(-way, self.core, 0 if way > 0 else 1)
            src = dst
        else:
            dst = self.piece(0, self.core)
            size = self.rows // 2
            src = self.src.at[pl.ds(pl.multiple_of(self.core * size, 16), size)]
        return remote_copy(src, dst, self.send.at[k], self.recv.at[k], self.side(way))

    def landing(self, way, forward):
        k = (0 if way > 0 else 1) + (2 if forward else 0)
        ref = self.piece(2, self.core, 0 if way > 0 else 1) if forward else self.piece(-way, self.core)
        return remote_copy(ref, ref, self.send.at[k], self.recv.at[k], self.side(way))

    def hand(self, i, arriving=False):
        k = (-1, 1, 2)[i]
        ref = self.piece(k, 1 - self.core if arriving else self.core)
        return remote_copy(
            ref, ref, self.core_send.at[i], self.core_recv.at[i], (self.z, self.y, 1 - self.core, self.x))

    def start(self):
        for way in (1, -1):
            self.hop(way, False).start()

    def near(self):
        for i, way in enumerate((1, -1)):
            self.landing(way, False).wait_recv()
            self.hop(way, True).start()
            self.hand(i).start()

    def far(self):
        for way in (1, -1):
            self.landing(way, True).wait_recv()
        self.hand(2).start()

    def finish(self):
        for i in range(3):
            self.hand(i, True).wait_recv()
        for way in (1, -1):
            for forward in (False, True):
                self.hop(way, forward).wait_send()
        for i in range(3):
            self.hand(i).wait_send()


def plane_sems():
    return [pltpu.SemaphoreType.DMA((k,)) for k in PlaneGather.SEMS]


def attention_kernel(
    q_ref, k_ref, v_ref, lg_ref, bias_ref, aux_ref, docrow_ref, gate_ref, gain_ref, shard_ref, wo_ref,
    mixed_ref, whole_ref, whole_wo_ref,
    cum_ref, glob_ref, blk_ref, states_ref, before_ref, run_ref, local_ref,
    own_t, own_e, part_t, part_e, chip_t, chip_e, recv_t, recv_e, mine_c, send_c, part_c, sum_ref,
    core_send, core_recv, t_send, t_recv, e_send, e_recv, *gather_sems,
):
    rows = q_ref.shape[0]
    blocks = rows // BL
    groups = rows // GR
    per = GR // BL
    z, y = lax.axis_index("sp_0"), lax.axis_index("sp_1")
    core, x = lax.axis_index("sp_2"), lax.axis_index("tp")
    chip = z * NY + y
    scale = DK ** (-0.5)

    def chip_peer(k):
        other = lax.rem(chip + k, NCHIP)
        return other, (other // NY, lax.rem(other, NY), core, x)

    partner = (z, y, 1 - core, x)

    recv_t[pl.ds(chip, 1)] = jnp.zeros((1, DV, DK), BF16)

    barrier = pltpu.get_barrier_semaphore()
    pl.semaphore_signal(barrier, inc=1, device_id=partner, device_id_type=MESH)
    for k in range(1, NCHIP):
        pl.semaphore_signal(barrier, inc=1, device_id=chip_peer(k)[1], device_id_type=MESH)
    for k in (1, 3):
        pl.semaphore_signal(
            barrier, inc=1, device_id=(z, y, core, lax.rem(x + k, 4)), device_id_type=MESH)
    pl.semaphore_wait(barrier, NCHIP + 2)
    plane = PlaneGather(shard_ref, whole_ref, gather_sems[:5])
    ring = RowGather(wo_ref, whole_wo_ref, gather_sems[5:])
    plane.start()
    ring.start()

    ri = lax.broadcasted_iota(jnp.int32, (GR, GR), 0)
    ci = lax.broadcasted_iota(jnp.int32, (GR, GR), 1)

    def first(g, base):
        at = pl.multiple_of(g * GR, GR)
        same_block = (ri & (GR - BL)) == (ci & (GR - BL))
        tri = jnp.where(same_block & (ci <= ri), 1.0, 0.0).astype(BF16)
        logits = lg_ref[pl.ds(at, GR), :].astype(F32) + bias_ref[...]
        ld = (jnp.minimum(logits, 0.0) - jnp.log1p(jnp.exp(-jnp.abs(logits)))) / TAU
        extra0 = jnp.broadcast_to(aux_ref[pl.ds(at, GR), 0:1], (GR, DK))
        extra1 = jnp.broadcast_to(aux_ref[pl.ds(at, GR), 1:2], (GR, DK))
        ld = ld + jnp.concatenate([extra0, extra1], axis=1)
        hi = ld.astype(BF16)
        rest = ld - hi.astype(F32)
        mid = rest.astype(BF16)
        low = (rest - mid.astype(F32)).astype(BF16)
        cum = nn_dot(tri, hi) + nn_dot(tri, mid) + nn_dot(tri, low)
        cum_ref[pl.ds(at, GR), :] = cum
        cum3 = cum.reshape(per, BL, 2 * DK)
        ends = cum3[:, BL - 1 : BL, :]
        off, offs = base, []
        for b in range(per):
            offs.append(off)
            blk_ref[pl.ds(g * per + b, 1)] = ends[b : b + 1]
            off = off + ends[b]
        for b in range(per):
            glob_ref[pl.ds(pl.multiple_of(at + b * BL, BL), BL), :] = cum3[b] + offs[b]
        doc = aux_ref[pl.ds(at, GR), 2:3].reshape(per, BL, 1)
        tail_mask = jnp.where(doc == doc[:, BL - 1 : BL], 1.0, 0.0)
        head_mask = jnp.where(doc == doc[:, 0:1], 1.0, 0.0)
        kf = k_ref[pl.ds(at, GR), :].astype(F32).reshape(per, BL, 2 * DK)
        tail = (kf * jnp.exp(ends - cum3) * tail_mask).astype(BF16)
        head = (kf * jnp.exp(cum3) * head_mask).astype(BF16)
        for b in range(per):
            for h in range(2):
                keys = jnp.concatenate(
                    [tail[b][:, h * DK : (h + 1) * DK], head[b][:, h * DK : (h + 1) * DK]], axis=1
                )
                vals = v_ref[pl.ds(pl.multiple_of(at + b * BL, BL), BL), h * DV : (h + 1) * DV]
                states_ref[pl.ds((g * per + b) * 2 + h, 1)] = tn_dot(vals, keys)[None]
        return off

    total = lax.fori_loop(0, groups, first, jnp.zeros((1, 2 * DK), F32))
    sum_ref[...] = total

    run_ref[...] = jnp.zeros_like(run_ref)

    def doc_at(r):
        return aux_ref[pl.ds(r, 1), 2:3]

    def step(b, _):
        lo = jnp.maximum(b * BL - 1, 0)
        keep = jnp.where(doc_at(lo) == doc_at(b * BL + BL - 1), 1.0, 0.0)
        decay = jnp.exp(blk_ref[pl.ds(b, 1)][0]) * keep
        r = blocks - 1 - b
        hi = jnp.minimum(r * BL + BL, rows - 1)
        keep_b = jnp.where(doc_at(hi) == doc_at(r * BL), 1.0, 0.0)
        decay_b = jnp.exp(blk_ref[pl.ds(r, 1)][0]) * keep_b
        for h in range(2):
            fw = run_ref[h, :, :DK]
            before_ref[pl.ds(b * 2 + h, 1), :, :DK] = fw.astype(BF16)[None]
            run_ref[h, :, :DK] = fw * decay[:, h * DK : (h + 1) * DK] + states_ref[b * 2 + h, :, :DK]
            bw = run_ref[h, :, DK:]
            before_ref[pl.ds(r * 2 + h, 1), :, DK:] = bw.astype(BF16)[None]
            run_ref[h, :, DK:] = bw * decay_b[:, h * DK : (h + 1) * DK] + states_ref[r * 2 + h, :, DK:]
        return 0

    lax.fori_loop(0, blocks, step, 0)
    first_doc = jnp.broadcast_to(doc_at(0), (1, DK))
    last_doc = jnp.broadcast_to(doc_at(rows - 1), (1, DK))
    for h in range(2):
        own_t[h, :DV] = run_ref[h, :, :DK].astype(BF16)
        own_t[h, DV:] = run_ref[h, :, DK:].astype(BF16)
        own_e[h, 0:1] = total[:, h * DK : (h + 1) * DK]
        own_e[h, 1:2] = first_doc
        own_e[h, 2:3] = last_doc
        own_e[h, 3:8] = jnp.zeros((5, DK), F32)

    swap_t = pltpu.make_async_remote_copy(
        own_t.at[1 - core], part_t, core_send.at[0], core_recv.at[0],
        device_id=partner, device_id_type=MESH)
    swap_e = pltpu.make_async_remote_copy(
        own_e.at[1 - core], part_e, core_send.at[1], core_recv.at[1],
        device_id=partner, device_id_type=MESH)
    swap_t.start()
    swap_e.start()
    swap_t.wait()
    swap_e.wait()
    is0 = core == 0
    mine_e = own_e[pl.ds(core, 1)][0]
    other_e = part_e[...]
    e0 = jnp.where(is0, mine_e, other_e)
    e1 = jnp.where(is0, other_e, mine_e)
    mine_t = own_t[pl.ds(core, 1)][0].astype(F32)
    other_t = part_t[...].astype(F32)
    t0 = jnp.where(is0, mine_t, other_t)
    t1 = jnp.where(is0, other_t, mine_t)
    through1 = jnp.exp(e1[0:1]) * jnp.where(e0[2:3] == e1[2:3], 1.0, 0.0)
    through0 = jnp.exp(e0[0:1]) * jnp.where(e1[1:2] == e0[1:2], 1.0, 0.0)
    chip_t[0] = (t1[:DV] + through1 * t0[:DV]).astype(BF16)
    chip_t[1] = (t0[DV:] + through0 * t1[DV:]).astype(BF16)
    chip_row = jnp.concatenate(
        [e0[0:1] + e1[0:1], e0[1:2], e1[2:3], jnp.zeros((5, DK), F32)], axis=0)
    chip_e[...] = chip_row
    recv_e[pl.ds(chip, 1)] = chip_row[None]

    sends = []
    for k in range(1, NCHIP):
        other, target = chip_peer(k)
        back = jnp.where(other > chip, 0, 1)
        sends.append(pltpu.make_async_remote_copy(
            chip_e, recv_e.at[chip], e_send.at[k], e_recv.at[k],
            device_id=target, device_id_type=MESH))
        sends.append(pltpu.make_async_remote_copy(
            chip_t.at[back], recv_t.at[chip], t_send.at[k], t_recv.at[k],
            device_id=target, device_id_type=MESH))
    for s in sends:
        s.start()
    plane.near()

    def inside(g, _):
        at = pl.multiple_of(g * GR, GR)
        same_block = (ri & (GR - BL)) == (ci & (GR - BL))
        doc = aux_ref[pl.ds(at, GR), 2:3]
        same = same_block & (doc == docrow_ref[pl.ds(g, 1), :])
        below = same & (ci <= ri)
        above = same & (ci >= ri)
        cum3 = cum_ref[pl.ds(at, GR), :].reshape(per, BL, 2 * DK)
        middle = cum3[:, BL // 2 - 1 : BL // 2]
        ends = cum3[:, BL - 1 : BL]
        rising = jnp.exp(cum3 - middle)
        falling = jnp.exp(middle - cum3)
        qf = q_ref[pl.ds(at, GR), :].astype(F32).reshape(per, BL, 2 * DK) * scale
        kf = k_ref[pl.ds(at, GR), :].astype(F32).reshape(per, BL, 2 * DK)
        q_rise = (qf * rising).astype(BF16).reshape(GR, 2 * DK)
        q_fall = (qf * falling).astype(BF16).reshape(GR, 2 * DK)
        k_rise = (kf * rising).astype(BF16).reshape(GR, 2 * DK)
        k_fall = (kf * falling).astype(BF16).reshape(GR, 2 * DK)
        q_fwd = qf * jnp.exp(cum3)
        q_bwd = qf * jnp.exp(ends - cum3)
        for h in range(2):
            c = slice(h * DK, (h + 1) * DK)
            fw = nt_dot(q_rise[:, c], k_fall[:, c])
            bw = nt_dot(q_fall[:, c], k_rise[:, c])
            scores = jnp.where(below, fw, 0.0) + jnp.where(above, bw, 0.0)
            vals = v_ref[pl.ds(at, GR), h * DV : (h + 1) * DV]
            local_ref[pl.ds(at, GR), h * DV : (h + 1) * DV] = nn_dot(scores.astype(BF16), vals)
        for b in range(per):
            start = at + b * BL
            prev = doc_at(jnp.maximum(start - 1, 0))
            following = doc_at(jnp.minimum(start + BL, rows - 1))
            rows_doc = doc[b * BL : (b + 1) * BL]
            hit_f = jnp.where(rows_doc == prev, 1.0, 0.0)
            hit_b = jnp.where(rows_doc == following, 1.0, 0.0)
            for h in range(2):
                c = slice(h * DK, (h + 1) * DK)
                both = jnp.concatenate([q_fwd[b][:, c] * hit_f, q_bwd[b][:, c] * hit_b], axis=1)
                here = pl.ds(pl.multiple_of(start, BL), BL)
                local_ref[here, h * DV : (h + 1) * DV] += nt_dot(
                    both.astype(BF16), before_ref[(g * per + b) * 2 + h])
        return 0

    lax.fori_loop(0, groups // 2, inside, 0)
    plane.far()
    plane.column(0)
    lax.fori_loop(groups // 2, groups, inside, 0)
    ring.near()
    plane.column(-1)

    for s in sends:
        s.wait()
    plane.column(1)
    run_ref[0] = jnp.zeros_like(run_ref[0])

    def earlier(j, _):
        e = recv_e[j]
        p = recv_e[jnp.maximum(j - 1, 0)]
        keep = jnp.exp(e[0:1]) * jnp.where(e[2:3] == p[2:3], 1.0, 0.0)
        run_ref[0, :, :DK] = recv_t[j].astype(F32) + run_ref[0, :, :DK] * keep
        return 0

    def later(i, _):
        j = NCHIP - 1 - i
        e = recv_e[j]
        p = recv_e[jnp.minimum(j + 1, NCHIP - 1)]
        keep = jnp.exp(e[0:1]) * jnp.where(e[1:2] == p[1:2], 1.0, 0.0)
        run_ref[0, :, DK:] = recv_t[j].astype(F32) + run_ref[0, :, DK:] * keep
        return 0

    lax.fori_loop(0, chip, earlier, 0)
    lax.fori_loop(0, NCHIP - 1 - chip, later, 0)
    cf, cb = run_ref[0, :, :DK], run_ref[0, :, DK:]
    before_doc = jnp.where(chip > 0, recv_e[jnp.maximum(chip - 1, 0)][2:3], -1.0)
    after_doc = jnp.where(
        chip < NCHIP - 1, recv_e[jnp.minimum(chip + 1, NCHIP - 1)][1:2], -1.0)
    pass0 = jnp.exp(e0[0:1]) * jnp.where(before_doc == e0[2:3], 1.0, 0.0)
    pass1 = jnp.exp(e1[0:1]) * jnp.where(after_doc == e1[1:2], 1.0, 0.0)
    mine_t = own_t[pl.ds(core, 1)][0].astype(F32)
    other_t = part_t[...].astype(F32)
    t0f = jnp.where(is0, mine_t[:DV], other_t[:DV])
    t1b = jnp.where(is0, other_t[DV:], mine_t[DV:])
    c0 = jnp.concatenate([cf, t1b + pass1 * cb], axis=1)
    c1 = jnp.concatenate([t0f + pass0 * cf, cb], axis=1)
    mine_c[...] = jnp.where(is0, c0, c1).astype(BF16)
    send_c[...] = jnp.where(is0, c1, c0).astype(BF16)
    swap_c = pltpu.make_async_remote_copy(
        send_c, part_c, core_send.at[2], core_recv.at[2],
        device_id=partner, device_id_type=MESH)
    swap_c.start()
    enter_f = jnp.where(is0, before_doc, e0[2:3])[:, 0:1]
    enter_b = jnp.where(is0, e1[1:2], after_doc)[:, 0:1]
    swap_c.wait()

    def last(g, _):
        at = pl.multiple_of(g * GR, GR)
        doc = aux_ref[pl.ds(at, GR), 2:3]
        hit_f = jnp.where(doc == enter_f, 1.0, 0.0)
        hit_b = jnp.where(doc == enter_b, 1.0, 0.0)
        glob = glob_ref[pl.ds(at, GR), :]
        qf = q_ref[pl.ds(at, GR), :].astype(F32) * scale
        q_fwd = (qf * jnp.exp(glob) * hit_f).astype(BF16)
        q_bwd = (qf * jnp.exp(sum_ref[...] - glob) * hit_b).astype(BF16)
        gain = gain_ref[...].astype(F32)
        for h in range(2):
            c = slice(h * DK, (h + 1) * DK)
            both = jnp.concatenate([q_fwd[:, c], q_bwd[:, c]], axis=1)
            carry = jnp.where(h == core, mine_c[...], part_c[...])
            out = local_ref[pl.ds(at, GR), h * DV : (h + 1) * DV] + nt_dot(both, carry)
            out = out * lax.rsqrt(jnp.mean(out * out, axis=-1, keepdims=True) + EPS) * gain
            u = gate_ref[pl.ds(at, GR), h * DV : (h + 1) * DV].astype(F32)
            mixed_ref[pl.ds(at, GR), h * DV : (h + 1) * DV] = (
                out * (u / (1.0 + jnp.exp(-u)))).astype(BF16)
        return 0

    lax.fori_loop(0, groups, last, 0)
    plane.column(2)
    for ja in PlaneGather.OFFS:
        plane.column_far(ja)
    ring.far()
    plane.finish()
    plane.drain()
    ring.finish()


def attention(q, k, v, lg, bias, extra, doc, gate, gain, shard, wo):
    rows = q.shape[0]
    doc_f = doc.astype(F32)
    aux = jnp.concatenate([extra, doc_f[:, None]], axis=1)
    docrow = doc_f.reshape(rows // GR, GR)
    vm = pl.BlockSpec(memory_space=pltpu.VMEM)
    hbm = pl.BlockSpec(memory_space=pl.ANY)
    blocks = rows // BL
    return pl.pallas_call(
        attention_kernel,
        out_shape=(
            jax.ShapeDtypeStruct((rows, 2 * DV), BF16),
            jax.ShapeDtypeStruct((shard.shape[0] * 2 * NCHIP, shard.shape[1]), BF16),
            jax.ShapeDtypeStruct((wo.shape[0] * 4, wo.shape[1]), BF16),
        ),
        in_specs=[vm] * 10 + [hbm],
        out_specs=(vm, hbm, hbm),
        scratch_shapes=[
            pltpu.VMEM((rows, 2 * DK), F32),
            pltpu.VMEM((rows, 2 * DK), F32),
            pltpu.VMEM((blocks, 1, 2 * DK), F32),
            pltpu.VMEM((blocks * 2, DV, 2 * DK), F32),
            pltpu.VMEM((blocks * 2, DV, 2 * DK), BF16),
            pltpu.VMEM((2, DV, 2 * DK), F32),
            pltpu.VMEM((rows, 2 * DV), F32),
            pltpu.VMEM((2, 2 * DV, DK), BF16),
            pltpu.VMEM((2, 8, DK), F32),
            pltpu.VMEM((2 * DV, DK), BF16),
            pltpu.VMEM((8, DK), F32),
            pltpu.VMEM((2, DV, DK), BF16),
            pltpu.VMEM((8, DK), F32),
            pltpu.VMEM((NCHIP, DV, DK), BF16),
            pltpu.VMEM((NCHIP, 8, DK), F32),
            pltpu.VMEM((DV, 2 * DK), BF16),
            pltpu.VMEM((DV, 2 * DK), BF16),
            pltpu.VMEM((DV, 2 * DK), BF16),
            pltpu.VMEM((1, 2 * DK), F32),
            pltpu.SemaphoreType.DMA((3,)),
            pltpu.SemaphoreType.DMA((3,)),
            pltpu.SemaphoreType.DMA((NCHIP,)),
            pltpu.SemaphoreType.DMA((NCHIP,)),
            pltpu.SemaphoreType.DMA((NCHIP,)),
            pltpu.SemaphoreType.DMA((NCHIP,)),
        ] + plane_sems() + [pltpu.SemaphoreType.DMA((k,)) for k in RowGather.SEMS],
        compiler_params=pltpu.CompilerParams(
            collective_id=0, has_side_effects=True, vmem_limit_bytes=48 * 2**20),
        cost_estimate=pl.CostEstimate(flops=3_000_000_000, bytes_accessed=8_000_000, transcendentals=0),
        name="attention",
    )(q, k, v, lg, bias.reshape(1, -1), aux, docrow, gate, gain.reshape(1, -1), shard, wo)


def ffn_kernel(
    mixed_ref, stream_ref, own_wo_ref, wo_ref, w_ref, shard_ref, gain_ref,
    out_ref,
    hm, st, wo_v, w_v, down_v, resid, normed, hidden, s2, s1, s3, ra, rb, rl, rr,
    local_sem, own_rs, own_ls, fwd_rs, fwd_ls, left_in, right_in, opp_l, opp_r,
    rs_send, rs_recv, *gather_sems,
):
    z, y, core = lax.axis_index("sp_0"), lax.axis_index("sp_1"), lax.axis_index("sp_2")
    me = lax.axis_index("tp")
    n = 4
    q_rows = GR
    half = q_rows // 2
    d = out_ref.shape[1]
    units = hidden.shape[1]
    ix_r, ix_l = lax.rem(me + 1, n), lax.rem(me + n - 1, n)
    right, left = (z, y, core, ix_r), (z, y, core, ix_l)

    own = pltpu.make_async_copy(mixed_ref, hm.at[me], local_sem.at[0])
    per = own_wo_ref.shape[0]

    def wo_rows(k):
        return pl.ds(pl.multiple_of(lax.rem(me + k, n) * per, per), per)

    load_wo = [pltpu.make_async_copy(own_wo_ref, wo_v.at[wo_rows(0)], local_sem.at[1])] + [
        pltpu.make_async_copy(wo_ref.at[wo_rows(k)], wo_v.at[wo_rows(k)], local_sem.at[3 + k])
        for k in range(1, n)
    ]
    load_st = pltpu.make_async_copy(stream_ref, st, local_sem.at[2])
    load_w = pltpu.make_async_copy(w_ref, w_v, local_sem.at[3])
    own.start()
    for c in load_wo:
        c.start()
    load_st.start()
    load_w.start()
    barrier = pltpu.get_barrier_semaphore()
    pl.semaphore_signal(barrier, inc=1, device_id=right, device_id_type=MESH)
    pl.semaphore_signal(barrier, inc=1, device_id=left, device_id_type=MESH)
    partner = (z, y, 1 - core, me)
    pl.semaphore_signal(barrier, inc=1, device_id=partner, device_id_type=MESH)
    plane = PlaneGather(shard_ref, down_v, gather_sems)
    for axis in ("z", "y"):
        for k in (1, -1):
            pl.semaphore_signal(
                barrier, inc=1, device_id=plane.chip_at(axis, k), device_id_type=MESH)
    pl.semaphore_wait(barrier, 7)
    own.wait()

    def piece(slot, r, part):
        return hm.at[slot, pl.ds(pl.multiple_of(r * q_rows + part * half, half), half)]

    def remote(ref, send, recv, target, dst=None):
        return pltpu.make_async_remote_copy(
            ref, ref if dst is None else dst, send, recv, device_id=target, device_id_type=MESH)

    order = (2, 1, 3, 0)

    def quarter_of(owner, offset):
        return lax.rem(owner + offset, n)

    def wire(slot, quarter, part, send, recv, target):
        return remote(piece(slot, quarter, part), send, recv, target)

    to_right = (((3, 0), (3, 1), (0, 0)), ((2, 0), (2, 1)), ((0, 1), (1, 0)), ((1, 1),))
    to_left = (((1, 1), (1, 0), (0, 1)), ((0, 0), (3, 1)), ((2, 1), (2, 0)), ((3, 0),))

    def own_right(o, p):
        return wire(me, quarter_of(me, o), p, own_rs.at[o * 2 + p], left_in.at[o * 2 + p], right)

    def own_left(o, p):
        return wire(me, quarter_of(me, o), p, own_ls.at[o * 2 + p], right_in.at[o * 2 + p], left)

    def came_left(o, p):
        return wire(ix_l, quarter_of(ix_l, o), p, own_rs.at[o * 2 + p], left_in.at[o * 2 + p], right)

    def came_right(o, p):
        return wire(ix_r, quarter_of(ix_r, o), p, own_ls.at[o * 2 + p], right_in.at[o * 2 + p], left)

    def fwd_right(i):
        return wire(ix_l, quarter_of(ix_r, order[i]), 0, fwd_rs.at[i], opp_l.at[i], right)

    def fwd_left(i):
        return wire(ix_r, quarter_of(ix_l, order[i]), 1, fwd_ls.at[i], opp_r.at[i], left)

    opposite = lax.rem(me + 2, n)

    def came_opp_l(i):
        return wire(opposite, quarter_of(me, order[i]), 0, fwd_rs.at[i], opp_l.at[i], right)

    def came_opp_r(i):
        return wire(opposite, quarter_of(me, order[i]), 1, fwd_ls.at[i], opp_r.at[i], left)

    def send_own(i):
        for k in range(len(to_right[i])):
            own_right(*to_right[i][k]).start()
            own_left(*to_left[i][k]).start()

    seen = set()

    def arrived(side, o, p):
        if (side, o, p) not in seen:
            seen.add((side, o, p))
            (came_left if side == "l" else came_right)(o, p).wait_recv()

    def pump(i):
        arrived("l", (2 + order[i]) % n, 0)
        fwd_right(i).start()
        arrived("r", (n - 2 + order[i]) % n, 1)
        fwd_left(i).start()

    send_own(0)
    plane.start()
    pump(0)
    send_own(1)
    plane.near()
    for c in load_wo:
        c.wait()
    load_st.wait()

    dh = d // 2
    to_r_a = remote(s2.at[:, pl.ds(0, dh)], rs_send.at[0], rs_recv.at[0], right, ra)
    to_l_b = remote(s2.at[:, pl.ds(dh, dh)], rs_send.at[1], rs_recv.at[1], left, rb)
    to_r = remote(s1, rs_send.at[2], rs_recv.at[2], right, rl)
    to_l = remote(s3, rs_send.at[3], rs_recv.at[3], left, rr)

    for i in range(n):
        q = quarter_of(me, order[i])
        at = pl.multiple_of(q * q_rows, q_rows)
        rows = pl.ds(at, q_rows)
        for p in range(2):
            arrived("l", (1 + order[i]) % n, p)
            arrived("r", (n - 1 + order[i]) % n, p)
        came_opp_l(i).wait_recv()
        came_opp_r(i).wait_recv()

        def project(j, total):
            cols = pl.ds(pl.multiple_of(j * 512, 512), 512)
            acc = st[rows, cols].astype(F32)
            for k in range(n):
                acc = acc + nn_dot(hm[k, rows, :], wo_v[k * 512 : (k + 1) * 512, cols])
            resid[:, cols] = acc
            return total + jnp.sum(acc * acc, axis=-1, keepdims=True)

        squares = lax.fori_loop(0, d // 512, project, jnp.zeros((q_rows, 1), F32))
        if i < n - 1:
            pump(i + 1)
        if i < n - 2:
            send_own(i + 2)
        if i == 0:
            plane.far()
            plane.column(0)
            load_w.wait()
        factor = lax.rsqrt(squares / d + EPS)
        normed[...] = (resid[...] * factor * gain_ref[...].astype(F32)).astype(BF16)

        def gate_up(j, _):
            both = nn_dot(normed[...], w_v[:, pl.ds(pl.multiple_of(j * 256, 256), 256)])
            g, u = both[:, :128], both[:, 128:]
            hidden[:, pl.ds(pl.multiple_of(j * 128, 128), 128)] = (
                g / (1.0 + jnp.exp(-g)) * u).astype(BF16)
            return 0

        lax.fori_loop(0, units // 128, gate_up, 0)
        if i == 0:
            for ja in (-1, 1, 2):
                plane.column(ja)
            for ja in PlaneGather.OFFS:
                plane.column_far(ja)
            plane.finish()
        target = (s2, s1, s3, resid)[i]

        def down(j, _):
            cols = pl.ds(pl.multiple_of(j * 256, 256), 256)
            part = nt_dot(hidden[...], down_v[cols, :]).astype(BF16)
            if i < n - 1:
                target[:, cols] = part
            else:
                target[:, cols] = target[:, cols] + part.astype(F32)
            return 0

        lax.fori_loop(0, d // 256, down, 0)
        if i == 0:
            to_r_a.start()
            to_l_b.start()
        if i == 2:
            to_r_a.wait_recv()
            s1[:, :dh] = (s1[:, :dh].astype(F32) + ra[...].astype(F32)).astype(BF16)
            to_r.start()
            to_l_b.wait_recv()
            s3[:, dh:] = (s3[:, dh:].astype(F32) + rb[...].astype(F32)).astype(BF16)
            to_l.start()

    to_r.wait_recv()
    to_l.wait_recv()
    out_ref[...] = (resid[...] + rl[...].astype(F32) + rr[...].astype(F32)).astype(BF16)

    for o in range(n):
        for p in range(2):
            own_right(o, p).wait_send()
            own_left(o, p).wait_send()
    for i in range(n):
        fwd_right(i).wait_send()
        fwd_left(i).wait_send()
    plane.drain()
    to_r_a.wait_send()
    to_l_b.wait_send()
    to_r.wait_send()
    to_l.wait_send()


def feed_forward(mixed, stream, own_wo, wo, w, shard, gain):
    rows, d = stream.shape
    units = shard.shape[1]
    vm = pl.BlockSpec(memory_space=pltpu.VMEM)
    hbm = pl.BlockSpec(memory_space=pl.ANY)
    dma = pltpu.SemaphoreType.DMA
    return pl.pallas_call(
        ffn_kernel,
        out_shape=jax.ShapeDtypeStruct((GR, d), BF16),
        in_specs=[hbm, hbm, hbm, hbm, hbm, vm, vm],
        out_specs=vm,
        scratch_shapes=[
            pltpu.VMEM((4, rows, mixed.shape[1]), BF16),
            pltpu.VMEM((rows, d), BF16),
            pltpu.VMEM(wo.shape, BF16),
            pltpu.VMEM(w.shape, BF16),
            pltpu.VMEM((d, units), BF16),
            pltpu.VMEM((GR, d), F32),
            pltpu.VMEM((GR, d), BF16),
            pltpu.VMEM((GR, units), BF16),
            pltpu.VMEM((GR, d), BF16),
            pltpu.VMEM((GR, d), BF16),
            pltpu.VMEM((GR, d), BF16),
            pltpu.VMEM((GR, d // 2), BF16),
            pltpu.VMEM((GR, d // 2), BF16),
            pltpu.VMEM((GR, d), BF16),
            pltpu.VMEM((GR, d), BF16),
            dma((8,)), dma((8,)), dma((8,)), dma((4,)), dma((4,)),
            dma((8,)), dma((8,)), dma((4,)), dma((4,)), dma((4,)), dma((4,)),
        ] + plane_sems(),
        compiler_params=pltpu.CompilerParams(
            collective_id=1, has_side_effects=True, vmem_limit_bytes=60 * 2**20),
        cost_estimate=pl.CostEstimate(
            flops=26_000_000_000, bytes_accessed=32_000_000, transcendentals=0),
        name="feed_forward",
    )(mixed, stream, own_wo, wo, w, shard, gain.reshape(1, -1))


def per_device(
    stream, queries, projected_keys, values, decay_gate_logits, decay_gate_bias, extra_log_decay,
    document_index, output_gate, head_norm_gain, output_weight, feedforward_norm_gain,
    gate_weight, up_weight, down_weight,
):
    own_rows, units = gate_weight.shape
    pair = jnp.stack(
        [gate_weight.reshape(own_rows, -1, 128), up_weight.reshape(own_rows, -1, 128)], axis=2)
    shard = pair.reshape(own_rows, 2 * units)
    head_mixed, weights, whole_out = attention(
        queries, projected_keys, values, decay_gate_logits, decay_gate_bias, extra_log_decay,
        document_index, output_gate, head_norm_gain, shard, output_weight)
    return feed_forward(
        head_mixed, stream, output_weight, whole_out, weights, down_weight.T, feedforward_norm_gain)


def solution(mesh):
    torus = Mesh(mesh.devices.reshape(4, 4, 2, mesh.shape["tp"]), ("sp_0", "sp_1", "sp_2", "tp"))
    placed = (
        P(SP, None), P(SP, "tp"), P(SP, "tp"), P(SP, "tp"), P(SP, "tp"), P("tp"), P(SP, "tp"),
        P(SP), P(SP, "tp"), P(), P("tp", None), P(), P(SP, "tp"), P(SP, "tp"), P("tp", SP),
    )
    return jax.shard_map(
        per_device, mesh=torus, in_specs=placed, out_specs=P(SP_TP, None), check_vma=False
    )
```

```python
import functools
import jax
import jax.numpy as jnp
from jax import lax
from jax.experimental import pallas as pl
from jax.experimental.pallas import tpu as pltpu
from jax.sharding import Mesh
from jax.sharding import PartitionSpec as P

SP = ("sp_0", "sp_1", "sp_2")
SP_TP = ("sp_0", "sp_1", "sp_2", "tp")
MESH = pl.DeviceIdType.MESH
F32 = jnp.float32
BF16 = jnp.bfloat16
TAU = 16.0
EPS = 1e-06
BL = 64
GR = 256
DK = 128
DV = 256
NZ, NY = 4, 4
NCHIP = NZ * NY


def nt_dot(a, b):
    return lax.dot_general(a, b, (((1,), (1,)), ((), ())), preferred_element_type=F32)


def tn_dot(a, b):
    return lax.dot_general(a, b, (((0,), (0,)), ((), ())), preferred_element_type=F32)


def nn_dot(a, b):
    return lax.dot_general(a, b, (((1,), (0,)), ((), ())), preferred_element_type=F32)


def remote_copy(src, dst, send, recv, target):
    return pltpu.make_async_remote_copy(
        src, dst, send, recv, device_id=target, device_id_type=MESH)


class PlaneGather:
    SEMS = (40, 40, 32, 32, 1)

    def __init__(self, src, dst, sems):
        self.src, self.dst = src, dst
        self.send, self.recv, self.core_send, self.core_recv, self.local = sems
        self.at = {"z": lax.axis_index("sp_0"), "y": lax.axis_index("sp_1")}
        self.core, self.x = lax.axis_index("sp_2"), lax.axis_index("tp")
        self.rows = src.shape[0] // 2

    def shifted(self, moves):
        at = dict(self.at)
        for axis, k in moves:
            at[axis] = lax.rem(at[axis] + (k + 4), 4)
        return at["z"], at["y"]

    def chip_at(self, axis, k):
        z, y = self.shifted([(axis, k)])
        return z, y, self.core, self.x

    def piece(self, hf, ja, jb, sub=None):
        a, b = ("y", "z") if hf == 0 else ("z", "y")
        z, y = self.shifted([(a, ja), (b, jb)])
        row = ((z * NY + y) * 2 + self.core) * (2 * self.rows) + hf * self.rows
        size = self.rows
        if sub is not None:
            size = size // 2
            row = row + sub * size
        return self.dst.at[pl.ds(pl.multiple_of(row, 16), size)]

    def axis(self, hf, stage):
        return ("y", "z")[(hf + stage) % 2]

    OFFS = (0, -1, 1, 2)

    def hop(self, hf, stage, ja, way, forward):
        axis = self.axis(hf, stage)
        k = hf * 20 + (0 if stage == 0 else 4 + 4 * self.OFFS.index(ja)) + (0 if way > 0 else 1)
        k = k + (2 if forward else 0)
        target = self.chip_at(axis, way)
        if forward:
            sub = 0 if way > 0 else 1
            ref = self.piece(hf, -way, 0, sub) if stage == 0 else self.piece(hf, ja, -way, sub)
            src = ref
        else:
            ref = self.piece(hf, 0, 0) if stage == 0 else self.piece(hf, ja, 0)
            own = stage == 0 or ja == 0
            src = self.src.at[pl.ds(hf * self.rows, self.rows)] if own else ref
        return remote_copy(src, ref, self.send.at[k], self.recv.at[k], target)

    def landing(self, hf, stage, ja, way, forward):
        axis = self.axis(hf, stage)
        k = hf * 20 + (0 if stage == 0 else 4 + 4 * self.OFFS.index(ja)) + (0 if way > 0 else 1)
        k = k + (2 if forward else 0)
        back = 2 if forward else -way
        sub = (0 if way > 0 else 1) if forward else None
        ref = self.piece(hf, back, 0, sub) if stage == 0 else self.piece(hf, ja, back, sub)
        return remote_copy(ref, ref, self.send.at[k], self.recv.at[k], self.chip_at(axis, way))

    def hand(self, hf, ja, jb):
        p = hf * 16 + self.OFFS.index(ja) * 4 + self.OFFS.index(jb)
        ref = self.piece(hf, ja, jb)
        src = self.src.at[pl.ds(hf * self.rows, self.rows)] if ja == 0 and jb == 0 else ref
        partner = (self.at["z"], self.at["y"], 1 - self.core, self.x)
        return remote_copy(src, ref, self.core_send.at[p], self.core_recv.at[p], partner)

    def handed(self, hf, ja, jb):
        p = hf * 16 + self.OFFS.index(ja) * 4 + self.OFFS.index(jb)
        a, b = ("y", "z") if hf == 0 else ("z", "y")
        z, y = self.shifted([(a, ja), (b, jb)])
        row = ((z * NY + y) * 2 + 1 - self.core) * (2 * self.rows) + hf * self.rows
        ref = self.dst.at[pl.ds(pl.multiple_of(row, 16), self.rows)]
        partner = (self.at["z"], self.at["y"], 1 - self.core, self.x)
        return remote_copy(ref, ref, self.core_send.at[p], self.core_recv.at[p], partner)

    def keep(self):
        row = ((self.at["z"] * NY + self.at["y"]) * 2 + self.core) * (2 * self.rows)
        return pltpu.make_async_copy(
            self.src, self.dst.at[pl.ds(pl.multiple_of(row, 16), 2 * self.rows)], self.local.at[0])

    def start(self):
        for stage in range(2):
            for hf in range(2):
                for way in (1, -1):
                    self.hop(hf, stage, 0, way, False).start()
        for hf in range(2):
            self.hand(hf, 0, 0).start()
        self.keep().start()

    def second(self, hf, ja):
        for way in (1, -1):
            self.hop(hf, 1, ja, way, False).start()
        self.hand(hf, ja, 0).start()

    def near(self):
        for way in (1, -1):
            for hf in range(2):
                self.landing(hf, 0, 0, way, False).wait_recv()
                self.hop(hf, 0, 0, way, True).start()
                self.second(hf, -way)

    def far(self):
        for hf in range(2):
            for way in (1, -1):
                self.landing(hf, 0, 0, way, True).wait_recv()
            self.second(hf, 2)

    def column(self, ja):
        for way in (1, -1):
            for hf in range(2):
                self.landing(hf, 1, ja, way, False).wait_recv()
                self.hop(hf, 1, ja, way, True).start()
                self.hand(hf, ja, -way).start()

    def column_far(self, ja):
        for hf in range(2):
            for way in (1, -1):
                self.landing(hf, 1, ja, way, True).wait_recv()
            self.hand(hf, ja, 2).start()

    def finish(self):
        self.keep().wait()
        for hf in range(2):
            for ja in self.OFFS:
                for jb in self.OFFS:
                    self.handed(hf, ja, jb).wait_recv()

    def drain(self):
        for hf in range(2):
            for way in (1, -1):
                for forward in (False, True):
                    self.hop(hf, 0, 0, way, forward).wait_send()
                    for ja in self.OFFS:
                        self.hop(hf, 1, ja, way, forward).wait_send()
            for ja in self.OFFS:
                for jb in self.OFFS:
                    self.hand(hf, ja, jb).wait_send()


class RowGather:
    SEMS = (4, 4, 3, 3)

    def __init__(self, rows, dst, sems):
        self.dst = dst
        self.send, self.recv, self.core_send, self.core_recv = sems
        self.z, self.y = lax.axis_index("sp_0"), lax.axis_index("sp_1")
        self.core, self.x = lax.axis_index("sp_2"), lax.axis_index("tp")
        self.rows = rows

    def piece(self, k, core, sub=None):
        size = self.rows // 2
        row = lax.rem(self.x + (k + 4), 4) * self.rows + core * size
        if sub is not None:
            size = size // 2
            row = row + sub * size
        return self.dst.at[pl.ds(pl.multiple_of(row, 16), size)]

    def side(self, way):
        return (self.z, self.y, self.core, lax.rem(self.x + (way + 4), 4))

    def hop(self, way, forward):
        k = (0 if way > 0 else 1) + (2 if forward else 0)
        if forward:
            dst = self.piece(-way, self.core, 0 if way > 0 else 1)
            src = dst
        else:
            dst = self.piece(0, self.core)
            src = dst
        return remote_copy(src, dst, self.send.at[k], self.recv.at[k], self.side(way))

    def landing(self, way, forward):
        k = (0 if way > 0 else 1) + (2 if forward else 0)
        ref = self.piece(2, self.core, 0 if way > 0 else 1) if forward else self.piece(-way, self.core)
        return remote_copy(ref, ref, self.send.at[k], self.recv.at[k], self.side(way))

    def hand(self, i, arriving=False):
        k = (-1, 1, 2)[i]
        ref = self.piece(k, 1 - self.core if arriving else self.core)
        return remote_copy(
            ref, ref, self.core_send.at[i], self.core_recv.at[i], (self.z, self.y, 1 - self.core, self.x))

    def start(self):
        for way in (1, -1):
            self.hop(way, False).start()

    def near(self):
        for i, way in enumerate((1, -1)):
            self.landing(way, False).wait_recv()
            self.hop(way, True).start()
            self.hand(i).start()

    def far(self):
        for way in (1, -1):
            self.landing(way, True).wait_recv()
        self.hand(2).start()

    def finish(self):
        for i in range(3):
            self.hand(i, True).wait_recv()
        for way in (1, -1):
            for forward in (False, True):
                self.hop(way, forward).wait_send()
        for i in range(3):
            self.hand(i).wait_send()


def plane_sems():
    return [pltpu.SemaphoreType.DMA((k,)) for k in PlaneGather.SEMS]


def layer_kernel(
    q_in, k_in, v_in, lg_in, gate_in, wo_in, stream_in, wg_in, wu_in, wd_in,
    bias_ref, rows_ref, gain_ref, ff_gain_ref,
    out_ref,
    q_ref, k_ref, v_ref, lg_ref, gate_ref, aux_ref, wg_ref, wu_ref, shard_ref, wd_ref,
    cum_ref, blk_ref, off_ref, states_ref, before_ref, run_ref, local_ref,
    own_t, own_e, part_t, part_e, chip_t, chip_e, recv_t, recv_e, mine_c, send_c, part_c, sum_ref,
    hm, st, wo_v, w_v, down_v, resid, normed, hidden, s2, s1, s3, ra, rb, rl, rr,
    local_sem, core_send, core_recv, t_send, t_recv, e_send, e_recv,
    own_rs, own_ls, fwd_rs, fwd_ls, left_in, right_in, opp_l, opp_r, rs_send, rs_recv,
    *gather_sems,
):
    rows = q_ref.shape[0]
    blocks = rows // BL
    groups = rows // GR
    per = GR // BL
    z, y = lax.axis_index("sp_0"), lax.axis_index("sp_1")
    core, me = lax.axis_index("sp_2"), lax.axis_index("tp")
    chip = z * NY + y
    scale = DK ** (-0.5)
    n = 4
    q_rows = GR
    half = q_rows // 2
    d = out_ref.shape[1]
    units = hidden.shape[1]
    ix_r, ix_l = lax.rem(me + 1, n), lax.rem(me + n - 1, n)
    right, left = (z, y, core, ix_r), (z, y, core, ix_l)
    partner = (z, y, 1 - core, me)
    order = (2, 1, 3, 0)

    def quarter_of(owner, offset):
        return lax.rem(owner + offset, n)

    def chip_peer(k):
        other = lax.rem(chip + k, NCHIP)
        return other, (other // NY, lax.rem(other, NY), core, me)

    wo_own = wo_in.shape[0]
    loads = {
        name: pltpu.make_async_copy(src, dst, local_sem.at[i])
        for i, (name, src, dst) in enumerate((
            ("wg", wg_in, wg_ref), ("wu", wu_in, wu_ref), ("wd", wd_in, wd_ref),
            ("wo", wo_in, wo_v.at[pl.ds(pl.multiple_of(me * wo_own, wo_own), wo_own)]),
            ("lg", lg_in, lg_ref), ("k", k_in, k_ref), ("v", v_in, v_ref), ("q", q_in, q_ref),
            ("gate", gate_in, gate_ref),
        ))
    }
    for copy in loads.values():
        copy.start()

    def load_stream(i):
        at = pl.multiple_of(quarter_of(me, order[i]) * q_rows, q_rows)
        return pltpu.make_async_copy(
            stream_in.at[pl.ds(at, q_rows)], st.at[i % 2], local_sem.at[9 + i])

    load_stream(0).start()
    load_stream(1).start()

    recv_t[pl.ds(chip, 1)] = jnp.zeros((1, DV, DK), BF16)

    barrier = pltpu.get_barrier_semaphore()
    pl.semaphore_signal(barrier, inc=1, device_id=partner, device_id_type=MESH)
    pl.semaphore_signal(barrier, inc=1, device_id=right, device_id_type=MESH)
    pl.semaphore_signal(barrier, inc=1, device_id=left, device_id_type=MESH)
    for k in range(1, NCHIP):
        pl.semaphore_signal(barrier, inc=1, device_id=chip_peer(k)[1], device_id_type=MESH)

    loads["wg"].wait()
    loads["wu"].wait()
    for j in range(units // 128):
        shard_ref[:, j * 256 : j * 256 + 128] = wg_ref[:, j * 128 : (j + 1) * 128]
        shard_ref[:, j * 256 + 128 : (j + 1) * 256] = wu_ref[:, j * 128 : (j + 1) * 128]
    loads["wd"].wait()
    loads["wo"].wait()

    pl.semaphore_wait(barrier, NCHIP + 2)
    g1 = PlaneGather(shard_ref, w_v, gather_sems[:5])
    g2 = PlaneGather(wd_ref, down_v, gather_sems[5:10])
    ring = RowGather(wo_own, wo_v, gather_sems[10:])
    ring.start()
    g1.start()
    g2.start()

    ri = lax.broadcasted_iota(jnp.int32, (GR, GR), 0)
    ci = lax.broadcasted_iota(jnp.int32, (GR, GR), 1)

    def columns(g, _):
        at = pl.multiple_of(g * GR, GR)
        for j in range(3):
            row = rows_ref[pl.ds(j * groups + g, 1), :]
            col = jnp.sum(jnp.where(ri == ci, row, 0.0), axis=1, keepdims=True)
            aux_ref[pl.ds(at, GR), j : j + 1] = col
        return 0

    lax.fori_loop(0, groups, columns, 0)
    loads["lg"].wait()
    loads["k"].wait()
    loads["v"].wait()
    run_ref[...] = jnp.zeros_like(run_ref)

    def doc_at(r):
        return aux_ref[pl.ds(r, 1), 2:3]

    def first(g, base):
        at = pl.multiple_of(g * GR, GR)
        same_block = (ri & (GR - BL)) == (ci & (GR - BL))
        tri = jnp.where(same_block & (ci <= ri), 1.0, 0.0).astype(BF16)
        logits = lg_ref[pl.ds(at, GR), :].astype(F32) + bias_ref[...]
        ld = (jnp.minimum(logits, 0.0) - jnp.log1p(jnp.exp(-jnp.abs(logits)))) / TAU
        extra0 = jnp.broadcast_to(aux_ref[pl.ds(at, GR), 0:1], (GR, DK))
        extra1 = jnp.broadcast_to(aux_ref[pl.ds(at, GR), 1:2], (GR, DK))
        ld = ld + jnp.concatenate([extra0, extra1], axis=1)
        hi = ld.astype(BF16)
        rest = ld - hi.astype(F32)
        mid = rest.astype(BF16)
        low = (rest - mid.astype(F32)).astype(BF16)
        cum = nn_dot(tri, hi) + nn_dot(tri, mid) + nn_dot(tri, low)
        cum_ref[pl.ds(at, GR), :] = cum
        cum3 = cum.reshape(per, BL, 2 * DK)
        ends = cum3[:, BL - 1 : BL, :]
        off = base
        for b in range(per):
            off_ref[pl.ds(g * per + b, 1)] = off[None]
            blk_ref[pl.ds(g * per + b, 1)] = ends[b : b + 1]
            off = off + ends[b]
        doc = aux_ref[pl.ds(at, GR), 2:3].reshape(per, BL, 1)
        tail_mask = jnp.where(doc == doc[:, BL - 1 : BL], 1.0, 0.0)
        head_mask = jnp.where(doc == doc[:, 0:1], 1.0, 0.0)
        kf = k_ref[pl.ds(at, GR), :].astype(F32).reshape(per, BL, 2 * DK)
        tail = (kf * jnp.exp(ends - cum3) * tail_mask).astype(BF16)
        head = (kf * jnp.exp(cum3) * head_mask).astype(BF16)
        for b in range(per):
            start = at + b * BL
            keep = jnp.where(doc_at(jnp.maximum(start - 1, 0)) == doc_at(start + BL - 1), 1.0, 0.0)
            decay = jnp.exp(ends[b]) * keep
            for h in range(2):
                c = slice(h * DK, (h + 1) * DK)
                keys = jnp.concatenate([tail[b][:, c], head[b][:, c]], axis=1)
                vals = v_ref[pl.ds(pl.multiple_of(start, BL), BL), h * DV : (h + 1) * DV]
                both = tn_dot(vals, keys)
                slot = (g * per + b) * 2 + h
                states_ref[pl.ds(slot, 1)] = both[None, :, DK:]
                fw = run_ref[h, :, :DK]
                before_ref[pl.ds(slot, 1), :, :DK] = fw.astype(BF16)[None]
                run_ref[h, :, :DK] = fw * decay[:, c] + both[:, :DK]
        return off

    total = lax.fori_loop(0, groups, first, jnp.zeros((1, 2 * DK), F32))
    sum_ref[...] = total

    def step(b, _):
        r = blocks - 1 - b
        hi = jnp.minimum(r * BL + BL, rows - 1)
        keep = jnp.where(doc_at(hi) == doc_at(r * BL), 1.0, 0.0)
        decay = jnp.exp(blk_ref[pl.ds(r, 1)][0]) * keep
        for h in range(2):
            bw = run_ref[h, :, DK:]
            before_ref[pl.ds(r * 2 + h, 1), :, DK:] = bw.astype(BF16)[None]
            run_ref[h, :, DK:] = bw * decay[:, h * DK : (h + 1) * DK] + states_ref[r * 2 + h]
        return 0

    lax.fori_loop(0, blocks, step, 0)
    first_doc = jnp.broadcast_to(doc_at(0), (1, DK))
    last_doc = jnp.broadcast_to(doc_at(rows - 1), (1, DK))
    for h in range(2):
        own_t[h, :DV] = run_ref[h, :, :DK].astype(BF16)
        own_t[h, DV:] = run_ref[h, :, DK:].astype(BF16)
        own_e[h, 0:1] = total[:, h * DK : (h + 1) * DK]
        own_e[h, 1:2] = first_doc
        own_e[h, 2:3] = last_doc
        own_e[h, 3:8] = jnp.zeros((5, DK), F32)

    swap_t = pltpu.make_async_remote_copy(
        own_t.at[1 - core], part_t, core_send.at[0], core_recv.at[0],
        device_id=partner, device_id_type=MESH)
    swap_e = pltpu.make_async_remote_copy(
        own_e.at[1 - core], part_e, core_send.at[1], core_recv.at[1],
        device_id=partner, device_id_type=MESH)
    swap_t.start()
    swap_e.start()
    swap_t.wait()
    swap_e.wait()
    is0 = core == 0
    mine_e = own_e[pl.ds(core, 1)][0]
    other_e = part_e[...]
    e0 = jnp.where(is0, mine_e, other_e)
    e1 = jnp.where(is0, other_e, mine_e)
    mine_t = own_t[pl.ds(core, 1)][0].astype(F32)
    other_t = part_t[...].astype(F32)
    t0 = jnp.where(is0, mine_t, other_t)
    t1 = jnp.where(is0, other_t, mine_t)
    through1 = jnp.exp(e1[0:1]) * jnp.where(e0[2:3] == e1[2:3], 1.0, 0.0)
    through0 = jnp.exp(e0[0:1]) * jnp.where(e1[1:2] == e0[1:2], 1.0, 0.0)
    chip_t[0] = (t1[:DV] + through1 * t0[:DV]).astype(BF16)
    chip_t[1] = (t0[DV:] + through0 * t1[DV:]).astype(BF16)
    chip_row = jnp.concatenate(
        [e0[0:1] + e1[0:1], e0[1:2], e1[2:3], jnp.zeros((5, DK), F32)], axis=0)
    chip_e[...] = chip_row
    recv_e[pl.ds(chip, 1)] = chip_row[None]

    sends = []
    for k in range(1, NCHIP):
        other, target = chip_peer(k)
        back = jnp.where(other > chip, 0, 1)
        sends.append(pltpu.make_async_remote_copy(
            chip_e, recv_e.at[chip], e_send.at[k], e_recv.at[k],
            device_id=target, device_id_type=MESH))
        sends.append(pltpu.make_async_remote_copy(
            chip_t.at[back], recv_t.at[chip], t_send.at[k], t_recv.at[k],
            device_id=target, device_id_type=MESH))
    for s in sends:
        s.start()
    g1.near()
    loads["q"].wait()

    def inside(g, _):
        at = pl.multiple_of(g * GR, GR)
        same_block = (ri & (GR - BL)) == (ci & (GR - BL))
        doc = aux_ref[pl.ds(at, GR), 2:3]
        same = same_block & (doc == rows_ref[pl.ds(2 * groups + g, 1), :])
        below = same & (ci <= ri)
        above = same & (ci >= ri)
        cum3 = cum_ref[pl.ds(at, GR), :].reshape(per, BL, 2 * DK)
        middle = cum3[:, BL // 2 - 1 : BL // 2]
        ends = cum3[:, BL - 1 : BL]
        rising = jnp.exp(cum3 - middle)
        falling = jnp.exp(middle - cum3)
        qf = q_ref[pl.ds(at, GR), :].astype(F32).reshape(per, BL, 2 * DK) * scale
        kf = k_ref[pl.ds(at, GR), :].astype(F32).reshape(per, BL, 2 * DK)
        q_rise = (qf * rising).astype(BF16).reshape(GR, 2 * DK)
        q_fall = (qf * falling).astype(BF16).reshape(GR, 2 * DK)
        k_rise = (kf * rising).astype(BF16).reshape(GR, 2 * DK)
        k_fall = (kf * falling).astype(BF16).reshape(GR, 2 * DK)
        q_fwd = qf * jnp.exp(cum3)
        q_bwd = qf * jnp.exp(ends - cum3)
        for h in range(2):
            c = slice(h * DK, (h + 1) * DK)
            fw = nt_dot(q_rise[:, c], k_fall[:, c])
            bw = nt_dot(q_fall[:, c], k_rise[:, c])
            scores = jnp.where(below, fw, 0.0) + jnp.where(above, bw, 0.0)
            vals = v_ref[pl.ds(at, GR), h * DV : (h + 1) * DV]
            local_ref[pl.ds(at, GR), h * DV : (h + 1) * DV] = nn_dot(scores.astype(BF16), vals)
        for b in range(per):
            start = at + b * BL
            prev = doc_at(jnp.maximum(start - 1, 0))
            following = doc_at(jnp.minimum(start + BL, rows - 1))
            rows_doc = doc[b * BL : (b + 1) * BL]
            hit_f = jnp.where(rows_doc == prev, 1.0, 0.0)
            hit_b = jnp.where(rows_doc == following, 1.0, 0.0)
            for h in range(2):
                c = slice(h * DK, (h + 1) * DK)
                both = jnp.concatenate([q_fwd[b][:, c] * hit_f, q_bwd[b][:, c] * hit_b], axis=1)
                here = pl.ds(pl.multiple_of(start, BL), BL)
                local_ref[here, h * DV : (h + 1) * DV] += nt_dot(
                    both.astype(BF16), before_ref[(g * per + b) * 2 + h])
        return 0

    lax.fori_loop(0, groups // 2, inside, 0)
    g2.near()
    lax.fori_loop(groups // 2, groups, inside, 0)
    g1.far()
    ring.near()

    for s in sends:
        s.wait()
    run_ref[0] = jnp.zeros_like(run_ref[0])

    def earlier(j, _):
        e = recv_e[j]
        p = recv_e[jnp.maximum(j - 1, 0)]
        keep = jnp.exp(e[0:1]) * jnp.where(e[2:3] == p[2:3], 1.0, 0.0)
        run_ref[0, :, :DK] = recv_t[j].astype(F32) + run_ref[0, :, :DK] * keep
        return 0

    def later(i, _):
        j = NCHIP - 1 - i
        e = recv_e[j]
        p = recv_e[jnp.minimum(j + 1, NCHIP - 1)]
        keep = jnp.exp(e[0:1]) * jnp.where(e[1:2] == p[1:2], 1.0, 0.0)
        run_ref[0, :, DK:] = recv_t[j].astype(F32) + run_ref[0, :, DK:] * keep
        return 0

    lax.fori_loop(0, chip, earlier, 0)
    lax.fori_loop(0, NCHIP - 1 - chip, later, 0)
    cf, cb = run_ref[0, :, :DK], run_ref[0, :, DK:]
    before_doc = jnp.where(chip > 0, recv_e[jnp.maximum(chip - 1, 0)][2:3], -1.0)
    after_doc = jnp.where(
        chip < NCHIP - 1, recv_e[jnp.minimum(chip + 1, NCHIP - 1)][1:2], -1.0)
    pass0 = jnp.exp(e0[0:1]) * jnp.where(before_doc == e0[2:3], 1.0, 0.0)
    pass1 = jnp.exp(e1[0:1]) * jnp.where(after_doc == e1[1:2], 1.0, 0.0)
    mine_t = own_t[pl.ds(core, 1)][0].astype(F32)
    other_t = part_t[...].astype(F32)
    t0f = jnp.where(is0, mine_t[:DV], other_t[:DV])
    t1b = jnp.where(is0, other_t[DV:], mine_t[DV:])
    c0 = jnp.concatenate([cf, t1b + pass1 * cb], axis=1)
    c1 = jnp.concatenate([t0f + pass0 * cf, cb], axis=1)
    mine_c[...] = jnp.where(is0, c0, c1).astype(BF16)
    send_c[...] = jnp.where(is0, c1, c0).astype(BF16)
    swap_c = pltpu.make_async_remote_copy(
        send_c, part_c, core_send.at[2], core_recv.at[2],
        device_id=partner, device_id_type=MESH)
    swap_c.start()
    enter_f = jnp.where(is0, before_doc, e0[2:3])[:, 0:1]
    enter_b = jnp.where(is0, e1[1:2], after_doc)[:, 0:1]
    swap_c.wait()

    loads["gate"].wait()

    def last(g):
        at = pl.multiple_of(g * GR, GR)
        doc = aux_ref[pl.ds(at, GR), 2:3]
        hit_f = jnp.where(doc == enter_f, 1.0, 0.0)
        hit_b = jnp.where(doc == enter_b, 1.0, 0.0)
        glob = cum_ref[pl.ds(at, GR), :].reshape(per, BL, 2 * DK) + off_ref[pl.ds(g * per, per)]
        glob = glob.reshape(GR, 2 * DK)
        qf = q_ref[pl.ds(at, GR), :].astype(F32) * scale
        q_fwd = (qf * jnp.exp(glob) * hit_f).astype(BF16)
        q_bwd = (qf * jnp.exp(sum_ref[...] - glob) * hit_b).astype(BF16)
        gain = gain_ref[...].astype(F32)
        for h in range(2):
            c = slice(h * DK, (h + 1) * DK)
            both = jnp.concatenate([q_fwd[:, c], q_bwd[:, c]], axis=1)
            carry = jnp.where(h == core, mine_c[...], part_c[...])
            out = local_ref[pl.ds(at, GR), h * DV : (h + 1) * DV] + nt_dot(both, carry)
            out = out * lax.rsqrt(jnp.mean(out * out, axis=-1, keepdims=True) + EPS) * gain
            u = gate_ref[pl.ds(at, GR), h * DV : (h + 1) * DV].astype(F32)
            hm[me, pl.ds(at, GR), h * DV : (h + 1) * DV] = (
                out * (u / (1.0 + jnp.exp(-u)))).astype(BF16)

    def three(i, _):
        last(quarter_of(me, i + i // 2))
        return 0

    lax.fori_loop(0, 3, three, 0)

    def piece(slot, r, part):
        return hm.at[slot, pl.ds(pl.multiple_of(r * q_rows + part * half, half), half)]

    def remote(ref, send, recv, target, dst=None):
        return pltpu.make_async_remote_copy(
            ref, ref if dst is None else dst, send, recv, device_id=target, device_id_type=MESH)

    def wire(slot, quarter, part, send, recv, target):
        return remote(piece(slot, quarter, part), send, recv, target)

    to_right = (((3, 0), (3, 1), (0, 0)), ((2, 0), (2, 1)), ((0, 1), (1, 0)), ((1, 1),))
    to_left = (((1, 1), (1, 0), (0, 1)), ((0, 0), (3, 1)), ((2, 1), (2, 0)), ((3, 0),))

    def own_right(o, p):
        return wire(me, quarter_of(me, o), p, own_rs.at[o * 2 + p], left_in.at[o * 2 + p], right)

    def own_left(o, p):
        return wire(me, quarter_of(me, o), p, own_ls.at[o * 2 + p], right_in.at[o * 2 + p], left)

    def came_left(o, p):
        return wire(ix_l, quarter_of(ix_l, o), p, own_rs.at[o * 2 + p], left_in.at[o * 2 + p], right)

    def came_right(o, p):
        return wire(ix_r, quarter_of(ix_r, o), p, own_ls.at[o * 2 + p], right_in.at[o * 2 + p], left)

    def fwd_right(i):
        return wire(ix_l, quarter_of(ix_r, order[i]), 0, fwd_rs.at[i], opp_l.at[i], right)

    def fwd_left(i):
        return wire(ix_r, quarter_of(ix_l, order[i]), 1, fwd_ls.at[i], opp_r.at[i], left)

    opposite = lax.rem(me + 2, n)

    def came_opp_l(i):
        return wire(opposite, quarter_of(me, order[i]), 0, fwd_rs.at[i], opp_l.at[i], right)

    def came_opp_r(i):
        return wire(opposite, quarter_of(me, order[i]), 1, fwd_ls.at[i], opp_r.at[i], left)

    def send_own(i):
        for k in range(len(to_right[i])):
            own_right(*to_right[i][k]).start()
            own_left(*to_left[i][k]).start()

    seen = set()

    def arrived(side, o, p):
        if (side, o, p) not in seen:
            seen.add((side, o, p))
            (came_left if side == "l" else came_right)(o, p).wait_recv()

    def pump(i):
        arrived("l", (2 + order[i]) % n, 0)
        fwd_right(i).start()
        arrived("r", (n - 2 + order[i]) % n, 1)
        fwd_left(i).start()

    send_own(0)
    last(quarter_of(me, 2))
    g1.column(0)
    pump(0)
    send_own(1)
    for ja in (-1, 1):
        g1.column(ja)
    g2.far()
    g2.column(0)
    ring.far()
    g1.column(2)
    ring.finish()

    dh = d // 2
    to_r_a = remote(s2.at[:, pl.ds(0, dh)], rs_send.at[0], rs_recv.at[0], right, ra)
    to_l_b = remote(s2.at[:, pl.ds(dh, dh)], rs_send.at[1], rs_recv.at[1], left, rb)
    to_r = remote(s1, rs_send.at[2], rs_recv.at[2], right, rl)
    to_l = remote(s3, rs_send.at[3], rs_recv.at[3], left, rr)

    for i in range(n):
        q = quarter_of(me, order[i])
        at = pl.multiple_of(q * q_rows, q_rows)
        rows = pl.ds(at, q_rows)
        for p in range(2):
            arrived("l", (1 + order[i]) % n, p)
            arrived("r", (n - 1 + order[i]) % n, p)
        came_opp_l(i).wait_recv()
        came_opp_r(i).wait_recv()

        load_stream(i).wait()

        def project(j, total):
            cols = pl.ds(pl.multiple_of(j * 512, 512), 512)
            acc = st[i % 2, :, cols].astype(F32)
            for k in range(n):
                acc = acc + nn_dot(hm[k, rows, :], wo_v[k * 512 : (k + 1) * 512, cols])
            resid[:, cols] = acc
            return total + jnp.sum(acc * acc, axis=-1, keepdims=True)

        squares = lax.fori_loop(0, d // 512, project, jnp.zeros((q_rows, 1), F32))
        if i < n - 1:
            pump(i + 1)
        if i < n - 2:
            send_own(i + 2)
            load_stream(i + 2).start()
        if i == 0:
            for ja in (-1, 1, 2):
                g2.column(ja)
            for ja in PlaneGather.OFFS:
                g1.column_far(ja)
            g1.finish()
        factor = lax.rsqrt(squares / d + EPS)
        normed[...] = (resid[...] * factor * ff_gain_ref[...].astype(F32)).astype(BF16)

        def gate_up(j, _):
            both = nn_dot(normed[...], w_v[:, pl.ds(pl.multiple_of(j * 256, 256), 256)])
            g, u = both[:, :128], both[:, 128:]
            hidden[:, pl.ds(pl.multiple_of(j * 128, 128), 128)] = (
                g / (1.0 + jnp.exp(-g)) * u).astype(BF16)
            return 0

        lax.fori_loop(0, units // 128, gate_up, 0)
        if i == 0:
            for ja in PlaneGather.OFFS:
                g2.column_far(ja)
            g2.finish()
        target = (s2, s1, s3, resid)[i]

        def down(j, _):
            cols = pl.ds(pl.multiple_of(j * 256, 256), 256)
            part = nt_dot(hidden[...], down_v[cols, :]).astype(BF16)
            if i < n - 1:
                target[:, cols] = part
            else:
                target[:, cols] = target[:, cols] + part.astype(F32)
            return 0

        lax.fori_loop(0, d // 256, down, 0)
        if i == 0:
            to_r_a.start()
            to_l_b.start()
        if i == 2:
            to_r_a.wait_recv()
            s1[:, :dh] = (s1[:, :dh].astype(F32) + ra[...].astype(F32)).astype(BF16)
            to_r.start()
            to_l_b.wait_recv()
            s3[:, dh:] = (s3[:, dh:].astype(F32) + rb[...].astype(F32)).astype(BF16)
            to_l.start()

    to_r.wait_recv()
    to_l.wait_recv()
    out_ref[...] = (resid[...] + rl[...].astype(F32) + rr[...].astype(F32)).astype(BF16)

    for o in range(n):
        for p in range(2):
            own_right(o, p).wait_send()
            own_left(o, p).wait_send()
    for i in range(n):
        fwd_right(i).wait_send()
        fwd_left(i).wait_send()
    g1.drain()
    g2.drain()
    to_r_a.wait_send()
    to_l_b.wait_send()
    to_r.wait_send()
    to_l.wait_send()


def layer(q, k, v, lg, bias, extra, doc, gate, gain, wo, stream, ff_gain, wg, wu, wd):
    rows, d = stream.shape
    units = wg.shape[1]
    groups = rows // GR
    table = jnp.concatenate([extra.T, doc.astype(F32)[None]], axis=0).reshape(3 * groups, GR)
    vm = pl.BlockSpec(memory_space=pltpu.VMEM)
    hbm = pl.BlockSpec(memory_space=pl.ANY)
    blocks = rows // BL
    dma = pltpu.SemaphoreType.DMA

    def buf(*shape, dtype=BF16):
        return pltpu.VMEM(shape, dtype)

    return pl.pallas_call(
        layer_kernel,
        out_shape=jax.ShapeDtypeStruct((GR, d), BF16),
        in_specs=[hbm] * 10 + [vm] * 4,
        out_specs=vm,
        scratch_shapes=[
            buf(rows, 2 * DK), buf(rows, 2 * DK), buf(rows, 2 * DV), buf(rows, 2 * DK),
            buf(rows, 2 * DV), buf(rows, 3, dtype=F32),
            buf(*wg.shape), buf(*wu.shape), buf(wg.shape[0], 2 * units), buf(*wd.shape),
            buf(rows, 2 * DK, dtype=F32),
            buf(blocks, 1, 2 * DK, dtype=F32),
            buf(blocks, 1, 2 * DK, dtype=F32),
            buf(blocks * 2, DV, DK, dtype=F32),
            buf(blocks * 2, DV, 2 * DK),
            buf(2, DV, 2 * DK, dtype=F32),
            buf(rows, 2 * DV, dtype=F32),
            buf(2, 2 * DV, DK), buf(2, 8, DK, dtype=F32),
            buf(2 * DV, DK), buf(8, DK, dtype=F32),
            buf(2, DV, DK), buf(8, DK, dtype=F32),
            buf(NCHIP, DV, DK), buf(NCHIP, 8, DK, dtype=F32),
            buf(DV, 2 * DK), buf(DV, 2 * DK), buf(DV, 2 * DK),
            buf(1, 2 * DK, dtype=F32),
            buf(4, rows, 2 * DV), buf(2, GR, d), buf(4 * wo.shape[0], d),
            buf(2 * NCHIP * wg.shape[0], 2 * units), buf(2 * NCHIP * wd.shape[0], units),
            buf(GR, d, dtype=F32), buf(GR, d), buf(GR, units),
            buf(GR, d), buf(GR, d), buf(GR, d), buf(GR, d // 2), buf(GR, d // 2), buf(GR, d), buf(GR, d),
            dma((13,)), dma((3,)), dma((3,)),
            dma((NCHIP,)), dma((NCHIP,)), dma((NCHIP,)), dma((NCHIP,)),
            dma((8,)), dma((8,)), dma((4,)), dma((4,)),
            dma((8,)), dma((8,)), dma((4,)), dma((4,)), dma((4,)), dma((4,)),
        ] + plane_sems() + plane_sems() + [dma((k,)) for k in RowGather.SEMS],
        compiler_params=pltpu.CompilerParams(
            collective_id=0, has_side_effects=True, vmem_limit_bytes=67_043_328),
        cost_estimate=pl.CostEstimate(
            flops=29_000_000_000, bytes_accessed=16_000_000, transcendentals=0),
        name="layer",
    )(q, k, v, lg, gate, wo, stream, wg, wu, wd,
      bias.reshape(1, -1), table, gain.reshape(1, -1), ff_gain.reshape(1, -1))


def per_device(
    stream, queries, projected_keys, values, decay_gate_logits, decay_gate_bias, extra_log_decay,
    document_index, output_gate, head_norm_gain, output_weight, feedforward_norm_gain,
    gate_weight, up_weight, down_weight,
):
    return layer(
        queries, projected_keys, values, decay_gate_logits, decay_gate_bias, extra_log_decay,
        document_index, output_gate, head_norm_gain, output_weight, stream,
        feedforward_norm_gain, gate_weight, up_weight, down_weight.T)


def solution(mesh):
    torus = Mesh(mesh.devices.reshape(4, 4, 2, mesh.shape["tp"]), ("sp_0", "sp_1", "sp_2", "tp"))
    placed = (
        P(SP, None), P(SP, "tp"), P(SP, "tp"), P(SP, "tp"), P(SP, "tp"), P("tp"), P(SP, "tp"),
        P(SP), P(SP, "tp"), P(), P("tp", None), P(), P(SP, "tp"), P(SP, "tp"), P("tp", SP),
    )
    return jax.shard_map(
        per_device, mesh=torus, in_specs=placed, out_specs=P(SP_TP, None), check_vma=False
    )
```

```python
import functools
import jax
import jax.numpy as jnp
from jax import lax
from jax.experimental import pallas as pl
from jax.experimental.pallas import tpu as pltpu
from jax.sharding import Mesh
from jax.sharding import PartitionSpec as P

SP = ("sp_0", "sp_1", "sp_2")
SP_TP = ("sp_0", "sp_1", "sp_2", "tp")
MESH = pl.DeviceIdType.MESH
F32 = jnp.float32
BF16 = jnp.bfloat16
TAU = 16.0
EPS = 1e-06
BL = 64
GR = 256
DK = 128
DV = 256
NZ, NY = 4, 4
NCHIP = NZ * NY


def nt_dot(a, b):
    return lax.dot_general(a, b, (((1,), (1,)), ((), ())), preferred_element_type=F32)


def tn_dot(a, b):
    return lax.dot_general(a, b, (((0,), (0,)), ((), ())), preferred_element_type=F32)


def nn_dot(a, b):
    return lax.dot_general(a, b, (((1,), (0,)), ((), ())), preferred_element_type=F32)


def remote_copy(src, dst, send, recv, target):
    return pltpu.make_async_remote_copy(
        src, dst, send, recv, device_id=target, device_id_type=MESH)


class PlaneGather:
    SEMS = (40, 40, 32, 32, 1)

    def __init__(self, src, dst, sems):
        self.src, self.dst = src, dst
        self.send, self.recv, self.core_send, self.core_recv, self.local = sems
        self.at = {"z": lax.axis_index("sp_0"), "y": lax.axis_index("sp_1")}
        self.core, self.x = lax.axis_index("sp_2"), lax.axis_index("tp")
        self.rows = src.shape[0] // 2

    def shifted(self, moves):
        at = dict(self.at)
        for axis, k in moves:
            at[axis] = lax.rem(at[axis] + (k + 4), 4)
        return at["z"], at["y"]

    def chip_at(self, axis, k):
        z, y = self.shifted([(axis, k)])
        return z, y, self.core, self.x

    def piece(self, hf, ja, jb, sub=None):
        a, b = ("y", "z") if hf == 0 else ("z", "y")
        z, y = self.shifted([(a, ja), (b, jb)])
        row = ((z * NY + y) * 2 + self.core) * (2 * self.rows) + hf * self.rows
        size = self.rows
        if sub is not None:
            size = size // 2
            row = row + sub * size
        return self.dst.at[pl.ds(pl.multiple_of(row, 16), size)]

    def axis(self, hf, stage):
        return ("y", "z")[(hf + stage) % 2]

    OFFS = (0, -1, 1, 2)

    def hop(self, hf, stage, ja, way, forward):
        axis = self.axis(hf, stage)
        k = hf * 20 + (0 if stage == 0 else 4 + 4 * self.OFFS.index(ja)) + (0 if way > 0 else 1)
        k = k + (2 if forward else 0)
        target = self.chip_at(axis, way)
        if forward:
            sub = 0 if way > 0 else 1
            ref = self.piece(hf, -way, 0, sub) if stage == 0 else self.piece(hf, ja, -way, sub)
            src = ref
        else:
            ref = self.piece(hf, 0, 0) if stage == 0 else self.piece(hf, ja, 0)
            own = stage == 0 or ja == 0
            src = self.src.at[pl.ds(hf * self.rows, self.rows)] if own else ref
        return remote_copy(src, ref, self.send.at[k], self.recv.at[k], target)

    def landing(self, hf, stage, ja, way, forward):
        axis = self.axis(hf, stage)
        k = hf * 20 + (0 if stage == 0 else 4 + 4 * self.OFFS.index(ja)) + (0 if way > 0 else 1)
        k = k + (2 if forward else 0)
        back = 2 if forward else -way
        sub = (0 if way > 0 else 1) if forward else None
        ref = self.piece(hf, back, 0, sub) if stage == 0 else self.piece(hf, ja, back, sub)
        return remote_copy(ref, ref, self.send.at[k], self.recv.at[k], self.chip_at(axis, way))

    def hand(self, hf, ja, jb):
        p = hf * 16 + self.OFFS.index(ja) * 4 + self.OFFS.index(jb)
        ref = self.piece(hf, ja, jb)
        src = self.src.at[pl.ds(hf * self.rows, self.rows)] if ja == 0 and jb == 0 else ref
        partner = (self.at["z"], self.at["y"], 1 - self.core, self.x)
        return remote_copy(src, ref, self.core_send.at[p], self.core_recv.at[p], partner)

    def handed(self, hf, ja, jb):
        p = hf * 16 + self.OFFS.index(ja) * 4 + self.OFFS.index(jb)
        a, b = ("y", "z") if hf == 0 else ("z", "y")
        z, y = self.shifted([(a, ja), (b, jb)])
        row = ((z * NY + y) * 2 + 1 - self.core) * (2 * self.rows) + hf * self.rows
        ref = self.dst.at[pl.ds(pl.multiple_of(row, 16), self.rows)]
        partner = (self.at["z"], self.at["y"], 1 - self.core, self.x)
        return remote_copy(ref, ref, self.core_send.at[p], self.core_recv.at[p], partner)

    def keep(self):
        row = ((self.at["z"] * NY + self.at["y"]) * 2 + self.core) * (2 * self.rows)
        return pltpu.make_async_copy(
            self.src, self.dst.at[pl.ds(pl.multiple_of(row, 16), 2 * self.rows)], self.local.at[0])

    def start(self):
        for stage in range(2):
            for hf in range(2):
                for way in (1, -1):
                    self.hop(hf, stage, 0, way, False).start()
        for hf in range(2):
            self.hand(hf, 0, 0).start()
        self.keep().start()

    def second(self, hf, ja):
        for way in (1, -1):
            self.hop(hf, 1, ja, way, False).start()
        self.hand(hf, ja, 0).start()

    def near(self):
        for way in (1, -1):
            for hf in range(2):
                self.landing(hf, 0, 0, way, False).wait_recv()
                self.hop(hf, 0, 0, way, True).start()
                self.second(hf, -way)

    def far(self):
        for hf in range(2):
            for way in (1, -1):
                self.landing(hf, 0, 0, way, True).wait_recv()
            self.second(hf, 2)

    def column(self, ja):
        for way in (1, -1):
            for hf in range(2):
                self.landing(hf, 1, ja, way, False).wait_recv()
                self.hop(hf, 1, ja, way, True).start()
                self.hand(hf, ja, -way).start()

    def column_far(self, ja):
        for hf in range(2):
            for way in (1, -1):
                self.landing(hf, 1, ja, way, True).wait_recv()
            self.hand(hf, ja, 2).start()

    def finish(self):
        self.keep().wait()
        for hf in range(2):
            for ja in self.OFFS:
                for jb in self.OFFS:
                    self.handed(hf, ja, jb).wait_recv()

    def drain(self):
        for hf in range(2):
            for way in (1, -1):
                for forward in (False, True):
                    self.hop(hf, 0, 0, way, forward).wait_send()
                    for ja in self.OFFS:
                        self.hop(hf, 1, ja, way, forward).wait_send()
            for ja in self.OFFS:
                for jb in self.OFFS:
                    self.hand(hf, ja, jb).wait_send()


class RowGather:
    SEMS = (4, 4, 3, 3)

    def __init__(self, rows, dst, sems):
        self.dst = dst
        self.send, self.recv, self.core_send, self.core_recv = sems
        self.z, self.y = lax.axis_index("sp_0"), lax.axis_index("sp_1")
        self.core, self.x = lax.axis_index("sp_2"), lax.axis_index("tp")
        self.rows = rows

    def piece(self, k, core, sub=None):
        size = self.rows // 2
        row = lax.rem(self.x + (k + 4), 4) * self.rows + core * size
        if sub is not None:
            size = size // 2
            row = row + sub * size
        return self.dst.at[pl.ds(pl.multiple_of(row, 16), size)]

    def side(self, way):
        return (self.z, self.y, self.core, lax.rem(self.x + (way + 4), 4))

    def hop(self, way, forward):
        k = (0 if way > 0 else 1) + (2 if forward else 0)
        if forward:
            dst = self.piece(-way, self.core, 0 if way > 0 else 1)
            src = dst
        else:
            dst = self.piece(0, self.core)
            src = dst
        return remote_copy(src, dst, self.send.at[k], self.recv.at[k], self.side(way))

    def landing(self, way, forward):
        k = (0 if way > 0 else 1) + (2 if forward else 0)
        ref = self.piece(2, self.core, 0 if way > 0 else 1) if forward else self.piece(-way, self.core)
        return remote_copy(ref, ref, self.send.at[k], self.recv.at[k], self.side(way))

    def hand(self, i, arriving=False):
        k = (-1, 1, 2)[i]
        ref = self.piece(k, 1 - self.core if arriving else self.core)
        return remote_copy(
            ref, ref, self.core_send.at[i], self.core_recv.at[i], (self.z, self.y, 1 - self.core, self.x))

    def start(self):
        for way in (1, -1):
            self.hop(way, False).start()

    def near(self):
        for way in (1, -1):
            self.landing(way, False).wait_recv()
            self.hop(way, True).start()

    def near_hand(self):
        for i in range(2):
            self.hand(i).start()

    def far(self):
        for way in (1, -1):
            self.landing(way, True).wait_recv()
        self.hand(2).start()

    def finish(self):
        for i in range(3):
            self.hand(i, True).wait_recv()

    def drain(self):
        for way in (1, -1):
            for forward in (False, True):
                self.hop(way, forward).wait_send()
        for i in range(3):
            self.hand(i).wait_send()


def plane_sems():
    return [pltpu.SemaphoreType.DMA((k,)) for k in PlaneGather.SEMS]


def layer_kernel(
    q_in, k_in, v_in, lg_in, gate_in, wo_in, stream_in, wg_in, wu_in, wd_in,
    bias_ref, extra_ref, doc_ref, gains_ref,
    out_ref,
    q_ref, k_ref, v_ref, lg_ref, gate_ref, aux_ref, wg_ref, wu_ref, shard_ref, wd_ref,
    cum_ref, blk_ref, off_ref, states_ref, before_ref, run_ref, local_ref,
    own_t, own_e, part_t, part_e, chip_t, chip_e, recv_t, recv_e, mine_c, send_c, part_c, sum_ref,
    hm, st, wo_v, w_v, down_v, resid, normed, hidden, s2, s1, s3, ra, rb, rl, rr,
    local_sem, core_send, core_recv, t_send, t_recv, e_send, e_recv,
    own_rs, own_ls, fwd_rs, fwd_ls, left_in, right_in, opp_l, opp_r, rs_send, rs_recv,
    *gather_sems,
):
    rows = q_ref.shape[0]
    blocks = rows // BL
    groups = rows // GR
    per = GR // BL
    z, y = lax.axis_index("sp_0"), lax.axis_index("sp_1")
    core, me = lax.axis_index("sp_2"), lax.axis_index("tp")
    chip = z * NY + y
    scale = DK ** (-0.5)
    n = 4
    q_rows = GR
    half = q_rows // 2
    d = out_ref.shape[1]
    units = hidden.shape[1]
    ix_r, ix_l = lax.rem(me + 1, n), lax.rem(me + n - 1, n)
    right, left = (z, y, core, ix_r), (z, y, core, ix_l)
    partner = (z, y, 1 - core, me)
    order = (2, 1, 3, 0)

    def quarter_of(owner, offset):
        return lax.rem(owner + offset, n)

    def chip_peer(k):
        other = lax.rem(chip + k, NCHIP)
        return other, (other // NY, lax.rem(other, NY), core, me)

    wo_own = wo_in.shape[0]
    loads = {
        name: pltpu.make_async_copy(src, dst, local_sem.at[i])
        for i, (name, src, dst) in enumerate((
            ("wg", wg_in, wg_ref), ("wu", wu_in, wu_ref), ("wd", wd_in, wd_ref),
            ("wo", wo_in, wo_v.at[pl.ds(pl.multiple_of(me * wo_own, wo_own), wo_own)]),
            ("lg", lg_in, lg_ref), ("k", k_in, k_ref), ("v", v_in, v_ref), ("q", q_in, q_ref),
            ("gate", gate_in, gate_ref),
        ))
    }
    for copy in loads.values():
        copy.start()

    def load_stream(i):
        at = pl.multiple_of(quarter_of(me, order[i]) * q_rows, q_rows)
        return pltpu.make_async_copy(
            stream_in.at[pl.ds(at, q_rows)], st.at[i % 2], local_sem.at[9 + i])

    load_stream(0).start()
    load_stream(1).start()

    recv_t[pl.ds(chip, 1)] = jnp.zeros((1, DV, DK), BF16)

    barrier = pltpu.get_barrier_semaphore()
    pl.semaphore_signal(barrier, inc=1, device_id=partner, device_id_type=MESH)
    pl.semaphore_signal(barrier, inc=1, device_id=right, device_id_type=MESH)
    pl.semaphore_signal(barrier, inc=1, device_id=left, device_id_type=MESH)
    for k in range(1, NCHIP):
        pl.semaphore_signal(barrier, inc=1, device_id=chip_peer(k)[1], device_id_type=MESH)

    loads["wg"].wait()
    loads["wu"].wait()
    for j in range(units // 128):
        shard_ref[:, j * 256 : j * 256 + 128] = wg_ref[:, j * 128 : (j + 1) * 128]
        shard_ref[:, j * 256 + 128 : (j + 1) * 256] = wu_ref[:, j * 128 : (j + 1) * 128]
    loads["wd"].wait()
    loads["wo"].wait()

    pl.semaphore_wait(barrier, NCHIP + 2)
    g1 = PlaneGather(shard_ref, w_v, gather_sems[:5])
    g2 = PlaneGather(wd_ref, down_v, gather_sems[5:10])
    ring = RowGather(wo_own, wo_v, gather_sems[10:])
    ring.start()
    g1.start()
    g2.start()

    ri = lax.broadcasted_iota(jnp.int32, (GR, GR), 0)
    ci = lax.broadcasted_iota(jnp.int32, (GR, GR), 1)

    def columns(g, _):
        at = pl.multiple_of(g * GR, GR)
        for j in range(3):
            lanes = pl.ds(pl.multiple_of(g * GR, GR), GR)
            row = doc_ref[:, lanes].astype(F32) if j == 2 else extra_ref[j : j + 1, lanes]
            col = jnp.sum(jnp.where(ri == ci, row, 0.0), axis=1, keepdims=True)
            aux_ref[pl.ds(at, GR), j : j + 1] = col
        return 0

    lax.fori_loop(0, groups, columns, 0)
    loads["lg"].wait()
    loads["k"].wait()
    loads["v"].wait()
    run_ref[...] = jnp.zeros_like(run_ref)

    def doc_at(r):
        return aux_ref[pl.ds(r, 1), 2:3]

    def first(g, base):
        at = pl.multiple_of(g * GR, GR)
        same_block = (ri & (GR - BL)) == (ci & (GR - BL))
        tri = jnp.where(same_block & (ci <= ri), 1.0, 0.0).astype(BF16)
        logits = lg_ref[pl.ds(at, GR), :].astype(F32) + bias_ref[...]
        ld = (jnp.minimum(logits, 0.0) - jnp.log1p(jnp.exp(-jnp.abs(logits)))) / TAU
        extra0 = jnp.broadcast_to(aux_ref[pl.ds(at, GR), 0:1], (GR, DK))
        extra1 = jnp.broadcast_to(aux_ref[pl.ds(at, GR), 1:2], (GR, DK))
        ld = ld + jnp.concatenate([extra0, extra1], axis=1)
        hi = ld.astype(BF16)
        rest = ld - hi.astype(F32)
        mid = rest.astype(BF16)
        low = (rest - mid.astype(F32)).astype(BF16)
        cum = nn_dot(tri, hi) + nn_dot(tri, mid) + nn_dot(tri, low)
        cum_ref[pl.ds(at, GR), :] = cum
        cum3 = cum.reshape(per, BL, 2 * DK)
        ends = cum3[:, BL - 1 : BL, :]
        off = base
        for b in range(per):
            off_ref[pl.ds(g * per + b, 1)] = off[None]
            blk_ref[pl.ds(g * per + b, 1)] = ends[b : b + 1]
            off = off + ends[b]
        doc = aux_ref[pl.ds(at, GR), 2:3].reshape(per, BL, 1)
        tail_mask = jnp.where(doc == doc[:, BL - 1 : BL], 1.0, 0.0)
        head_mask = jnp.where(doc == doc[:, 0:1], 1.0, 0.0)
        kf = k_ref[pl.ds(at, GR), :].astype(F32).reshape(per, BL, 2 * DK)
        tail = (kf * jnp.exp(ends - cum3) * tail_mask).astype(BF16)
        head = (kf * jnp.exp(cum3) * head_mask).astype(BF16)
        for b in range(per):
            start = at + b * BL
            keep = jnp.where(doc_at(jnp.maximum(start - 1, 0)) == doc_at(start + BL - 1), 1.0, 0.0)
            decay = jnp.exp(ends[b]) * keep
            for h in range(2):
                c = slice(h * DK, (h + 1) * DK)
                keys = jnp.concatenate([tail[b][:, c], head[b][:, c]], axis=1)
                vals = v_ref[pl.ds(pl.multiple_of(start, BL), BL), h * DV : (h + 1) * DV]
                both = tn_dot(vals, keys)
                slot = (g * per + b) * 2 + h
                states_ref[pl.ds(slot, 1)] = both[None, :, DK:]
                fw = run_ref[h, :, :DK]
                before_ref[pl.ds(slot, 1), :, :DK] = fw.astype(BF16)[None]
                run_ref[h, :, :DK] = fw * decay[:, c] + both[:, :DK]
        return off

    total = lax.fori_loop(0, groups, first, jnp.zeros((1, 2 * DK), F32))
    sum_ref[...] = total

    def step(b, _):
        r = blocks - 1 - b
        hi = jnp.minimum(r * BL + BL, rows - 1)
        keep = jnp.where(doc_at(hi) == doc_at(r * BL), 1.0, 0.0)
        decay = jnp.exp(blk_ref[pl.ds(r, 1)][0]) * keep
        for h in range(2):
            bw = run_ref[h, :, DK:]
            before_ref[pl.ds(r * 2 + h, 1), :, DK:] = bw.astype(BF16)[None]
            run_ref[h, :, DK:] = bw * decay[:, h * DK : (h + 1) * DK] + states_ref[r * 2 + h]
        return 0

    lax.fori_loop(0, blocks, step, 0)
    first_doc = jnp.broadcast_to(doc_at(0), (1, DK))
    last_doc = jnp.broadcast_to(doc_at(rows - 1), (1, DK))
    for h in range(2):
        own_t[h, :DV] = run_ref[h, :, :DK].astype(BF16)
        own_t[h, DV:] = run_ref[h, :, DK:].astype(BF16)
        own_e[h, 0:1] = total[:, h * DK : (h + 1) * DK]
        own_e[h, 1:2] = first_doc
        own_e[h, 2:3] = last_doc
        own_e[h, 3:8] = jnp.zeros((5, DK), F32)

    swap_t = pltpu.make_async_remote_copy(
        own_t.at[1 - core], part_t, core_send.at[0], core_recv.at[0],
        device_id=partner, device_id_type=MESH)
    swap_e = pltpu.make_async_remote_copy(
        own_e.at[1 - core], part_e, core_send.at[1], core_recv.at[1],
        device_id=partner, device_id_type=MESH)
    swap_t.start()
    swap_e.start()
    swap_t.wait()
    swap_e.wait()
    is0 = core == 0
    mine_e = own_e[pl.ds(core, 1)][0]
    other_e = part_e[...]
    e0 = jnp.where(is0, mine_e, other_e)
    e1 = jnp.where(is0, other_e, mine_e)
    mine_t = own_t[pl.ds(core, 1)][0].astype(F32)
    other_t = part_t[...].astype(F32)
    t0 = jnp.where(is0, mine_t, other_t)
    t1 = jnp.where(is0, other_t, mine_t)
    through1 = jnp.exp(e1[0:1]) * jnp.where(e0[2:3] == e1[2:3], 1.0, 0.0)
    through0 = jnp.exp(e0[0:1]) * jnp.where(e1[1:2] == e0[1:2], 1.0, 0.0)
    chip_t[0] = (t1[:DV] + through1 * t0[:DV]).astype(BF16)
    chip_t[1] = (t0[DV:] + through0 * t1[DV:]).astype(BF16)
    chip_row = jnp.concatenate(
        [e0[0:1] + e1[0:1], e0[1:2], e1[2:3], jnp.zeros((5, DK), F32)], axis=0)
    chip_e[...] = chip_row
    recv_e[pl.ds(chip, 1)] = chip_row[None]

    sends = []
    for k in range(1, NCHIP):
        other, target = chip_peer(k)
        back = jnp.where(other > chip, 0, 1)
        sends.append(pltpu.make_async_remote_copy(
            chip_e, recv_e.at[chip], e_send.at[k], e_recv.at[k],
            device_id=target, device_id_type=MESH))
        sends.append(pltpu.make_async_remote_copy(
            chip_t.at[back], recv_t.at[chip], t_send.at[k], t_recv.at[k],
            device_id=target, device_id_type=MESH))
    for s in sends:
        s.start()
    g1.near()
    loads["q"].wait()

    def inside(g, _):
        at = pl.multiple_of(g * GR, GR)
        same_block = (ri & (GR - BL)) == (ci & (GR - BL))
        doc = aux_ref[pl.ds(at, GR), 2:3]
        same = same_block & (doc == doc_ref[:, pl.ds(at, GR)].astype(F32))
        below = same & (ci <= ri)
        above = same & (ci >= ri)
        cum3 = cum_ref[pl.ds(at, GR), :].reshape(per, BL, 2 * DK)
        middle = cum3[:, BL // 2 - 1 : BL // 2]
        ends = cum3[:, BL - 1 : BL]
        rising = jnp.exp(cum3 - middle)
        falling = jnp.exp(middle - cum3)
        qf = q_ref[pl.ds(at, GR), :].astype(F32).reshape(per, BL, 2 * DK) * scale
        kf = k_ref[pl.ds(at, GR), :].astype(F32).reshape(per, BL, 2 * DK)
        q_rise = (qf * rising).astype(BF16).reshape(GR, 2 * DK)
        q_fall = (qf * falling).astype(BF16).reshape(GR, 2 * DK)
        k_rise = (kf * rising).astype(BF16).reshape(GR, 2 * DK)
        k_fall = (kf * falling).astype(BF16).reshape(GR, 2 * DK)
        q_fwd = qf * jnp.exp(cum3)
        q_bwd = qf * jnp.exp(ends - cum3)
        for h in range(2):
            c = slice(h * DK, (h + 1) * DK)
            fw = nt_dot(q_rise[:, c], k_fall[:, c])
            bw = nt_dot(q_fall[:, c], k_rise[:, c])
            scores = jnp.where(below, fw, 0.0) + jnp.where(above, bw, 0.0)
            vals = v_ref[pl.ds(at, GR), h * DV : (h + 1) * DV]
            local_ref[pl.ds(at, GR), h * DV : (h + 1) * DV] = nn_dot(scores.astype(BF16), vals)
        for b in range(per):
            start = at + b * BL
            prev = doc_at(jnp.maximum(start - 1, 0))
            following = doc_at(jnp.minimum(start + BL, rows - 1))
            rows_doc = doc[b * BL : (b + 1) * BL]
            hit_f = jnp.where(rows_doc == prev, 1.0, 0.0)
            hit_b = jnp.where(rows_doc == following, 1.0, 0.0)
            for h in range(2):
                c = slice(h * DK, (h + 1) * DK)
                both = jnp.concatenate([q_fwd[b][:, c] * hit_f, q_bwd[b][:, c] * hit_b], axis=1)
                here = pl.ds(pl.multiple_of(start, BL), BL)
                local_ref[here, h * DV : (h + 1) * DV] += nt_dot(
                    both.astype(BF16), before_ref[(g * per + b) * 2 + h])
        return 0

    lax.fori_loop(0, groups // 2, inside, 0)
    g2.near()
    g1.column(0)
    lax.fori_loop(groups // 2, groups, inside, 0)

    for s in sends:
        s.wait()
    ring.near()
    run_ref[0] = jnp.zeros_like(run_ref[0])

    def earlier(j, _):
        e = recv_e[j]
        p = recv_e[jnp.maximum(j - 1, 0)]
        keep = jnp.exp(e[0:1]) * jnp.where(e[2:3] == p[2:3], 1.0, 0.0)
        run_ref[0, :, :DK] = recv_t[j].astype(F32) + run_ref[0, :, :DK] * keep
        return 0

    def later(i, _):
        j = NCHIP - 1 - i
        e = recv_e[j]
        p = recv_e[jnp.minimum(j + 1, NCHIP - 1)]
        keep = jnp.exp(e[0:1]) * jnp.where(e[1:2] == p[1:2], 1.0, 0.0)
        run_ref[0, :, DK:] = recv_t[j].astype(F32) + run_ref[0, :, DK:] * keep
        return 0

    lax.fori_loop(0, chip, earlier, 0)
    lax.fori_loop(0, NCHIP - 1 - chip, later, 0)
    cf, cb = run_ref[0, :, :DK], run_ref[0, :, DK:]
    before_doc = jnp.where(chip > 0, recv_e[jnp.maximum(chip - 1, 0)][2:3], -1.0)
    after_doc = jnp.where(
        chip < NCHIP - 1, recv_e[jnp.minimum(chip + 1, NCHIP - 1)][1:2], -1.0)
    pass0 = jnp.exp(e0[0:1]) * jnp.where(before_doc == e0[2:3], 1.0, 0.0)
    pass1 = jnp.exp(e1[0:1]) * jnp.where(after_doc == e1[1:2], 1.0, 0.0)
    mine_t = own_t[pl.ds(core, 1)][0].astype(F32)
    other_t = part_t[...].astype(F32)
    t0f = jnp.where(is0, mine_t[:DV], other_t[:DV])
    t1b = jnp.where(is0, other_t[DV:], mine_t[DV:])
    c0 = jnp.concatenate([cf, t1b + pass1 * cb], axis=1)
    c1 = jnp.concatenate([t0f + pass0 * cf, cb], axis=1)
    mine_c[...] = jnp.where(is0, c0, c1).astype(BF16)
    send_c[...] = jnp.where(is0, c1, c0).astype(BF16)
    swap_c = pltpu.make_async_remote_copy(
        send_c, part_c, core_send.at[2], core_recv.at[2],
        device_id=partner, device_id_type=MESH)
    swap_c.start()
    ring.near_hand()
    g2.column(0)
    enter_f = jnp.where(is0, before_doc, e0[2:3])[:, 0:1]
    enter_b = jnp.where(is0, e1[1:2], after_doc)[:, 0:1]
    swap_c.wait()

    loads["gate"].wait()

    def last(g):
        at = pl.multiple_of(g * GR, GR)
        doc = aux_ref[pl.ds(at, GR), 2:3]
        hit_f = jnp.where(doc == enter_f, 1.0, 0.0)
        hit_b = jnp.where(doc == enter_b, 1.0, 0.0)
        glob = cum_ref[pl.ds(at, GR), :].reshape(per, BL, 2 * DK) + off_ref[pl.ds(g * per, per)]
        glob = glob.reshape(GR, 2 * DK)
        qf = q_ref[pl.ds(at, GR), :].astype(F32) * scale
        q_fwd = (qf * jnp.exp(glob) * hit_f).astype(BF16)
        q_bwd = (qf * jnp.exp(sum_ref[...] - glob) * hit_b).astype(BF16)
        gain = gains_ref[:, :DV]
        for h in range(2):
            c = slice(h * DK, (h + 1) * DK)
            both = jnp.concatenate([q_fwd[:, c], q_bwd[:, c]], axis=1)
            carry = jnp.where(h == core, mine_c[...], part_c[...])
            out = local_ref[pl.ds(at, GR), h * DV : (h + 1) * DV] + nt_dot(both, carry)
            out = out * lax.rsqrt(jnp.mean(out * out, axis=-1, keepdims=True) + EPS) * gain
            u = gate_ref[pl.ds(at, GR), h * DV : (h + 1) * DV].astype(F32)
            hm[pl.ds(at, GR), pl.ds(pl.multiple_of(me * 2 * DV + h * DV, DV), DV)] = (
                out * (u / (1.0 + jnp.exp(-u)))).astype(BF16)

    def three(i, _):
        last(quarter_of(me, i + i // 2))
        return 0

    lax.fori_loop(0, 3, three, 0)

    def piece(slot, r, part):
        return hm.at[
            pl.ds(pl.multiple_of(r * q_rows + part * half, half), half),
            pl.ds(pl.multiple_of(slot * 2 * DV, 2 * DV), 2 * DV)]

    def remote(ref, send, recv, target, dst=None):
        return pltpu.make_async_remote_copy(
            ref, ref if dst is None else dst, send, recv, device_id=target, device_id_type=MESH)

    def wire(slot, quarter, part, send, recv, target):
        return remote(piece(slot, quarter, part), send, recv, target)

    to_right = (((0, 0), (3, 0), (3, 1)), ((2, 0), (2, 1)), ((1, 0), (0, 1)), ((1, 1),))
    to_left = (((0, 1), (1, 1), (1, 0)), ((3, 1), (0, 0)), ((2, 1), (2, 0)), ((3, 0),))

    def own_right(o, p):
        return wire(me, quarter_of(me, o), p, own_rs.at[o * 2 + p], left_in.at[o * 2 + p], right)

    def own_left(o, p):
        return wire(me, quarter_of(me, o), p, own_ls.at[o * 2 + p], right_in.at[o * 2 + p], left)

    def came_left(o, p):
        return wire(ix_l, quarter_of(ix_l, o), p, own_rs.at[o * 2 + p], left_in.at[o * 2 + p], right)

    def came_right(o, p):
        return wire(ix_r, quarter_of(ix_r, o), p, own_ls.at[o * 2 + p], right_in.at[o * 2 + p], left)

    def fwd_right(i):
        return wire(ix_l, quarter_of(ix_r, order[i]), 0, fwd_rs.at[i], opp_l.at[i], right)

    def fwd_left(i):
        return wire(ix_r, quarter_of(ix_l, order[i]), 1, fwd_ls.at[i], opp_r.at[i], left)

    opposite = lax.rem(me + 2, n)

    def came_opp_l(i):
        return wire(opposite, quarter_of(me, order[i]), 0, fwd_rs.at[i], opp_l.at[i], right)

    def came_opp_r(i):
        return wire(opposite, quarter_of(me, order[i]), 1, fwd_ls.at[i], opp_r.at[i], left)

    def send_own(i):
        for k in range(len(to_right[i])):
            own_right(*to_right[i][k]).start()
            own_left(*to_left[i][k]).start()

    seen = set()

    def arrived(side, o, p):
        if (side, o, p) not in seen:
            seen.add((side, o, p))
            (came_left if side == "l" else came_right)(o, p).wait_recv()

    def pump(i):
        arrived("l", (2 + order[i]) % n, 0)
        fwd_right(i).start()
        arrived("r", (n - 2 + order[i]) % n, 1)
        fwd_left(i).start()

    send_own(0)
    last(quarter_of(me, 2))
    g1.far()
    for ja in (-1, 1):
        g1.column(ja)
    g2.far()
    pump(0)
    send_own(1)
    ring.far()
    g1.column(2)
    for ja in (-1, 1):
        g2.column(ja)
    ring.finish()

    dh = d // 2
    to_r_a = remote(s2.at[:, pl.ds(0, dh)], rs_send.at[0], rs_recv.at[0], right, ra)
    to_l_b = remote(s2.at[:, pl.ds(dh, dh)], rs_send.at[1], rs_recv.at[1], left, rb)
    lo, up = pl.ds(0, dh), pl.ds(dh, dh)
    to_r = remote(s1.at[:, up], rs_send.at[2], rs_recv.at[2], right, rl.at[:, up])
    to_l = remote(s3.at[:, lo], rs_send.at[3], rs_recv.at[3], left, rr.at[:, lo])
    to_r_sum = remote(s1.at[:, lo], rs_send.at[4], rs_recv.at[4], right, rl.at[:, lo])
    to_l_sum = remote(s3.at[:, up], rs_send.at[5], rs_recv.at[5], left, rr.at[:, up])

    for i in range(n):
        q = quarter_of(me, order[i])
        at = pl.multiple_of(q * q_rows, q_rows)
        rows = pl.ds(at, q_rows)
        for p in range(2):
            arrived("l", (1 + order[i]) % n, p)
            arrived("r", (n - 1 + order[i]) % n, p)
        came_opp_l(i).wait_recv()
        came_opp_r(i).wait_recv()

        load_stream(i).wait()

        def project(j, total):
            cols = pl.ds(pl.multiple_of(j * 1024, 1024), 1024)
            acc = st[i % 2, :, cols].astype(F32) + nn_dot(hm[rows, :], wo_v[:, cols])
            resid[:, cols] = acc
            return total + jnp.sum(acc * acc, axis=-1, keepdims=True)

        squares = lax.fori_loop(0, d // 1024, project, jnp.zeros((q_rows, 1), F32))
        if i == 0:
            pump(1)
            send_own(2)
            send_own(3)
        if i < n - 2:
            load_stream(i + 2).start()
        if i == 0:
            g2.column(2)
            for ja in PlaneGather.OFFS:
                g1.column_far(ja)
            g1.finish()
        factor = lax.rsqrt(squares / d + EPS)
        normed[...] = (resid[...] * factor * gains_ref[:, DV:]).astype(BF16)

        def gate_up(at, width):
            both = nn_dot(normed[...], w_v[:, pl.ds(pl.multiple_of(at * 2, 256), 2 * width)])
            for b in range(width // 128):
                g = both[:, b * 256 : b * 256 + 128]
                u = both[:, b * 256 + 128 : (b + 1) * 256]
                hidden[:, pl.ds(pl.multiple_of(at + b * 128, 128), 128)] = (
                    g / (1.0 + jnp.exp(-g)) * u).astype(BF16)

        def gate_up_pair(j, _):
            gate_up(j * 256, 256)
            return 0

        lax.fori_loop(0, units // 256, gate_up_pair, 0)
        gate_up(units // 256 * 256, units % 256)
        if i == 0:
            for ja in PlaneGather.OFFS:
                g2.column_far(ja)
            g2.finish()
        if i == 2:
            to_r_a.wait_recv()
            s1[:, :dh] = (s1[:, :dh].astype(F32) + ra[...].astype(F32)).astype(BF16)
            to_r_sum.start()
        target = (s2, s1, s3, resid)[i]

        def down(j, _):
            cols = pl.ds(pl.multiple_of(j * 512, 512), 512)
            part = nt_dot(hidden[...], down_v[cols, :]).astype(BF16)
            if i < n - 1:
                target[:, cols] = part
            else:
                target[:, cols] = target[:, cols] + part.astype(F32)
            return 0

        lax.fori_loop(0, d // 512, down, 0)
        if i == 0:
            pump(2)
            pump(3)
            to_r_a.start()
            to_l_b.start()
        if i == 1:
            to_r.start()
        if i == 2:
            to_l.start()
            to_l_b.wait_recv()
            s3[:, dh:] = (s3[:, dh:].astype(F32) + rb[...].astype(F32)).astype(BF16)
            to_l_sum.start()

    to_r.wait_recv()
    to_l.wait_recv()
    to_r_sum.wait_recv()
    to_l_sum.wait_recv()
    out_ref[...] = (resid[...] + rl[...].astype(F32) + rr[...].astype(F32)).astype(BF16)

    for o in range(n):
        for p in range(2):
            own_right(o, p).wait_send()
            own_left(o, p).wait_send()
    for i in range(n):
        fwd_right(i).wait_send()
        fwd_left(i).wait_send()
    g1.drain()
    g2.drain()
    ring.drain()
    to_r_a.wait_send()
    to_l_b.wait_send()
    to_r.wait_send()
    to_l.wait_send()
    to_r_sum.wait_send()
    to_l_sum.wait_send()


def layer(q, k, v, lg, bias, extra, doc, gate, gain, wo, stream, ff_gain, wg, wu, wd):
    rows, d = stream.shape
    units = wg.shape[1]
    gains = jnp.concatenate([gain, ff_gain]).astype(F32).reshape(1, -1)
    vm = pl.BlockSpec(memory_space=pltpu.VMEM)
    hbm = pl.BlockSpec(memory_space=pl.ANY)
    blocks = rows // BL
    dma = pltpu.SemaphoreType.DMA

    def buf(*shape, dtype=BF16):
        return pltpu.VMEM(shape, dtype)

    return pl.pallas_call(
        layer_kernel,
        out_shape=jax.ShapeDtypeStruct((GR, d), BF16),
        in_specs=[hbm] * 10 + [vm] * 4,
        out_specs=vm,
        scratch_shapes=[
            buf(rows, 2 * DK), buf(rows, 2 * DK), buf(rows, 2 * DV), buf(rows, 2 * DK),
            buf(rows, 2 * DV), buf(rows, 3, dtype=F32),
            buf(*wg.shape), buf(*wu.shape), buf(wg.shape[0], 2 * units), buf(*wd.shape),
            buf(rows, 2 * DK, dtype=F32),
            buf(blocks, 1, 2 * DK, dtype=F32),
            buf(blocks, 1, 2 * DK, dtype=F32),
            buf(blocks * 2, DV, DK, dtype=F32),
            buf(blocks * 2, DV, 2 * DK),
            buf(2, DV, 2 * DK, dtype=F32),
            buf(rows, 2 * DV, dtype=F32),
            buf(2, 2 * DV, DK), buf(2, 8, DK, dtype=F32),
            buf(2 * DV, DK), buf(8, DK, dtype=F32),
            buf(2, DV, DK), buf(8, DK, dtype=F32),
            buf(NCHIP, DV, DK), buf(NCHIP, 8, DK, dtype=F32),
            buf(DV, 2 * DK), buf(DV, 2 * DK), buf(DV, 2 * DK),
            buf(1, 2 * DK, dtype=F32),
            buf(rows, 4 * 2 * DV), buf(2, GR, d), buf(4 * wo.shape[0], d),
            buf(2 * NCHIP * wg.shape[0], 2 * units), buf(2 * NCHIP * wd.shape[0], units),
            buf(GR, d, dtype=F32), buf(GR, d), buf(GR, units),
            buf(GR, d), buf(GR, d), buf(GR, d), buf(GR, d // 2), buf(GR, d // 2), buf(GR, d), buf(GR, d),
            dma((13,)), dma((3,)), dma((3,)),
            dma((NCHIP,)), dma((NCHIP,)), dma((NCHIP,)), dma((NCHIP,)),
            dma((8,)), dma((8,)), dma((4,)), dma((4,)),
            dma((8,)), dma((8,)), dma((4,)), dma((4,)), dma((6,)), dma((6,)),
        ] + plane_sems() + plane_sems() + [dma((k,)) for k in RowGather.SEMS],
        compiler_params=pltpu.CompilerParams(
            collective_id=0, has_side_effects=True, vmem_limit_bytes=67_043_328),
        cost_estimate=pl.CostEstimate(
            flops=29_000_000_000, bytes_accessed=16_000_000, transcendentals=0),
        name="layer",
    )(q, k, v, lg, gate, wo, stream, wg, wu, wd,
      bias.reshape(1, -1), extra.T, doc.reshape(1, -1), gains)


def per_device(
    stream, queries, projected_keys, values, decay_gate_logits, decay_gate_bias, extra_log_decay,
    document_index, output_gate, head_norm_gain, output_weight, feedforward_norm_gain,
    gate_weight, up_weight, down_weight,
):
    return layer(
        queries, projected_keys, values, decay_gate_logits, decay_gate_bias, extra_log_decay,
        document_index, output_gate, head_norm_gain, output_weight, stream,
        feedforward_norm_gain, gate_weight, up_weight, down_weight.T)


def solution(mesh):
    torus = Mesh(mesh.devices.reshape(4, 4, 2, mesh.shape["tp"]), ("sp_0", "sp_1", "sp_2", "tp"))
    placed = (
        P(SP, None), P(SP, "tp"), P(SP, "tp"), P(SP, "tp"), P(SP, "tp"), P("tp"), P(SP, "tp"),
        P(SP), P(SP, "tp"), P(), P("tp", None), P(), P(SP, "tp"), P(SP, "tp"), P("tp", SP),
    )
    return jax.shard_map(
        per_device, mesh=torus, in_specs=placed, out_specs=P(SP_TP, None), check_vma=False
    )
```

```python
import functools
import jax
import jax.numpy as jnp
from jax import lax
from jax.experimental import pallas as pl
from jax.experimental.pallas import tpu as pltpu
from jax.sharding import Mesh
from jax.sharding import PartitionSpec as P

SP = ("sp_0", "sp_1", "sp_2")
SP_TP = ("sp_0", "sp_1", "sp_2", "tp")
MESH = pl.DeviceIdType.MESH
F32 = jnp.float32
BF16 = jnp.bfloat16
TAU = 16.0
EPS = 1e-06
BL = 64
GR = 256
DK = 128
DV = 256
NZ, NY = 4, 4
NCHIP = NZ * NY


def nt_dot(a, b):
    return lax.dot_general(a, b, (((1,), (1,)), ((), ())), preferred_element_type=F32)


def tn_dot(a, b):
    return lax.dot_general(a, b, (((0,), (0,)), ((), ())), preferred_element_type=F32)


def nn_dot(a, b):
    return lax.dot_general(a, b, (((1,), (0,)), ((), ())), preferred_element_type=F32)


def remote_copy(src, dst, send, recv, target):
    return pltpu.make_async_remote_copy(
        src, dst, send, recv, device_id=target, device_id_type=MESH)


class PlaneGather:
    SEMS = (40, 40, 32, 32, 1)

    def __init__(self, src, dst, sems):
        self.src, self.dst = src, dst
        self.send, self.recv, self.core_send, self.core_recv, self.local = sems
        self.at = {"z": lax.axis_index("sp_0"), "y": lax.axis_index("sp_1")}
        self.core, self.x = lax.axis_index("sp_2"), lax.axis_index("tp")
        self.rows = src.shape[0] // 2

    def shifted(self, moves):
        at = dict(self.at)
        for axis, k in moves:
            at[axis] = lax.rem(at[axis] + (k + 4), 4)
        return at["z"], at["y"]

    def chip_at(self, axis, k):
        z, y = self.shifted([(axis, k)])
        return z, y, self.core, self.x

    def piece(self, hf, ja, jb, sub=None):
        a, b = ("y", "z") if hf == 0 else ("z", "y")
        z, y = self.shifted([(a, ja), (b, jb)])
        row = ((z * NY + y) * 2 + self.core) * (2 * self.rows) + hf * self.rows
        size = self.rows
        if sub is not None:
            size = size // 2
            row = row + sub * size
        return self.dst.at[pl.ds(pl.multiple_of(row, 16), size)]

    def axis(self, hf, stage):
        return ("y", "z")[(hf + stage) % 2]

    OFFS = (0, -1, 1, 2)

    def hop(self, hf, stage, ja, way, forward):
        axis = self.axis(hf, stage)
        k = hf * 20 + (0 if stage == 0 else 4 + 4 * self.OFFS.index(ja)) + (0 if way > 0 else 1)
        k = k + (2 if forward else 0)
        target = self.chip_at(axis, way)
        if forward:
            sub = 0 if way > 0 else 1
            ref = self.piece(hf, -way, 0, sub) if stage == 0 else self.piece(hf, ja, -way, sub)
            src = ref
        else:
            ref = self.piece(hf, 0, 0) if stage == 0 else self.piece(hf, ja, 0)
            own = stage == 0 or ja == 0
            src = self.src.at[pl.ds(hf * self.rows, self.rows)] if own else ref
        return remote_copy(src, ref, self.send.at[k], self.recv.at[k], target)

    def landing(self, hf, stage, ja, way, forward):
        axis = self.axis(hf, stage)
        k = hf * 20 + (0 if stage == 0 else 4 + 4 * self.OFFS.index(ja)) + (0 if way > 0 else 1)
        k = k + (2 if forward else 0)
        back = 2 if forward else -way
        sub = (0 if way > 0 else 1) if forward else None
        ref = self.piece(hf, back, 0, sub) if stage == 0 else self.piece(hf, ja, back, sub)
        return remote_copy(ref, ref, self.send.at[k], self.recv.at[k], self.chip_at(axis, way))

    def hand(self, hf, ja, jb):
        p = hf * 16 + self.OFFS.index(ja) * 4 + self.OFFS.index(jb)
        ref = self.piece(hf, ja, jb)
        src = self.src.at[pl.ds(hf * self.rows, self.rows)] if ja == 0 and jb == 0 else ref
        partner = (self.at["z"], self.at["y"], 1 - self.core, self.x)
        return remote_copy(src, ref, self.core_send.at[p], self.core_recv.at[p], partner)

    def handed(self, hf, ja, jb):
        p = hf * 16 + self.OFFS.index(ja) * 4 + self.OFFS.index(jb)
        a, b = ("y", "z") if hf == 0 else ("z", "y")
        z, y = self.shifted([(a, ja), (b, jb)])
        row = ((z * NY + y) * 2 + 1 - self.core) * (2 * self.rows) + hf * self.rows
        ref = self.dst.at[pl.ds(pl.multiple_of(row, 16), self.rows)]
        partner = (self.at["z"], self.at["y"], 1 - self.core, self.x)
        return remote_copy(ref, ref, self.core_send.at[p], self.core_recv.at[p], partner)

    def keep(self):
        row = ((self.at["z"] * NY + self.at["y"]) * 2 + self.core) * (2 * self.rows)
        return pltpu.make_async_copy(
            self.src, self.dst.at[pl.ds(pl.multiple_of(row, 16), 2 * self.rows)], self.local.at[0])

    def start(self):
        for stage in range(2):
            for hf in range(2):
                for way in (1, -1):
                    self.hop(hf, stage, 0, way, False).start()
        for hf in range(2):
            self.hand(hf, 0, 0).start()
        self.keep().start()

    def second(self, hf, ja):
        for way in (1, -1):
            self.hop(hf, 1, ja, way, False).start()
        self.hand(hf, ja, 0).start()

    def near(self):
        for way in (1, -1):
            for hf in range(2):
                self.landing(hf, 0, 0, way, False).wait_recv()
                self.hop(hf, 0, 0, way, True).start()

    def near_second(self, hf):
        for way in (1, -1):
            self.second(hf, -way)

    def far(self):
        for hf in range(2):
            for way in (1, -1):
                self.landing(hf, 0, 0, way, True).wait_recv()
            self.second(hf, 2)

    def column(self, ja):
        for way in (1, -1):
            for hf in range(2):
                self.landing(hf, 1, ja, way, False).wait_recv()
                self.hop(hf, 1, ja, way, True).start()
                self.hand(hf, ja, -way).start()

    def column_far(self, ja):
        for hf in range(2):
            for way in (1, -1):
                self.landing(hf, 1, ja, way, True).wait_recv()
            self.hand(hf, ja, 2).start()

    def finish(self):
        self.keep().wait()
        for hf in range(2):
            for ja in self.OFFS:
                for jb in self.OFFS:
                    self.handed(hf, ja, jb).wait_recv()

    def drain(self):
        for hf in range(2):
            for way in (1, -1):
                for forward in (False, True):
                    self.hop(hf, 0, 0, way, forward).wait_send()
                    for ja in self.OFFS:
                        self.hop(hf, 1, ja, way, forward).wait_send()
            for ja in self.OFFS:
                for jb in self.OFFS:
                    self.hand(hf, ja, jb).wait_send()


class RowGather:
    SEMS = (6, 6, 3, 3)

    def __init__(self, rows, dst, sems):
        self.dst = dst
        self.send, self.recv, self.core_send, self.core_recv = sems
        self.z, self.y = lax.axis_index("sp_0"), lax.axis_index("sp_1")
        self.core, self.x = lax.axis_index("sp_2"), lax.axis_index("tp")
        self.rows = rows

    def piece(self, k, core, sub=None):
        size = self.rows // 2
        row = lax.rem(self.x + (k + 4), 4) * self.rows + core * size
        if sub is not None:
            size = size // 2
            row = row + sub * size
        return self.dst.at[pl.ds(pl.multiple_of(row, 16), size)]

    def side(self, way):
        return (self.z, self.y, self.core, lax.rem(self.x + (way + 4), 4))

    def copy(self, ref, k, way):
        return remote_copy(ref, ref, self.send.at[k], self.recv.at[k], self.side(way))

    def key(self, way, part):
        return (0 if way > 0 else 1) + 2 * part

    def hop(self, way, part):
        first = 0 if way > 0 else 1
        if part == 2:
            ref = self.piece(-way, self.core, first)
        else:
            ref = self.piece(0, self.core, first if part == 0 else 1 - first)
        return self.copy(ref, self.key(way, part), way)

    def landing(self, way, part):
        first = 0 if way > 0 else 1
        if part == 2:
            ref = self.piece(2, self.core, first)
        else:
            ref = self.piece(-way, self.core, first if part == 0 else 1 - first)
        return self.copy(ref, self.key(way, part), way)

    def hand(self, i, arriving=False):
        k = (-1, 1, 2)[i]
        ref = self.piece(k, 1 - self.core if arriving else self.core)
        return remote_copy(
            ref, ref, self.core_send.at[i], self.core_recv.at[i], (self.z, self.y, 1 - self.core, self.x))

    def start(self):
        for part in range(2):
            for way in (1, -1):
                self.hop(way, part).start()

    def near(self):
        for way in (1, -1):
            self.landing(way, 0).wait_recv()
            self.hop(way, 2).start()

    def near_hand(self):
        for i, way in enumerate((1, -1)):
            self.landing(way, 1).wait_recv()
            self.hand(i).start()

    def far(self):
        for way in (1, -1):
            self.landing(way, 2).wait_recv()
        self.hand(2).start()

    def finish(self):
        for i in range(3):
            self.hand(i, True).wait_recv()

    def drain(self):
        for way in (1, -1):
            for part in range(3):
                self.hop(way, part).wait_send()
        for i in range(3):
            self.hand(i).wait_send()


def plane_sems():
    return [pltpu.SemaphoreType.DMA((k,)) for k in PlaneGather.SEMS]


def layer_kernel(
    q_in, k_in, v_in, lg_in, gate_in, wo_in, stream_in, wg_in, wu_in, wd_in,
    bias_ref, extra_ref, doc_ref, gains_ref,
    out_ref,
    q_ref, k_ref, v_ref, lg_ref, gate_ref, aux_ref, wg_ref, wu_ref, shard_ref, wd_ref,
    cum_ref, blk_ref, off_ref, states_ref, before_ref, run_ref, local_ref,
    own_t, own_e, part_t, part_e, chip_t, chip_e, ry_t, ry_e, row_t, row_e, rz_t, rz_e, mine_c, send_c, part_c, sum_ref,
    hm, st, wo_v, w_v, down_v, resid, normed, hidden, s2, s1, s3, ra, rb, rl, rr,
    local_sem, core_send, core_recv, t_send, t_recv, e_send, e_recv,
    own_rs, own_ls, fwd_rs, fwd_ls, left_in, right_in, opp_l, opp_r, rs_send, rs_recv,
    *gather_sems,
):
    rows = q_ref.shape[0]
    blocks = rows // BL
    groups = rows // GR
    per = GR // BL
    z, y = lax.axis_index("sp_0"), lax.axis_index("sp_1")
    core, me = lax.axis_index("sp_2"), lax.axis_index("tp")
    scale = DK ** (-0.5)
    n = 4
    q_rows = GR
    half = q_rows // 2
    d = out_ref.shape[1]
    units = hidden.shape[1]
    ix_r, ix_l = lax.rem(me + 1, n), lax.rem(me + n - 1, n)
    right, left = (z, y, core, ix_r), (z, y, core, ix_l)
    partner = (z, y, 1 - core, me)
    order = (2, 1, 3, 0)

    def quarter_of(owner, offset):
        return lax.rem(owner + offset, n)

    def along_y(k):
        return (z, lax.rem(y + k, NY), core, me)

    def along_z(k):
        return (lax.rem(z + k, NZ), y, core, me)

    wo_own = wo_in.shape[0]
    loads = {
        name: pltpu.make_async_copy(src, dst, local_sem.at[i])
        for i, (name, src, dst) in enumerate((
            ("wg", wg_in, wg_ref), ("wu", wu_in, wu_ref), ("wd", wd_in, wd_ref),
            ("wo", wo_in, wo_v.at[pl.ds(pl.multiple_of(me * wo_own, wo_own), wo_own)]),
            ("lg", lg_in, lg_ref), ("k", k_in, k_ref), ("v", v_in, v_ref), ("q", q_in, q_ref),
            ("gate", gate_in, gate_ref),
        ))
    }
    for copy in loads.values():
        copy.start()

    def load_stream(i):
        at = pl.multiple_of(quarter_of(me, order[i]) * q_rows, q_rows)
        return pltpu.make_async_copy(
            stream_in.at[pl.ds(at, q_rows)], st.at[i % 2], local_sem.at[9 + i])

    load_stream(0).start()
    load_stream(1).start()

    rz_t[pl.ds(z, 1)] = jnp.zeros((1, DV, DK), BF16)

    barrier = pltpu.get_barrier_semaphore()
    pl.semaphore_signal(barrier, inc=1, device_id=partner, device_id_type=MESH)
    pl.semaphore_signal(barrier, inc=1, device_id=right, device_id_type=MESH)
    pl.semaphore_signal(barrier, inc=1, device_id=left, device_id_type=MESH)
    for k in range(1, NY):
        pl.semaphore_signal(barrier, inc=1, device_id=along_y(k), device_id_type=MESH)
        pl.semaphore_signal(barrier, inc=1, device_id=along_z(k), device_id_type=MESH)

    loads["wg"].wait()
    loads["wu"].wait()
    for j in range(units // 128):
        shard_ref[:, j * 256 : j * 256 + 128] = wg_ref[:, j * 128 : (j + 1) * 128]
        shard_ref[:, j * 256 + 128 : (j + 1) * 256] = wu_ref[:, j * 128 : (j + 1) * 128]
    loads["wd"].wait()
    loads["wo"].wait()

    pl.semaphore_wait(barrier, 9)
    g1 = PlaneGather(shard_ref, w_v, gather_sems[:5])
    g2 = PlaneGather(wd_ref, down_v, gather_sems[5:10])
    ring = RowGather(wo_own, wo_v, gather_sems[10:])
    ring.start()
    g1.start()

    ri = lax.broadcasted_iota(jnp.int32, (GR, GR), 0)
    ci = lax.broadcasted_iota(jnp.int32, (GR, GR), 1)

    def columns(g, _):
        at = pl.multiple_of(g * GR, GR)
        for j in range(3):
            lanes = pl.ds(pl.multiple_of(g * GR, GR), GR)
            row = doc_ref[:, lanes].astype(F32) if j == 2 else extra_ref[j : j + 1, lanes]
            col = jnp.sum(jnp.where(ri == ci, row, 0.0), axis=1, keepdims=True)
            aux_ref[pl.ds(at, GR), j : j + 1] = col
        return 0

    lax.fori_loop(0, groups, columns, 0)
    loads["lg"].wait()
    loads["k"].wait()
    loads["v"].wait()
    run_ref[...] = jnp.zeros_like(run_ref)

    def doc_at(r):
        return aux_ref[pl.ds(r, 1), 2:3]

    def first(g, base):
        at = pl.multiple_of(g * GR, GR)
        same_block = (ri & (GR - BL)) == (ci & (GR - BL))
        tri = jnp.where(same_block & (ci <= ri), 1.0, 0.0).astype(BF16)
        logits = lg_ref[pl.ds(at, GR), :].astype(F32) + bias_ref[...]
        ld = (jnp.minimum(logits, 0.0) - jnp.log1p(jnp.exp(-jnp.abs(logits)))) / TAU
        extra0 = jnp.broadcast_to(aux_ref[pl.ds(at, GR), 0:1], (GR, DK))
        extra1 = jnp.broadcast_to(aux_ref[pl.ds(at, GR), 1:2], (GR, DK))
        ld = ld + jnp.concatenate([extra0, extra1], axis=1)
        hi = ld.astype(BF16)
        rest = ld - hi.astype(F32)
        mid = rest.astype(BF16)
        low = (rest - mid.astype(F32)).astype(BF16)
        cum = nn_dot(tri, hi) + nn_dot(tri, mid) + nn_dot(tri, low)
        cum_ref[pl.ds(at, GR), :] = cum
        cum3 = cum.reshape(per, BL, 2 * DK)
        ends = cum3[:, BL - 1 : BL, :]
        off = base
        for b in range(per):
            off_ref[pl.ds(g * per + b, 1)] = off[None]
            blk_ref[pl.ds(g * per + b, 1)] = ends[b : b + 1]
            off = off + ends[b]
        doc = aux_ref[pl.ds(at, GR), 2:3].reshape(per, BL, 1)
        tail_mask = jnp.where(doc == doc[:, BL - 1 : BL], 1.0, 0.0)
        head_mask = jnp.where(doc == doc[:, 0:1], 1.0, 0.0)
        kf = k_ref[pl.ds(at, GR), :].astype(F32).reshape(per, BL, 2 * DK)
        tail = (kf * jnp.exp(ends - cum3) * tail_mask).astype(BF16)
        head = (kf * jnp.exp(cum3) * head_mask).astype(BF16)
        for b in range(per):
            start = at + b * BL
            keep = jnp.where(doc_at(jnp.maximum(start - 1, 0)) == doc_at(start + BL - 1), 1.0, 0.0)
            decay = jnp.exp(ends[b]) * keep
            for h in range(2):
                c = slice(h * DK, (h + 1) * DK)
                keys = jnp.concatenate([tail[b][:, c], head[b][:, c]], axis=1)
                vals = v_ref[pl.ds(pl.multiple_of(start, BL), BL), h * DV : (h + 1) * DV]
                both = tn_dot(vals, keys)
                slot = (g * per + b) * 2 + h
                states_ref[pl.ds(slot, 1)] = both[None, :, DK:]
                fw = run_ref[h, :, :DK]
                before_ref[pl.ds(slot, 1), :, :DK] = fw.astype(BF16)[None]
                run_ref[h, :, :DK] = fw * decay[:, c] + both[:, :DK]
        return off

    total = lax.fori_loop(0, groups, first, jnp.zeros((1, 2 * DK), F32))
    sum_ref[...] = total

    def step(b, _):
        r = blocks - 1 - b
        hi = jnp.minimum(r * BL + BL, rows - 1)
        keep = jnp.where(doc_at(hi) == doc_at(r * BL), 1.0, 0.0)
        decay = jnp.exp(blk_ref[pl.ds(r, 1)][0]) * keep
        for h in range(2):
            bw = run_ref[h, :, DK:]
            before_ref[pl.ds(r * 2 + h, 1), :, DK:] = bw.astype(BF16)[None]
            run_ref[h, :, DK:] = bw * decay[:, h * DK : (h + 1) * DK] + states_ref[r * 2 + h]
        return 0

    lax.fori_loop(0, blocks, step, 0)
    first_doc = jnp.broadcast_to(doc_at(0), (1, DK))
    last_doc = jnp.broadcast_to(doc_at(rows - 1), (1, DK))
    for h in range(2):
        own_t[h, :DV] = run_ref[h, :, :DK].astype(BF16)
        own_t[h, DV:] = run_ref[h, :, DK:].astype(BF16)
        own_e[h, 0:1] = total[:, h * DK : (h + 1) * DK]
        own_e[h, 1:2] = first_doc
        own_e[h, 2:3] = last_doc
        own_e[h, 3:8] = jnp.zeros((5, DK), F32)

    g1.near()
    swap_t = pltpu.make_async_remote_copy(
        own_t.at[1 - core], part_t, core_send.at[0], core_recv.at[0],
        device_id=partner, device_id_type=MESH)
    swap_e = pltpu.make_async_remote_copy(
        own_e.at[1 - core], part_e, core_send.at[1], core_recv.at[1],
        device_id=partner, device_id_type=MESH)
    swap_t.start()
    swap_e.start()
    swap_t.wait()
    swap_e.wait()
    is0 = core == 0
    mine_e = own_e[pl.ds(core, 1)][0]
    other_e = part_e[...]
    e0 = jnp.where(is0, mine_e, other_e)
    e1 = jnp.where(is0, other_e, mine_e)
    mine_t = own_t[pl.ds(core, 1)][0].astype(F32)
    other_t = part_t[...].astype(F32)
    t0 = jnp.where(is0, mine_t, other_t)
    t1 = jnp.where(is0, other_t, mine_t)
    through1 = jnp.exp(e1[0:1]) * jnp.where(e0[2:3] == e1[2:3], 1.0, 0.0)
    through0 = jnp.exp(e0[0:1]) * jnp.where(e1[1:2] == e0[1:2], 1.0, 0.0)
    chip_t[0] = (t1[:DV] + through1 * t0[:DV]).astype(BF16)
    chip_t[1] = (t0[DV:] + through0 * t1[DV:]).astype(BF16)
    chip_row = jnp.concatenate(
        [e0[0:1] + e1[0:1], e0[1:2], e1[2:3], jnp.zeros((5, DK), F32)], axis=0)
    chip_e[...] = chip_row
    ry_e[pl.ds(y, 1)] = chip_row[None]
    ry_t[pl.ds(y, 1)] = chip_t[...][None]

    y_sends = []
    for k in range(1, NY):
        y_sends.append(remote_copy(chip_e, ry_e.at[y], e_send.at[k], e_recv.at[k], along_y(k)))
        y_sends.append(remote_copy(chip_t, ry_t.at[y], t_send.at[k], t_recv.at[k], along_y(k)))
    for s in y_sends:
        s.start()
    g1.near_second(0)
    g2.start()
    loads["q"].wait()

    def inside(g, _):
        at = pl.multiple_of(g * GR, GR)
        same_block = (ri & (GR - BL)) == (ci & (GR - BL))
        doc = aux_ref[pl.ds(at, GR), 2:3]
        same = same_block & (doc == doc_ref[:, pl.ds(at, GR)].astype(F32))
        below = same & (ci <= ri)
        above = same & (ci >= ri)
        cum3 = cum_ref[pl.ds(at, GR), :].reshape(per, BL, 2 * DK)
        middle = cum3[:, BL // 2 - 1 : BL // 2]
        ends = cum3[:, BL - 1 : BL]
        rising = jnp.exp(cum3 - middle)
        falling = jnp.exp(middle - cum3)
        qf = q_ref[pl.ds(at, GR), :].astype(F32).reshape(per, BL, 2 * DK) * scale
        kf = k_ref[pl.ds(at, GR), :].astype(F32).reshape(per, BL, 2 * DK)
        q_rise = (qf * rising).astype(BF16).reshape(GR, 2 * DK)
        q_fall = (qf * falling).astype(BF16).reshape(GR, 2 * DK)
        k_rise = (kf * rising).astype(BF16).reshape(GR, 2 * DK)
        k_fall = (kf * falling).astype(BF16).reshape(GR, 2 * DK)
        q_fwd = qf * jnp.exp(cum3)
        q_bwd = qf * jnp.exp(ends - cum3)
        for h in range(2):
            c = slice(h * DK, (h + 1) * DK)
            fw = nt_dot(q_rise[:, c], k_fall[:, c])
            bw = nt_dot(q_fall[:, c], k_rise[:, c])
            scores = jnp.where(below, fw, 0.0) + jnp.where(above, bw, 0.0)
            vals = v_ref[pl.ds(at, GR), h * DV : (h + 1) * DV]
            local_ref[pl.ds(at, GR), h * DV : (h + 1) * DV] = nn_dot(scores.astype(BF16), vals)
        for b in range(per):
            start = at + b * BL
            prev = doc_at(jnp.maximum(start - 1, 0))
            following = doc_at(jnp.minimum(start + BL, rows - 1))
            rows_doc = doc[b * BL : (b + 1) * BL]
            hit_f = jnp.where(rows_doc == prev, 1.0, 0.0)
            hit_b = jnp.where(rows_doc == following, 1.0, 0.0)
            for h in range(2):
                c = slice(h * DK, (h + 1) * DK)
                both = jnp.concatenate([q_fwd[b][:, c] * hit_f, q_bwd[b][:, c] * hit_b], axis=1)
                here = pl.ds(pl.multiple_of(start, BL), BL)
                local_ref[here, h * DV : (h + 1) * DV] += nt_dot(
                    both.astype(BF16), before_ref[(g * per + b) * 2 + h])
        return 0

    lax.fori_loop(0, groups // 2, inside, 0)
    g1.column(0)
    lax.fori_loop(groups // 2, groups, inside, 0)

    ring.near()
    for s in y_sends:
        s.wait()
    run_ref[0] = jnp.zeros_like(run_ref[0])

    def earlier(states, table):
        def body(j, _):
            e = table[j]
            p = table[jnp.maximum(j - 1, 0)]
            keep = jnp.exp(e[0:1]) * jnp.where(e[2:3] == p[2:3], 1.0, 0.0)
            run_ref[0, :, :DK] = states(j, 0).astype(F32) + run_ref[0, :, :DK] * keep
            return 0
        return body

    def later(states, table):
        def body(i, _):
            j = NY - 1 - i
            e = table[j]
            p = table[jnp.minimum(j + 1, NY - 1)]
            keep = jnp.exp(e[0:1]) * jnp.where(e[1:2] == p[1:2], 1.0, 0.0)
            run_ref[0, :, DK:] = states(j, 1).astype(F32) + run_ref[0, :, DK:] * keep
            return 0
        return body

    def row_state(j, way):
        return ry_t[j, way]

    def column_state(j, way):
        return rz_t[j]

    lax.fori_loop(0, y, earlier(row_state, ry_e), 0)
    lax.fori_loop(0, NY - 1 - y, later(row_state, ry_e), 0)
    run_ref[1] = run_ref[0]
    lax.fori_loop(y, NY, earlier(row_state, ry_e), 0)
    lax.fori_loop(NY - 1 - y, NY, later(row_state, ry_e), 0)
    row_t[0] = run_ref[0, :, :DK].astype(BF16)
    row_t[1] = run_ref[0, :, DK:].astype(BF16)
    in_row = [ry_e[j] for j in range(NY)]
    row_sum = in_row[0][0:1] + in_row[1][0:1] + in_row[2][0:1] + in_row[3][0:1]
    sum_before = jnp.zeros((1, DK), F32)
    sum_after = jnp.zeros((1, DK), F32)
    for j in range(NY):
        sum_before = sum_before + jnp.where(j < y, in_row[j][0:1], 0.0)
        sum_after = sum_after + jnp.where(j > y, in_row[j][0:1], 0.0)
    last_before = ry_e[jnp.maximum(y - 1, 0)][2:3]
    first_after = ry_e[jnp.minimum(y + 1, NY - 1)][1:2]
    row_row = jnp.concatenate(
        [row_sum, in_row[0][1:2], in_row[NY - 1][2:3], jnp.zeros((5, DK), F32)], axis=0)
    row_e[...] = row_row
    rz_e[pl.ds(z, 1)] = row_row[None]
    z_sends = []
    for k in range(1, NZ):
        back = jnp.where(lax.rem(z + k, NZ) > z, 0, 1)
        z_sends.append(
            remote_copy(row_e, rz_e.at[z], e_send.at[4 + k], e_recv.at[4 + k], along_z(k)))
        z_sends.append(
            remote_copy(row_t.at[back], rz_t.at[z], t_send.at[4 + k], t_recv.at[4 + k], along_z(k)))
    for s in z_sends:
        s.start()
    g1.near_second(1)
    g1.far()
    for s in z_sends:
        s.wait()
    g2.near()
    g2.near_second(0)
    g2.near_second(1)

    run_ref[0] = jnp.zeros_like(run_ref[0])
    lax.fori_loop(0, z, earlier(column_state, rz_e), 0)
    lax.fori_loop(0, NZ - 1 - z, later(column_state, rz_e), 0)
    prev_last = jnp.where(z > 0, rz_e[jnp.maximum(z - 1, 0)][2:3], -1.0)
    next_first = jnp.where(z < NZ - 1, rz_e[jnp.minimum(z + 1, NZ - 1)][1:2], -1.0)
    pass_f = jnp.exp(sum_before) * jnp.where(
        y == 0, 1.0, jnp.where(prev_last == last_before, 1.0, 0.0))
    pass_b = jnp.exp(sum_after) * jnp.where(
        y == NY - 1, 1.0, jnp.where(next_first == first_after, 1.0, 0.0))
    cf = run_ref[1, :, :DK] + pass_f * run_ref[0, :, :DK]
    cb = run_ref[1, :, DK:] + pass_b * run_ref[0, :, DK:]
    before_doc = jnp.where(y > 0, last_before, prev_last)
    after_doc = jnp.where(y < NY - 1, first_after, next_first)
    pass0 = jnp.exp(e0[0:1]) * jnp.where(before_doc == e0[2:3], 1.0, 0.0)
    pass1 = jnp.exp(e1[0:1]) * jnp.where(after_doc == e1[1:2], 1.0, 0.0)
    mine_t = own_t[pl.ds(core, 1)][0].astype(F32)
    other_t = part_t[...].astype(F32)
    t0f = jnp.where(is0, mine_t[:DV], other_t[:DV])
    t1b = jnp.where(is0, other_t[DV:], mine_t[DV:])
    c0 = jnp.concatenate([cf, t1b + pass1 * cb], axis=1)
    c1 = jnp.concatenate([t0f + pass0 * cf, cb], axis=1)
    mine_c[...] = jnp.where(is0, c0, c1).astype(BF16)
    send_c[...] = jnp.where(is0, c1, c0).astype(BF16)
    swap_c = pltpu.make_async_remote_copy(
        send_c, part_c, core_send.at[2], core_recv.at[2],
        device_id=partner, device_id_type=MESH)
    swap_c.start()
    ring.near_hand()
    enter_f = jnp.where(is0, before_doc, e0[2:3])[:, 0:1]
    enter_b = jnp.where(is0, e1[1:2], after_doc)[:, 0:1]
    swap_c.wait()

    loads["gate"].wait()

    def last(g):
        at = pl.multiple_of(g * GR, GR)
        doc = aux_ref[pl.ds(at, GR), 2:3]
        hit_f = jnp.where(doc == enter_f, 1.0, 0.0)
        hit_b = jnp.where(doc == enter_b, 1.0, 0.0)
        glob = cum_ref[pl.ds(at, GR), :].reshape(per, BL, 2 * DK) + off_ref[pl.ds(g * per, per)]
        glob = glob.reshape(GR, 2 * DK)
        qf = q_ref[pl.ds(at, GR), :].astype(F32) * scale
        q_fwd = (qf * jnp.exp(glob) * hit_f).astype(BF16)
        q_bwd = (qf * jnp.exp(sum_ref[...] - glob) * hit_b).astype(BF16)
        gain = gains_ref[:, :DV]
        for h in range(2):
            c = slice(h * DK, (h + 1) * DK)
            both = jnp.concatenate([q_fwd[:, c], q_bwd[:, c]], axis=1)
            carry = jnp.where(h == core, mine_c[...], part_c[...])
            out = local_ref[pl.ds(at, GR), h * DV : (h + 1) * DV] + nt_dot(both, carry)
            out = out * lax.rsqrt(jnp.mean(out * out, axis=-1, keepdims=True) + EPS) * gain
            u = gate_ref[pl.ds(at, GR), h * DV : (h + 1) * DV].astype(F32)
            hm[pl.ds(at, GR), pl.ds(pl.multiple_of(me * 2 * DV + h * DV, DV), DV)] = (
                out * (u / (1.0 + jnp.exp(-u)))).astype(BF16)

    def three(i, _):
        last(quarter_of(me, i + i // 2))
        return 0

    lax.fori_loop(0, 3, three, 0)

    def piece(slot, r, part):
        return hm.at[
            pl.ds(pl.multiple_of(r * q_rows + part * half, half), half),
            pl.ds(pl.multiple_of(slot * 2 * DV, 2 * DV), 2 * DV)]

    def remote(ref, send, recv, target, dst=None):
        return pltpu.make_async_remote_copy(
            ref, ref if dst is None else dst, send, recv, device_id=target, device_id_type=MESH)

    def wire(slot, quarter, part, send, recv, target):
        return remote(piece(slot, quarter, part), send, recv, target)

    to_right = (((0, 0), (3, 0), (3, 1)), ((2, 0), (2, 1)), ((1, 0), (0, 1)), ((1, 1),))
    to_left = (((0, 1), (1, 1), (1, 0)), ((3, 1), (0, 0)), ((2, 1), (2, 0)), ((3, 0),))

    def own_right(o, p):
        return wire(me, quarter_of(me, o), p, own_rs.at[o * 2 + p], left_in.at[o * 2 + p], right)

    def own_left(o, p):
        return wire(me, quarter_of(me, o), p, own_ls.at[o * 2 + p], right_in.at[o * 2 + p], left)

    def came_left(o, p):
        return wire(ix_l, quarter_of(ix_l, o), p, own_rs.at[o * 2 + p], left_in.at[o * 2 + p], right)

    def came_right(o, p):
        return wire(ix_r, quarter_of(ix_r, o), p, own_ls.at[o * 2 + p], right_in.at[o * 2 + p], left)

    def fwd_right(i):
        return wire(ix_l, quarter_of(ix_r, order[i]), 0, fwd_rs.at[i], opp_l.at[i], right)

    def fwd_left(i):
        return wire(ix_r, quarter_of(ix_l, order[i]), 1, fwd_ls.at[i], opp_r.at[i], left)

    opposite = lax.rem(me + 2, n)

    def came_opp_l(i):
        return wire(opposite, quarter_of(me, order[i]), 0, fwd_rs.at[i], opp_l.at[i], right)

    def came_opp_r(i):
        return wire(opposite, quarter_of(me, order[i]), 1, fwd_ls.at[i], opp_r.at[i], left)

    def send_own(i):
        for k in range(len(to_right[i])):
            own_right(*to_right[i][k]).start()
            own_left(*to_left[i][k]).start()

    seen = set()

    def arrived(side, o, p):
        if (side, o, p) not in seen:
            seen.add((side, o, p))
            (came_left if side == "l" else came_right)(o, p).wait_recv()

    def pump(i):
        arrived("l", (2 + order[i]) % n, 0)
        fwd_right(i).start()
        arrived("r", (n - 2 + order[i]) % n, 1)
        fwd_left(i).start()

    send_own(0)
    last(quarter_of(me, 2))
    for ja in (-1, 1):
        g1.column(ja)
    g2.column(0)
    ring.far()
    pump(0)
    send_own(1)
    g1.column(2)
    g2.far()
    send_own(2)
    for ja in (-1, 1):
        g2.column(ja)
    ring.finish()

    dh = d // 2
    to_r_a = remote(s2.at[:, pl.ds(0, dh)], rs_send.at[0], rs_recv.at[0], right, ra)
    to_l_b = remote(s2.at[:, pl.ds(dh, dh)], rs_send.at[1], rs_recv.at[1], left, rb)
    lo, up = pl.ds(0, dh), pl.ds(dh, dh)
    to_r = remote(s1.at[:, up], rs_send.at[2], rs_recv.at[2], right, rl.at[:, up])
    to_l = remote(s3.at[:, lo], rs_send.at[3], rs_recv.at[3], left, rr.at[:, lo])
    to_r_sum = remote(s1.at[:, lo], rs_send.at[4], rs_recv.at[4], right, rl.at[:, lo])
    to_l_sum = remote(s3.at[:, up], rs_send.at[5], rs_recv.at[5], left, rr.at[:, up])

    def prepare(i):
        at = pl.multiple_of(quarter_of(me, order[i]) * q_rows, q_rows)
        rows = pl.ds(at, q_rows)
        for p in range(2):
            arrived("l", (1 + order[i]) % n, p)
            arrived("r", (n - 1 + order[i]) % n, p)
        came_opp_l(i).wait_recv()
        came_opp_r(i).wait_recv()
        load_stream(i).wait()

        def project(j, total):
            cols = pl.ds(pl.multiple_of(j * 1024, 1024), 1024)
            acc = st[i % 2, :, cols].astype(F32) + nn_dot(hm[rows, :], wo_v[:, cols])
            resid[:, cols] = acc
            return total + jnp.sum(acc * acc, axis=-1, keepdims=True)

        squares = lax.fori_loop(0, d // 1024, project, jnp.zeros((q_rows, 1), F32))
        if i < n - 2:
            load_stream(i + 2).start()
        factor = lax.rsqrt(squares / d + EPS)
        normed[...] = (resid[...] * factor * gains_ref[:, DV:]).astype(BF16)

    prepare(0)
    pump(1)
    send_own(3)
    g2.column(2)
    for i in range(n):
        if i == 0:
            for ja in PlaneGather.OFFS:
                g1.column_far(ja)
            g1.finish()
        else:
            prepare(i)

        def gate_up(at, width):
            both = nn_dot(normed[...], w_v[:, pl.ds(pl.multiple_of(at * 2, 256), 2 * width)])
            for b in range(width // 128):
                g = both[:, b * 256 : b * 256 + 128]
                u = both[:, b * 256 + 128 : (b + 1) * 256]
                hidden[:, pl.ds(pl.multiple_of(at + b * 128, 128), 128)] = (
                    g / (1.0 + jnp.exp(-g)) * u).astype(BF16)

        def gate_up_pair(j, _):
            gate_up(j * 256, 256)
            return 0

        lax.fori_loop(0, units // 256, gate_up_pair, 0)
        gate_up(units // 256 * 256, units % 256)
        if i == 0:
            for ja in PlaneGather.OFFS:
                g2.column_far(ja)
            g2.finish()
        if i == 2:
            to_r_a.wait_recv()
            s1[:, :dh] = (s1[:, :dh].astype(F32) + ra[...].astype(F32)).astype(BF16)
            to_r_sum.start()
        target = (s2, s1, s3, resid)[i]

        def down(j, _):
            cols = pl.ds(pl.multiple_of(j * 512, 512), 512)
            part = nt_dot(hidden[...], down_v[cols, :]).astype(BF16)
            if i < n - 1:
                target[:, cols] = part
            else:
                target[:, cols] = target[:, cols] + part.astype(F32)
            return 0

        lax.fori_loop(0, d // 512, down, 0)
        if i == 0:
            pump(2)
            pump(3)
            to_r_a.start()
            to_l_b.start()
        if i == 1:
            to_r.start()
        if i == 2:
            to_l.start()
            to_l_b.wait_recv()
            s3[:, dh:] = (s3[:, dh:].astype(F32) + rb[...].astype(F32)).astype(BF16)
            to_l_sum.start()

    to_r.wait_recv()
    to_l.wait_recv()
    to_r_sum.wait_recv()
    to_l_sum.wait_recv()
    out_ref[...] = (resid[...] + rl[...].astype(F32) + rr[...].astype(F32)).astype(BF16)

    for o in range(n):
        for p in range(2):
            own_right(o, p).wait_send()
            own_left(o, p).wait_send()
    for i in range(n):
        fwd_right(i).wait_send()
        fwd_left(i).wait_send()
    g1.drain()
    g2.drain()
    ring.drain()
    to_r_a.wait_send()
    to_l_b.wait_send()
    to_r.wait_send()
    to_l.wait_send()
    to_r_sum.wait_send()
    to_l_sum.wait_send()


def layer(q, k, v, lg, bias, extra, doc, gate, gain, wo, stream, ff_gain, wg, wu, wd):
    rows, d = stream.shape
    units = wg.shape[1]
    gains = jnp.concatenate([gain, ff_gain]).astype(F32).reshape(1, -1)
    vm = pl.BlockSpec(memory_space=pltpu.VMEM)
    hbm = pl.BlockSpec(memory_space=pl.ANY)
    blocks = rows // BL
    dma = pltpu.SemaphoreType.DMA

    def buf(*shape, dtype=BF16):
        return pltpu.VMEM(shape, dtype)

    return pl.pallas_call(
        layer_kernel,
        out_shape=jax.ShapeDtypeStruct((GR, d), BF16),
        in_specs=[hbm] * 10 + [vm] * 4,
        out_specs=vm,
        scratch_shapes=[
            buf(rows, 2 * DK), buf(rows, 2 * DK), buf(rows, 2 * DV), buf(rows, 2 * DK),
            buf(rows, 2 * DV), buf(rows, 3, dtype=F32),
            buf(*wg.shape), buf(*wu.shape), buf(wg.shape[0], 2 * units), buf(*wd.shape),
            buf(rows, 2 * DK, dtype=F32),
            buf(blocks, 1, 2 * DK, dtype=F32),
            buf(blocks, 1, 2 * DK, dtype=F32),
            buf(blocks * 2, DV, DK, dtype=F32),
            buf(blocks * 2, DV, 2 * DK),
            buf(2, DV, 2 * DK, dtype=F32),
            buf(rows, 2 * DV, dtype=F32),
            buf(2, 2 * DV, DK), buf(2, 8, DK, dtype=F32),
            buf(2 * DV, DK), buf(8, DK, dtype=F32),
            buf(2, DV, DK), buf(8, DK, dtype=F32),
            buf(NY, 2, DV, DK), buf(NY, 8, DK, dtype=F32),
            buf(2, DV, DK), buf(8, DK, dtype=F32),
            buf(NZ, DV, DK), buf(NZ, 8, DK, dtype=F32),
            buf(DV, 2 * DK), buf(DV, 2 * DK), buf(DV, 2 * DK),
            buf(1, 2 * DK, dtype=F32),
            buf(rows, 4 * 2 * DV), buf(2, GR, d), buf(4 * wo.shape[0], d),
            buf(2 * NCHIP * wg.shape[0], 2 * units), buf(2 * NCHIP * wd.shape[0], units),
            buf(GR, d, dtype=F32), buf(GR, d), buf(GR, units),
            buf(GR, d), buf(GR, d), buf(GR, d), buf(GR, d // 2), buf(GR, d // 2), buf(GR, d), buf(GR, d),
            dma((13,)), dma((3,)), dma((3,)),
            dma((8,)), dma((8,)), dma((8,)), dma((8,)),
            dma((8,)), dma((8,)), dma((4,)), dma((4,)),
            dma((8,)), dma((8,)), dma((4,)), dma((4,)), dma((6,)), dma((6,)),
        ] + plane_sems() + plane_sems() + [dma((k,)) for k in RowGather.SEMS],
        compiler_params=pltpu.CompilerParams(
            collective_id=0, has_side_effects=True, vmem_limit_bytes=67_043_328),
        cost_estimate=pl.CostEstimate(
            flops=29_000_000_000, bytes_accessed=16_000_000, transcendentals=0),
        name="layer",
    )(q, k, v, lg, gate, wo, stream, wg, wu, wd,
      bias.reshape(1, -1), extra.T, doc.reshape(1, -1), gains)


def per_device(
    stream, queries, projected_keys, values, decay_gate_logits, decay_gate_bias, extra_log_decay,
    document_index, output_gate, head_norm_gain, output_weight, feedforward_norm_gain,
    gate_weight, up_weight, down_weight,
):
    return layer(
        queries, projected_keys, values, decay_gate_logits, decay_gate_bias, extra_log_decay,
        document_index, output_gate, head_norm_gain, output_weight, stream,
        feedforward_norm_gain, gate_weight, up_weight, down_weight.T)


def solution(mesh):
    torus = Mesh(mesh.devices.reshape(4, 4, 2, mesh.shape["tp"]), ("sp_0", "sp_1", "sp_2", "tp"))
    placed = (
        P(SP, None), P(SP, "tp"), P(SP, "tp"), P(SP, "tp"), P(SP, "tp"), P("tp"), P(SP, "tp"),
        P(SP), P(SP, "tp"), P(), P("tp", None), P(), P(SP, "tp"), P(SP, "tp"), P("tp", SP),
    )
    return jax.shard_map(
        per_device, mesh=torus, in_specs=placed, out_specs=P(SP_TP, None), check_vma=False
    )
```

```python
import functools
import jax
import jax.numpy as jnp
from jax import lax
from jax.experimental import pallas as pl
from jax.experimental.pallas import tpu as pltpu
from jax.sharding import Mesh
from jax.sharding import PartitionSpec as P

SP = ("sp_0", "sp_1", "sp_2")
SP_TP = ("sp_0", "sp_1", "sp_2", "tp")
MESH = pl.DeviceIdType.MESH
F32 = jnp.float32
BF16 = jnp.bfloat16
TAU = 16.0
EPS = 1e-06
BL = 64
GR = 256
DK = 128
DV = 256
NZ, NY = 4, 4
NCHIP = NZ * NY


def nt_dot(a, b):
    return lax.dot_general(a, b, (((1,), (1,)), ((), ())), preferred_element_type=F32)


def tn_dot(a, b):
    return lax.dot_general(a, b, (((0,), (0,)), ((), ())), preferred_element_type=F32)


def nn_dot(a, b):
    return lax.dot_general(a, b, (((1,), (0,)), ((), ())), preferred_element_type=F32)


def remote_copy(src, dst, send, recv, target):
    return pltpu.make_async_remote_copy(
        src, dst, send, recv, device_id=target, device_id_type=MESH)


class PlaneGather:
    SEMS = (40, 40, 32, 32, 1)

    def __init__(self, src, dst, sems):
        self.src, self.dst = src, dst
        self.send, self.recv, self.core_send, self.core_recv, self.local = sems
        self.at = {"z": lax.axis_index("sp_0"), "y": lax.axis_index("sp_1")}
        self.core, self.x = lax.axis_index("sp_2"), lax.axis_index("tp")
        self.rows = src.shape[0] // 2

    def shifted(self, moves):
        at = dict(self.at)
        for axis, k in moves:
            at[axis] = lax.rem(at[axis] + (k + 4), 4)
        return at["z"], at["y"]

    def chip_at(self, axis, k):
        z, y = self.shifted([(axis, k)])
        return z, y, self.core, self.x

    def piece(self, hf, ja, jb, sub=None):
        a, b = ("y", "z") if hf == 0 else ("z", "y")
        z, y = self.shifted([(a, ja), (b, jb)])
        row = ((z * NY + y) * 2 + self.core) * (2 * self.rows) + hf * self.rows
        size = self.rows
        if sub is not None:
            size = size // 2
            row = row + sub * size
        return self.dst.at[pl.ds(pl.multiple_of(row, 16), size)]

    def axis(self, hf, stage):
        return ("y", "z")[(hf + stage) % 2]

    OFFS = (0, -1, 1, 2)

    def hop(self, hf, stage, ja, way, forward):
        axis = self.axis(hf, stage)
        k = hf * 20 + (0 if stage == 0 else 4 + 4 * self.OFFS.index(ja)) + (0 if way > 0 else 1)
        k = k + (2 if forward else 0)
        target = self.chip_at(axis, way)
        if forward:
            sub = 0 if way > 0 else 1
            ref = self.piece(hf, -way, 0, sub) if stage == 0 else self.piece(hf, ja, -way, sub)
            src = ref
        else:
            ref = self.piece(hf, 0, 0) if stage == 0 else self.piece(hf, ja, 0)
            own = stage == 0 or ja == 0
            src = self.src.at[pl.ds(hf * self.rows, self.rows)] if own else ref
        return remote_copy(src, ref, self.send.at[k], self.recv.at[k], target)

    def landing(self, hf, stage, ja, way, forward):
        axis = self.axis(hf, stage)
        k = hf * 20 + (0 if stage == 0 else 4 + 4 * self.OFFS.index(ja)) + (0 if way > 0 else 1)
        k = k + (2 if forward else 0)
        back = 2 if forward else -way
        sub = (0 if way > 0 else 1) if forward else None
        ref = self.piece(hf, back, 0, sub) if stage == 0 else self.piece(hf, ja, back, sub)
        return remote_copy(ref, ref, self.send.at[k], self.recv.at[k], self.chip_at(axis, way))

    def hand(self, hf, ja, jb):
        p = hf * 16 + self.OFFS.index(ja) * 4 + self.OFFS.index(jb)
        ref = self.piece(hf, ja, jb)
        src = self.src.at[pl.ds(hf * self.rows, self.rows)] if ja == 0 and jb == 0 else ref
        partner = (self.at["z"], self.at["y"], 1 - self.core, self.x)
        return remote_copy(src, ref, self.core_send.at[p], self.core_recv.at[p], partner)

    def handed(self, hf, ja, jb):
        p = hf * 16 + self.OFFS.index(ja) * 4 + self.OFFS.index(jb)
        a, b = ("y", "z") if hf == 0 else ("z", "y")
        z, y = self.shifted([(a, ja), (b, jb)])
        row = ((z * NY + y) * 2 + 1 - self.core) * (2 * self.rows) + hf * self.rows
        ref = self.dst.at[pl.ds(pl.multiple_of(row, 16), self.rows)]
        partner = (self.at["z"], self.at["y"], 1 - self.core, self.x)
        return remote_copy(ref, ref, self.core_send.at[p], self.core_recv.at[p], partner)

    def keep(self):
        row = ((self.at["z"] * NY + self.at["y"]) * 2 + self.core) * (2 * self.rows)
        return pltpu.make_async_copy(
            self.src, self.dst.at[pl.ds(pl.multiple_of(row, 16), 2 * self.rows)], self.local.at[0])

    def start(self):
        for stage in range(2):
            for hf in range(2):
                for way in (1, -1):
                    self.hop(hf, stage, 0, way, False).start()
        for hf in range(2):
            self.hand(hf, 0, 0).start()
        self.keep().start()

    def second(self, hf, ja):
        for way in (1, -1):
            self.hop(hf, 1, ja, way, False).start()
        self.hand(hf, ja, 0).start()

    def near(self):
        for way in (1, -1):
            for hf in range(2):
                self.landing(hf, 0, 0, way, False).wait_recv()
                self.hop(hf, 0, 0, way, True).start()

    def near_second(self, hf):
        for way in (1, -1):
            self.second(hf, -way)

    def far(self):
        for hf in range(2):
            for way in (1, -1):
                self.landing(hf, 0, 0, way, True).wait_recv()
            self.second(hf, 2)

    def column(self, ja):
        for way in (1, -1):
            for hf in range(2):
                self.landing(hf, 1, ja, way, False).wait_recv()
                self.hop(hf, 1, ja, way, True).start()
                self.hand(hf, ja, -way).start()

    def column_far(self, ja):
        for hf in range(2):
            for way in (1, -1):
                self.landing(hf, 1, ja, way, True).wait_recv()
            self.hand(hf, ja, 2).start()

    def finish(self):
        self.keep().wait()
        for hf in range(2):
            for ja in self.OFFS:
                for jb in self.OFFS:
                    self.handed(hf, ja, jb).wait_recv()

    def drain(self):
        for hf in range(2):
            for way in (1, -1):
                for forward in (False, True):
                    self.hop(hf, 0, 0, way, forward).wait_send()
                    for ja in self.OFFS:
                        self.hop(hf, 1, ja, way, forward).wait_send()
            for ja in self.OFFS:
                for jb in self.OFFS:
                    self.hand(hf, ja, jb).wait_send()


class RowGather:
    SEMS = (6, 6, 3, 3)

    def __init__(self, rows, dst, sems):
        self.dst = dst
        self.send, self.recv, self.core_send, self.core_recv = sems
        self.z, self.y = lax.axis_index("sp_0"), lax.axis_index("sp_1")
        self.core, self.x = lax.axis_index("sp_2"), lax.axis_index("tp")
        self.rows = rows

    def piece(self, k, core, sub=None):
        size = self.rows // 2
        row = lax.rem(self.x + (k + 4), 4) * self.rows + core * size
        if sub is not None:
            size = size // 2
            row = row + sub * size
        return self.dst.at[pl.ds(pl.multiple_of(row, 16), size)]

    def side(self, way):
        return (self.z, self.y, self.core, lax.rem(self.x + (way + 4), 4))

    def copy(self, ref, k, way):
        return remote_copy(ref, ref, self.send.at[k], self.recv.at[k], self.side(way))

    def key(self, way, part):
        return (0 if way > 0 else 1) + 2 * part

    def hop(self, way, part):
        first = 0 if way > 0 else 1
        if part == 2:
            ref = self.piece(-way, self.core, first)
        else:
            ref = self.piece(0, self.core, first if part == 0 else 1 - first)
        return self.copy(ref, self.key(way, part), way)

    def landing(self, way, part):
        first = 0 if way > 0 else 1
        if part == 2:
            ref = self.piece(2, self.core, first)
        else:
            ref = self.piece(-way, self.core, first if part == 0 else 1 - first)
        return self.copy(ref, self.key(way, part), way)

    def hand(self, i, arriving=False):
        k = (-1, 1, 2)[i]
        ref = self.piece(k, 1 - self.core if arriving else self.core)
        return remote_copy(
            ref, ref, self.core_send.at[i], self.core_recv.at[i], (self.z, self.y, 1 - self.core, self.x))

    def start(self):
        for part in range(2):
            for way in (1, -1):
                self.hop(way, part).start()

    def near(self):
        for way in (1, -1):
            self.landing(way, 0).wait_recv()
            self.hop(way, 2).start()

    def near_hand(self):
        for i, way in enumerate((1, -1)):
            self.landing(way, 1).wait_recv()
            self.hand(i).start()

    def far(self):
        for way in (1, -1):
            self.landing(way, 2).wait_recv()
        self.hand(2).start()

    def finish(self):
        for i in range(3):
            self.hand(i, True).wait_recv()

    def drain(self):
        for way in (1, -1):
            for part in range(3):
                self.hop(way, part).wait_send()
        for i in range(3):
            self.hand(i).wait_send()


def plane_sems():
    return [pltpu.SemaphoreType.DMA((k,)) for k in PlaneGather.SEMS]


def layer_kernel(
    q_in, k_in, v_in, lg_in, gate_in, wo_in, stream_in, wg_in, wu_in, wd_in,
    bias_ref, extra_ref, doc_ref, gain_ref, ff_gain_ref,
    out_ref,
    q_ref, k_ref, v_ref, lg_ref, gate_ref, aux_ref, wg_ref, wu_ref, shard_ref, wd_ref,
    cum_ref, blk_ref, off_ref, states_ref, before_ref, run_ref, local_ref,
    own_t, own_e, part_t, part_e, chip_t, chip_e, ry_t, ry_e, row_t, row_e, rz_t, rz_e, mine_c, send_c, part_c, sum_ref,
    hm, st, wo_v, w_v, down_v, resid, normed, hidden, s2, s1, s3, ra, rb, rl, rr,
    local_sem, core_send, core_recv, t_send, t_recv, e_send, e_recv,
    own_rs, own_ls, fwd_rs, fwd_ls, left_in, right_in, opp_l, opp_r, rs_send, rs_recv,
    *gather_sems,
):
    rows = q_ref.shape[0]
    blocks = rows // BL
    groups = rows // GR
    per = GR // BL
    z, y = lax.axis_index("sp_0"), lax.axis_index("sp_1")
    core, me = lax.axis_index("sp_2"), lax.axis_index("tp")
    scale = DK ** (-0.5)
    n = 4
    q_rows = GR
    half = q_rows // 2
    d = out_ref.shape[1]
    units = hidden.shape[1]
    ix_r, ix_l = lax.rem(me + 1, n), lax.rem(me + n - 1, n)
    right, left = (z, y, core, ix_r), (z, y, core, ix_l)
    partner = (z, y, 1 - core, me)
    order = (2, 1, 3, 0)

    def quarter_of(owner, offset):
        return lax.rem(owner + offset, n)

    def along_y(k):
        return (z, lax.rem(y + k, NY), core, me)

    def along_z(k):
        return (lax.rem(z + k, NZ), y, core, me)

    wo_own = wo_in.shape[0]
    loads = {
        name: pltpu.make_async_copy(src, dst, local_sem.at[i])
        for i, (name, src, dst) in enumerate((
            ("wg", wg_in, wg_ref), ("wu", wu_in, wu_ref), ("wd", wd_in, wd_ref),
            ("wo", wo_in, wo_v.at[pl.ds(pl.multiple_of(me * wo_own, wo_own), wo_own)]),
            ("lg", lg_in, lg_ref), ("k", k_in, k_ref), ("v", v_in, v_ref), ("q", q_in, q_ref),
            ("gate", gate_in, gate_ref),
        ))
    }
    for copy in loads.values():
        copy.start()

    def load_stream(i):
        at = pl.multiple_of(quarter_of(me, order[i]) * q_rows, q_rows)
        return pltpu.make_async_copy(
            stream_in.at[pl.ds(at, q_rows)], st.at[i % 2], local_sem.at[9 + i])

    load_stream(0).start()
    load_stream(1).start()

    rz_t[pl.ds(z, 1)] = jnp.zeros((1, DV, DK), BF16)

    barrier = pltpu.get_barrier_semaphore()
    pl.semaphore_signal(barrier, inc=1, device_id=partner, device_id_type=MESH)
    pl.semaphore_signal(barrier, inc=1, device_id=right, device_id_type=MESH)
    pl.semaphore_signal(barrier, inc=1, device_id=left, device_id_type=MESH)
    for k in range(1, NY):
        pl.semaphore_signal(barrier, inc=1, device_id=along_y(k), device_id_type=MESH)
        pl.semaphore_signal(barrier, inc=1, device_id=along_z(k), device_id_type=MESH)

    loads["wg"].wait()
    loads["wu"].wait()
    for j in range(units // 128):
        shard_ref[:, j * 256 : j * 256 + 128] = wg_ref[:, j * 128 : (j + 1) * 128]
        shard_ref[:, j * 256 + 128 : (j + 1) * 256] = wu_ref[:, j * 128 : (j + 1) * 128]
    loads["wd"].wait()
    loads["wo"].wait()

    pl.semaphore_wait(barrier, 9)
    g1 = PlaneGather(shard_ref, w_v, gather_sems[:5])
    g2 = PlaneGather(wd_ref, down_v, gather_sems[5:10])
    ring = RowGather(wo_own, wo_v, gather_sems[10:])
    ring.start()
    g1.start()

    ri = lax.broadcasted_iota(jnp.int32, (GR, GR), 0)
    ci = lax.broadcasted_iota(jnp.int32, (GR, GR), 1)

    def columns(g, _):
        at = pl.multiple_of(g * GR, GR)
        for j in range(3):
            lanes = pl.ds(pl.multiple_of(g * GR, GR), GR)
            row = doc_ref[:, lanes].astype(F32) if j == 2 else extra_ref[j : j + 1, lanes]
            col = jnp.sum(jnp.where(ri == ci, row, 0.0), axis=1, keepdims=True)
            aux_ref[pl.ds(at, GR), j : j + 1] = col
        return 0

    lax.fori_loop(0, groups, columns, 0)
    loads["lg"].wait()
    loads["k"].wait()
    loads["v"].wait()
    run_ref[...] = jnp.zeros_like(run_ref)

    def doc_at(r):
        return aux_ref[pl.ds(r, 1), 2:3]

    def first(g, base):
        at = pl.multiple_of(g * GR, GR)
        same_block = (ri & (GR - BL)) == (ci & (GR - BL))
        tri = jnp.where(same_block & (ci <= ri), 1.0, 0.0).astype(BF16)
        logits = lg_ref[pl.ds(at, GR), :].astype(F32) + bias_ref[...]
        ld = (jnp.minimum(logits, 0.0) - jnp.log1p(jnp.exp(-jnp.abs(logits)))) / TAU
        extra0 = jnp.broadcast_to(aux_ref[pl.ds(at, GR), 0:1], (GR, DK))
        extra1 = jnp.broadcast_to(aux_ref[pl.ds(at, GR), 1:2], (GR, DK))
        ld = ld + jnp.concatenate([extra0, extra1], axis=1)
        hi = ld.astype(BF16)
        rest = ld - hi.astype(F32)
        mid = rest.astype(BF16)
        low = (rest - mid.astype(F32)).astype(BF16)
        cum = nn_dot(tri, hi) + nn_dot(tri, mid) + nn_dot(tri, low)
        cum_ref[pl.ds(at, GR), :] = cum
        cum3 = cum.reshape(per, BL, 2 * DK)
        ends = cum3[:, BL - 1 : BL, :]
        off = base
        for b in range(per):
            off_ref[pl.ds(g * per + b, 1)] = off[None]
            blk_ref[pl.ds(g * per + b, 1)] = ends[b : b + 1]
            off = off + ends[b]
        doc = aux_ref[pl.ds(at, GR), 2:3].reshape(per, BL, 1)
        tail_mask = jnp.where(doc == doc[:, BL - 1 : BL], 1.0, 0.0)
        head_mask = jnp.where(doc == doc[:, 0:1], 1.0, 0.0)
        kf = k_ref[pl.ds(at, GR), :].astype(F32).reshape(per, BL, 2 * DK)
        tail = (kf * jnp.exp(ends - cum3) * tail_mask).astype(BF16)
        head = (kf * jnp.exp(cum3) * head_mask).astype(BF16)
        for b in range(per):
            start = at + b * BL
            keep = jnp.where(doc_at(jnp.maximum(start - 1, 0)) == doc_at(start + BL - 1), 1.0, 0.0)
            decay = jnp.exp(ends[b]) * keep
            for h in range(2):
                c = slice(h * DK, (h + 1) * DK)
                keys = jnp.concatenate([tail[b][:, c], head[b][:, c]], axis=1)
                vals = v_ref[pl.ds(pl.multiple_of(start, BL), BL), h * DV : (h + 1) * DV]
                both = tn_dot(vals, keys)
                slot = (g * per + b) * 2 + h
                states_ref[pl.ds(slot, 1)] = both[None, :, DK:]
                fw = run_ref[h, :, :DK]
                before_ref[pl.ds(slot, 1), :, :DK] = fw.astype(BF16)[None]
                run_ref[h, :, :DK] = fw * decay[:, c] + both[:, :DK]
        return off

    total = lax.fori_loop(0, groups, first, jnp.zeros((1, 2 * DK), F32))
    sum_ref[...] = total

    def step(b, _):
        r = blocks - 1 - b
        hi = jnp.minimum(r * BL + BL, rows - 1)
        keep = jnp.where(doc_at(hi) == doc_at(r * BL), 1.0, 0.0)
        decay = jnp.exp(blk_ref[pl.ds(r, 1)][0]) * keep
        for h in range(2):
            bw = run_ref[h, :, DK:]
            before_ref[pl.ds(r * 2 + h, 1), :, DK:] = bw.astype(BF16)[None]
            run_ref[h, :, DK:] = bw * decay[:, h * DK : (h + 1) * DK] + states_ref[r * 2 + h]
        return 0

    lax.fori_loop(0, blocks, step, 0)
    first_doc = jnp.broadcast_to(doc_at(0), (1, DK))
    last_doc = jnp.broadcast_to(doc_at(rows - 1), (1, DK))
    for h in range(2):
        own_t[h, :DV] = run_ref[h, :, :DK].astype(BF16)
        own_t[h, DV:] = run_ref[h, :, DK:].astype(BF16)
        own_e[h, 0:1] = total[:, h * DK : (h + 1) * DK]
        own_e[h, 1:2] = first_doc
        own_e[h, 2:3] = last_doc
        own_e[h, 3:8] = jnp.zeros((5, DK), F32)

    g1.near()
    swap_t = pltpu.make_async_remote_copy(
        own_t.at[1 - core], part_t, core_send.at[0], core_recv.at[0],
        device_id=partner, device_id_type=MESH)
    swap_e = pltpu.make_async_remote_copy(
        own_e.at[1 - core], part_e, core_send.at[1], core_recv.at[1],
        device_id=partner, device_id_type=MESH)
    swap_t.start()
    swap_e.start()
    swap_t.wait()
    swap_e.wait()
    is0 = core == 0
    mine_e = own_e[pl.ds(core, 1)][0]
    other_e = part_e[...]
    e0 = jnp.where(is0, mine_e, other_e)
    e1 = jnp.where(is0, other_e, mine_e)
    mine_t = own_t[pl.ds(core, 1)][0].astype(F32)
    other_t = part_t[...].astype(F32)
    t0 = jnp.where(is0, mine_t, other_t)
    t1 = jnp.where(is0, other_t, mine_t)
    through1 = jnp.exp(e1[0:1]) * jnp.where(e0[2:3] == e1[2:3], 1.0, 0.0)
    through0 = jnp.exp(e0[0:1]) * jnp.where(e1[1:2] == e0[1:2], 1.0, 0.0)
    chip_t[0] = (t1[:DV] + through1 * t0[:DV]).astype(BF16)
    chip_t[1] = (t0[DV:] + through0 * t1[DV:]).astype(BF16)
    chip_row = jnp.concatenate(
        [e0[0:1] + e1[0:1], e0[1:2], e1[2:3], jnp.zeros((5, DK), F32)], axis=0)
    chip_e[...] = chip_row
    ry_e[pl.ds(y, 1)] = chip_row[None]
    ry_t[pl.ds(y, 1)] = chip_t[...][None]

    y_sends = []
    for k in range(1, NY):
        y_sends.append(remote_copy(chip_e, ry_e.at[y], e_send.at[k], e_recv.at[k], along_y(k)))
        y_sends.append(remote_copy(chip_t, ry_t.at[y], t_send.at[k], t_recv.at[k], along_y(k)))
    for s in y_sends:
        s.start()
    g1.near_second(0)
    g2.start()
    loads["q"].wait()

    def inside(g, _):
        at = pl.multiple_of(g * GR, GR)
        same_block = (ri & (GR - BL)) == (ci & (GR - BL))
        doc = aux_ref[pl.ds(at, GR), 2:3]
        same = same_block & (doc == doc_ref[:, pl.ds(at, GR)].astype(F32))
        below = same & (ci <= ri)
        above = same & (ci >= ri)
        cum3 = cum_ref[pl.ds(at, GR), :].reshape(per, BL, 2 * DK)
        middle = cum3[:, BL // 2 - 1 : BL // 2]
        ends = cum3[:, BL - 1 : BL]
        rising = jnp.exp(cum3 - middle)
        falling = jnp.exp(middle - cum3)
        qf = q_ref[pl.ds(at, GR), :].astype(F32).reshape(per, BL, 2 * DK) * scale
        kf = k_ref[pl.ds(at, GR), :].astype(F32).reshape(per, BL, 2 * DK)
        q_rise = (qf * rising).astype(BF16).reshape(GR, 2 * DK)
        q_fall = (qf * falling).astype(BF16).reshape(GR, 2 * DK)
        k_rise = (kf * rising).astype(BF16).reshape(GR, 2 * DK)
        k_fall = (kf * falling).astype(BF16).reshape(GR, 2 * DK)
        q_fwd = qf * jnp.exp(cum3)
        q_bwd = qf * jnp.exp(ends - cum3)
        for h in range(2):
            c = slice(h * DK, (h + 1) * DK)
            fw = nt_dot(q_rise[:, c], k_fall[:, c])
            bw = nt_dot(q_fall[:, c], k_rise[:, c])
            scores = jnp.where(below, fw, 0.0) + jnp.where(above, bw, 0.0)
            vals = v_ref[pl.ds(at, GR), h * DV : (h + 1) * DV]
            local_ref[pl.ds(at, GR), h * DV : (h + 1) * DV] = nn_dot(scores.astype(BF16), vals)
        for b in range(per):
            start = at + b * BL
            prev = doc_at(jnp.maximum(start - 1, 0))
            following = doc_at(jnp.minimum(start + BL, rows - 1))
            rows_doc = doc[b * BL : (b + 1) * BL]
            hit_f = jnp.where(rows_doc == prev, 1.0, 0.0)
            hit_b = jnp.where(rows_doc == following, 1.0, 0.0)
            for h in range(2):
                c = slice(h * DK, (h + 1) * DK)
                both = jnp.concatenate([q_fwd[b][:, c] * hit_f, q_bwd[b][:, c] * hit_b], axis=1)
                here = pl.ds(pl.multiple_of(start, BL), BL)
                local_ref[here, h * DV : (h + 1) * DV] += nt_dot(
                    both.astype(BF16), before_ref[(g * per + b) * 2 + h])
        return 0

    lax.fori_loop(0, groups // 2, inside, 0)
    g1.column(0)
    lax.fori_loop(groups // 2, groups, inside, 0)

    ring.near()
    for s in y_sends:
        s.wait()
    run_ref[0] = jnp.zeros_like(run_ref[0])

    def earlier(states, table):
        def body(j, _):
            e = table[j]
            p = table[jnp.maximum(j - 1, 0)]
            keep = jnp.exp(e[0:1]) * jnp.where(e[2:3] == p[2:3], 1.0, 0.0)
            run_ref[0, :, :DK] = states(j, 0).astype(F32) + run_ref[0, :, :DK] * keep
            return 0
        return body

    def later(states, table):
        def body(i, _):
            j = NY - 1 - i
            e = table[j]
            p = table[jnp.minimum(j + 1, NY - 1)]
            keep = jnp.exp(e[0:1]) * jnp.where(e[1:2] == p[1:2], 1.0, 0.0)
            run_ref[0, :, DK:] = states(j, 1).astype(F32) + run_ref[0, :, DK:] * keep
            return 0
        return body

    def row_state(j, way):
        return ry_t[j, way]

    def column_state(j, way):
        return rz_t[j]

    lax.fori_loop(0, y, earlier(row_state, ry_e), 0)
    lax.fori_loop(0, NY - 1 - y, later(row_state, ry_e), 0)
    run_ref[1] = run_ref[0]
    lax.fori_loop(y, NY, earlier(row_state, ry_e), 0)
    lax.fori_loop(NY - 1 - y, NY, later(row_state, ry_e), 0)
    row_t[0] = run_ref[0, :, :DK].astype(BF16)
    row_t[1] = run_ref[0, :, DK:].astype(BF16)
    in_row = [ry_e[j] for j in range(NY)]
    row_sum = in_row[0][0:1] + in_row[1][0:1] + in_row[2][0:1] + in_row[3][0:1]
    sum_before = jnp.zeros((1, DK), F32)
    sum_after = jnp.zeros((1, DK), F32)
    for j in range(NY):
        sum_before = sum_before + jnp.where(j < y, in_row[j][0:1], 0.0)
        sum_after = sum_after + jnp.where(j > y, in_row[j][0:1], 0.0)
    last_before = ry_e[jnp.maximum(y - 1, 0)][2:3]
    first_after = ry_e[jnp.minimum(y + 1, NY - 1)][1:2]
    row_row = jnp.concatenate(
        [row_sum, in_row[0][1:2], in_row[NY - 1][2:3], jnp.zeros((5, DK), F32)], axis=0)
    row_e[...] = row_row
    rz_e[pl.ds(z, 1)] = row_row[None]
    z_sends = []
    for k in range(1, NZ):
        back = jnp.where(lax.rem(z + k, NZ) > z, 0, 1)
        z_sends.append(
            remote_copy(row_e, rz_e.at[z], e_send.at[4 + k], e_recv.at[4 + k], along_z(k)))
        z_sends.append(
            remote_copy(row_t.at[back], rz_t.at[z], t_send.at[4 + k], t_recv.at[4 + k], along_z(k)))
    for s in z_sends:
        s.start()
    g1.near_second(1)
    g1.far()
    for s in z_sends:
        s.wait()
    g2.near()
    g2.near_second(0)
    g2.near_second(1)

    run_ref[0] = jnp.zeros_like(run_ref[0])
    lax.fori_loop(0, z, earlier(column_state, rz_e), 0)
    lax.fori_loop(0, NZ - 1 - z, later(column_state, rz_e), 0)
    prev_last = jnp.where(z > 0, rz_e[jnp.maximum(z - 1, 0)][2:3], -1.0)
    next_first = jnp.where(z < NZ - 1, rz_e[jnp.minimum(z + 1, NZ - 1)][1:2], -1.0)
    pass_f = jnp.exp(sum_before) * jnp.where(
        y == 0, 1.0, jnp.where(prev_last == last_before, 1.0, 0.0))
    pass_b = jnp.exp(sum_after) * jnp.where(
        y == NY - 1, 1.0, jnp.where(next_first == first_after, 1.0, 0.0))
    cf = run_ref[1, :, :DK] + pass_f * run_ref[0, :, :DK]
    cb = run_ref[1, :, DK:] + pass_b * run_ref[0, :, DK:]
    before_doc = jnp.where(y > 0, last_before, prev_last)
    after_doc = jnp.where(y < NY - 1, first_after, next_first)
    pass0 = jnp.exp(e0[0:1]) * jnp.where(before_doc == e0[2:3], 1.0, 0.0)
    pass1 = jnp.exp(e1[0:1]) * jnp.where(after_doc == e1[1:2], 1.0, 0.0)
    mine_t = own_t[pl.ds(core, 1)][0].astype(F32)
    other_t = part_t[...].astype(F32)
    t0f = jnp.where(is0, mine_t[:DV], other_t[:DV])
    t1b = jnp.where(is0, other_t[DV:], mine_t[DV:])
    c0 = jnp.concatenate([cf, t1b + pass1 * cb], axis=1)
    c1 = jnp.concatenate([t0f + pass0 * cf, cb], axis=1)
    mine_c[...] = jnp.where(is0, c0, c1).astype(BF16)
    send_c[...] = jnp.where(is0, c1, c0).astype(BF16)
    swap_c = pltpu.make_async_remote_copy(
        send_c, part_c, core_send.at[2], core_recv.at[2],
        device_id=partner, device_id_type=MESH)
    swap_c.start()
    ring.near_hand()
    enter_f = jnp.where(is0, before_doc, e0[2:3])[:, 0:1]
    enter_b = jnp.where(is0, e1[1:2], after_doc)[:, 0:1]
    swap_c.wait()

    loads["gate"].wait()

    def last(g):
        at = pl.multiple_of(g * GR, GR)
        doc = aux_ref[pl.ds(at, GR), 2:3]
        hit_f = jnp.where(doc == enter_f, 1.0, 0.0)
        hit_b = jnp.where(doc == enter_b, 1.0, 0.0)
        glob = cum_ref[pl.ds(at, GR), :].reshape(per, BL, 2 * DK) + off_ref[pl.ds(g * per, per)]
        glob = glob.reshape(GR, 2 * DK)
        qf = q_ref[pl.ds(at, GR), :].astype(F32) * scale
        q_fwd = (qf * jnp.exp(glob) * hit_f).astype(BF16)
        q_bwd = (qf * jnp.exp(sum_ref[...] - glob) * hit_b).astype(BF16)
        gain = gain_ref[...].astype(F32).reshape(1, DV)
        for h in range(2):
            c = slice(h * DK, (h + 1) * DK)
            both = jnp.concatenate([q_fwd[:, c], q_bwd[:, c]], axis=1)
            carry = jnp.where(h == core, mine_c[...], part_c[...])
            out = local_ref[pl.ds(at, GR), h * DV : (h + 1) * DV] + nt_dot(both, carry)
            out = out * lax.rsqrt(jnp.mean(out * out, axis=-1, keepdims=True) + EPS) * gain
            u = gate_ref[pl.ds(at, GR), h * DV : (h + 1) * DV].astype(F32)
            hm[pl.ds(at, GR), pl.ds(pl.multiple_of(me * 2 * DV + h * DV, DV), DV)] = (
                out * (u / (1.0 + jnp.exp(-u)))).astype(BF16)

    def three(i, _):
        last(quarter_of(me, i + i // 2))
        return 0

    lax.fori_loop(0, 3, three, 0)

    def piece(slot, r, part):
        return hm.at[
            pl.ds(pl.multiple_of(r * q_rows + part * half, half), half),
            pl.ds(pl.multiple_of(slot * 2 * DV, 2 * DV), 2 * DV)]

    def remote(ref, send, recv, target, dst=None):
        return pltpu.make_async_remote_copy(
            ref, ref if dst is None else dst, send, recv, device_id=target, device_id_type=MESH)

    def wire(slot, quarter, part, send, recv, target):
        return remote(piece(slot, quarter, part), send, recv, target)

    to_right = (((0, 0), (3, 0), (3, 1)), ((2, 0), (2, 1)), ((1, 0), (0, 1)), ((1, 1),))
    to_left = (((0, 1), (1, 1), (1, 0)), ((3, 1), (0, 0)), ((2, 1), (2, 0)), ((3, 0),))

    def own_right(o, p):
        return wire(me, quarter_of(me, o), p, own_rs.at[o * 2 + p], left_in.at[o * 2 + p], right)

    def own_left(o, p):
        return wire(me, quarter_of(me, o), p, own_ls.at[o * 2 + p], right_in.at[o * 2 + p], left)

    def came_left(o, p):
        return wire(ix_l, quarter_of(ix_l, o), p, own_rs.at[o * 2 + p], left_in.at[o * 2 + p], right)

    def came_right(o, p):
        return wire(ix_r, quarter_of(ix_r, o), p, own_ls.at[o * 2 + p], right_in.at[o * 2 + p], left)

    def fwd_right(i):
        return wire(ix_l, quarter_of(ix_r, order[i]), 0, fwd_rs.at[i], opp_l.at[i], right)

    def fwd_left(i):
        return wire(ix_r, quarter_of(ix_l, order[i]), 1, fwd_ls.at[i], opp_r.at[i], left)

    opposite = lax.rem(me + 2, n)

    def came_opp_l(i):
        return wire(opposite, quarter_of(me, order[i]), 0, fwd_rs.at[i], opp_l.at[i], right)

    def came_opp_r(i):
        return wire(opposite, quarter_of(me, order[i]), 1, fwd_ls.at[i], opp_r.at[i], left)

    def send_own(i):
        for k in range(len(to_right[i])):
            own_right(*to_right[i][k]).start()
            own_left(*to_left[i][k]).start()

    seen = set()

    def arrived(side, o, p):
        if (side, o, p) not in seen:
            seen.add((side, o, p))
            (came_left if side == "l" else came_right)(o, p).wait_recv()

    def pump(i):
        arrived("l", (2 + order[i]) % n, 0)
        fwd_right(i).start()
        arrived("r", (n - 2 + order[i]) % n, 1)
        fwd_left(i).start()

    send_own(0)
    last(quarter_of(me, 2))
    for ja in (-1, 1):
        g1.column(ja)
    g2.column(0)
    ring.far()
    pump(0)
    send_own(1)
    g1.column(2)
    g2.far()
    send_own(2)
    for ja in (0, -1, 1):
        g1.column_far(ja)
    for ja in (-1, 1):
        g2.column(ja)
    ring.finish()

    dh = d // 2
    to_r_a = remote(s2.at[:, pl.ds(0, dh)], rs_send.at[0], rs_recv.at[0], right, ra)
    to_l_b = remote(s2.at[:, pl.ds(dh, dh)], rs_send.at[1], rs_recv.at[1], left, rb)
    lo, up = pl.ds(0, dh), pl.ds(dh, dh)
    to_r = remote(s1.at[:, up], rs_send.at[2], rs_recv.at[2], right, rl.at[:, up])
    to_l = remote(s3.at[:, lo], rs_send.at[3], rs_recv.at[3], left, rr.at[:, lo])
    to_r_sum = remote(s1.at[:, lo], rs_send.at[4], rs_recv.at[4], right, rl.at[:, lo])
    to_l_sum = remote(s3.at[:, up], rs_send.at[5], rs_recv.at[5], left, rr.at[:, up])

    def prepare(i):
        at = pl.multiple_of(quarter_of(me, order[i]) * q_rows, q_rows)
        rows = pl.ds(at, q_rows)
        for p in range(2):
            arrived("l", (1 + order[i]) % n, p)
            arrived("r", (n - 1 + order[i]) % n, p)
        came_opp_l(i).wait_recv()
        came_opp_r(i).wait_recv()
        load_stream(i).wait()

        def project(j, total):
            cols = pl.ds(pl.multiple_of(j * 1024, 1024), 1024)
            acc = st[i % 2, :, cols].astype(F32) + nn_dot(hm[rows, :], wo_v[:, cols])
            resid[:, cols] = acc
            return total + jnp.sum(acc * acc, axis=-1, keepdims=True)

        squares = lax.fori_loop(0, d // 1024, project, jnp.zeros((q_rows, 1), F32))
        if i < n - 2:
            load_stream(i + 2).start()
        factor = lax.rsqrt(squares / d + EPS)
        normed[...] = (resid[...] * factor * ff_gain_ref[...].astype(F32).reshape(1, d)).astype(BF16)

    prepare(0)
    pump(1)
    send_own(3)
    g2.column(2)
    g1.column_far(2)
    for ja in (0, -1, 1):
        g2.column_far(ja)
    for i in range(n):
        if i == 0:
            g1.finish()
        else:
            prepare(i)

        def gate_up(at, width):
            both = nn_dot(normed[...], w_v[:, pl.ds(pl.multiple_of(at * 2, 256), 2 * width)])
            for b in range(width // 128):
                g = both[:, b * 256 : b * 256 + 128]
                u = both[:, b * 256 + 128 : (b + 1) * 256]
                hidden[:, pl.ds(pl.multiple_of(at + b * 128, 128), 128)] = (
                    g / (1.0 + jnp.exp(-g)) * u).astype(BF16)

        def gate_up_pair(j, _):
            gate_up(j * 256, 256)
            return 0

        lax.fori_loop(0, units // 256, gate_up_pair, 0)
        gate_up(units // 256 * 256, units % 256)
        if i == 0:
            g2.column_far(2)
            pump(2)
            pump(3)
            g2.finish()
        if i == 2:
            to_r_a.wait_recv()
            s1[:, :dh] = (s1[:, :dh].astype(F32) + ra[...].astype(F32)).astype(BF16)
            to_r_sum.start()
        target = (s2, s1, s3, resid)[i]

        def down(j, _):
            cols = pl.ds(pl.multiple_of(j * 512, 512), 512)
            part = nt_dot(hidden[...], down_v[cols, :]).astype(BF16)
            if i < n - 1:
                target[:, cols] = part
            else:
                target[:, cols] = target[:, cols] + part.astype(F32)
            return 0

        tiles = d // 1024
        first_half, second_half = ((tiles, 2 * tiles), (0, tiles)) if i == 1 else (
            (0, tiles), (tiles, 2 * tiles))
        lax.fori_loop(*first_half, down, 0)
        if i == 0:
            to_r_a.start()
        if i == 1:
            to_r.start()
        if i == 2:
            to_l.start()
        lax.fori_loop(*second_half, down, 0)
        if i == 0:
            to_l_b.start()
        if i == 2:
            to_l_b.wait_recv()
            s3[:, dh:] = (s3[:, dh:].astype(F32) + rb[...].astype(F32)).astype(BF16)
            to_l_sum.start()

    to_r.wait_recv()
    to_l.wait_recv()
    to_r_sum.wait_recv()
    to_l_sum.wait_recv()
    out_ref[...] = (resid[...] + rl[...].astype(F32) + rr[...].astype(F32)).astype(BF16)

    for o in range(n):
        for p in range(2):
            own_right(o, p).wait_send()
            own_left(o, p).wait_send()
    for i in range(n):
        fwd_right(i).wait_send()
        fwd_left(i).wait_send()
    g1.drain()
    g2.drain()
    ring.drain()
    to_r_a.wait_send()
    to_l_b.wait_send()
    to_r.wait_send()
    to_l.wait_send()
    to_r_sum.wait_send()
    to_l_sum.wait_send()


def layer(q, k, v, lg, bias, extra, doc, gate, gain, wo, stream, ff_gain, wg, wu, wd):
    rows, d = stream.shape
    units = wg.shape[1]
    vm = pl.BlockSpec(memory_space=pltpu.VMEM)
    hbm = pl.BlockSpec(memory_space=pl.ANY)
    blocks = rows // BL
    dma = pltpu.SemaphoreType.DMA

    def buf(*shape, dtype=BF16):
        return pltpu.VMEM(shape, dtype)

    return pl.pallas_call(
        layer_kernel,
        out_shape=jax.ShapeDtypeStruct((GR, d), BF16),
        in_specs=[hbm] * 10 + [vm] * 5,
        out_specs=vm,
        scratch_shapes=[
            buf(rows, 2 * DK), buf(rows, 2 * DK), buf(rows, 2 * DV), buf(rows, 2 * DK),
            buf(rows, 2 * DV), buf(rows, 3, dtype=F32),
            buf(*wg.shape), buf(*wu.shape), buf(wg.shape[0], 2 * units), buf(*wd.shape),
            buf(rows, 2 * DK, dtype=F32),
            buf(blocks, 1, 2 * DK, dtype=F32),
            buf(blocks, 1, 2 * DK, dtype=F32),
            buf(blocks * 2, DV, DK, dtype=F32),
            buf(blocks * 2, DV, 2 * DK),
            buf(2, DV, 2 * DK, dtype=F32),
            buf(rows, 2 * DV, dtype=F32),
            buf(2, 2 * DV, DK), buf(2, 8, DK, dtype=F32),
            buf(2 * DV, DK), buf(8, DK, dtype=F32),
            buf(2, DV, DK), buf(8, DK, dtype=F32),
            buf(NY, 2, DV, DK), buf(NY, 8, DK, dtype=F32),
            buf(2, DV, DK), buf(8, DK, dtype=F32),
            buf(NZ, DV, DK), buf(NZ, 8, DK, dtype=F32),
            buf(DV, 2 * DK), buf(DV, 2 * DK), buf(DV, 2 * DK),
            buf(1, 2 * DK, dtype=F32),
            buf(rows, 4 * 2 * DV), buf(2, GR, d), buf(4 * wo.shape[0], d),
            buf(2 * NCHIP * wg.shape[0], 2 * units), buf(2 * NCHIP * wd.shape[0], units),
            buf(GR, d, dtype=F32), buf(GR, d), buf(GR, units),
            buf(GR, d), buf(GR, d), buf(GR, d), buf(GR, d // 2), buf(GR, d // 2), buf(GR, d), buf(GR, d),
            dma((13,)), dma((3,)), dma((3,)),
            dma((8,)), dma((8,)), dma((8,)), dma((8,)),
            dma((8,)), dma((8,)), dma((4,)), dma((4,)),
            dma((8,)), dma((8,)), dma((4,)), dma((4,)), dma((6,)), dma((6,)),
        ] + plane_sems() + plane_sems() + [dma((k,)) for k in RowGather.SEMS],
        compiler_params=pltpu.CompilerParams(
            collective_id=0, has_side_effects=True, vmem_limit_bytes=67_043_328),
        cost_estimate=pl.CostEstimate(
            flops=29_000_000_000, bytes_accessed=16_000_000, transcendentals=0),
        name="layer",
    )(q, k, v, lg, gate, wo, stream, wg, wu, wd,
      bias.reshape(1, -1), extra.T, doc.reshape(1, -1), gain, ff_gain)


def per_device(
    stream, queries, projected_keys, values, decay_gate_logits, decay_gate_bias, extra_log_decay,
    document_index, output_gate, head_norm_gain, output_weight, feedforward_norm_gain,
    gate_weight, up_weight, down_weight,
):
    return layer(
        queries, projected_keys, values, decay_gate_logits, decay_gate_bias, extra_log_decay,
        document_index, output_gate, head_norm_gain, output_weight, stream,
        feedforward_norm_gain, gate_weight, up_weight, down_weight.T)


def solution(mesh):
    torus = Mesh(mesh.devices.reshape(4, 4, 2, mesh.shape["tp"]), ("sp_0", "sp_1", "sp_2", "tp"))
    placed = (
        P(SP, None), P(SP, "tp"), P(SP, "tp"), P(SP, "tp"), P(SP, "tp"), P("tp"), P(SP, "tp"),
        P(SP), P(SP, "tp"), P(), P("tp", None), P(), P(SP, "tp"), P(SP, "tp"), P("tp", SP),
    )
    return jax.shard_map(
        per_device, mesh=torus, in_specs=placed, out_specs=P(SP_TP, None), check_vma=False
    )
```

```python
import functools
import jax
import jax.numpy as jnp
from jax import lax
from jax.experimental import pallas as pl
from jax.experimental.pallas import tpu as pltpu
from jax.sharding import Mesh
from jax.sharding import PartitionSpec as P

SP = ("sp_0", "sp_1", "sp_2")
SP_TP = ("sp_0", "sp_1", "sp_2", "tp")
MESH = pl.DeviceIdType.MESH
F32 = jnp.float32
BF16 = jnp.bfloat16
TAU = 16.0
EPS = 1e-06
BL = 64
GR = 256
DK = 128
DV = 256
NZ, NY = 4, 4
NCHIP = NZ * NY


def nt_dot(a, b):
    return lax.dot_general(a, b, (((1,), (1,)), ((), ())), preferred_element_type=F32)


def tn_dot(a, b):
    return lax.dot_general(a, b, (((0,), (0,)), ((), ())), preferred_element_type=F32)


def nn_dot(a, b):
    return lax.dot_general(a, b, (((1,), (0,)), ((), ())), preferred_element_type=F32)


def remote_copy(src, dst, send, recv, target):
    return pltpu.make_async_remote_copy(
        src, dst, send, recv, device_id=target, device_id_type=MESH)


class PlaneGather:
    SEMS = (40, 40, 32, 32, 1)

    def __init__(self, src, dst, sems):
        self.src, self.dst = src, dst
        self.send, self.recv, self.core_send, self.core_recv, self.local = sems
        self.at = {"z": lax.axis_index("sp_0"), "y": lax.axis_index("sp_1")}
        self.core, self.x = lax.axis_index("sp_2"), lax.axis_index("tp")
        self.rows = src.shape[0] // 2

    def shifted(self, moves):
        at = dict(self.at)
        for axis, k in moves:
            at[axis] = lax.rem(at[axis] + (k + 4), 4)
        return at["z"], at["y"]

    def chip_at(self, axis, k):
        z, y = self.shifted([(axis, k)])
        return z, y, self.core, self.x

    def piece(self, hf, ja, jb, sub=None):
        a, b = ("y", "z") if hf == 0 else ("z", "y")
        z, y = self.shifted([(a, ja), (b, jb)])
        row = ((z * NY + y) * 2 + self.core) * (2 * self.rows) + hf * self.rows
        size = self.rows
        if sub is not None:
            size = size // 2
            row = row + sub * size
        return self.dst.at[pl.ds(pl.multiple_of(row, 16), size)]

    def axis(self, hf, stage):
        return ("y", "z")[(hf + stage) % 2]

    OFFS = (0, -1, 1, 2)

    def hop(self, hf, stage, ja, way, forward):
        axis = self.axis(hf, stage)
        k = hf * 20 + (0 if stage == 0 else 4 + 4 * self.OFFS.index(ja)) + (0 if way > 0 else 1)
        k = k + (2 if forward else 0)
        target = self.chip_at(axis, way)
        if forward:
            sub = 0 if way > 0 else 1
            ref = self.piece(hf, -way, 0, sub) if stage == 0 else self.piece(hf, ja, -way, sub)
            src = ref
        else:
            ref = self.piece(hf, 0, 0) if stage == 0 else self.piece(hf, ja, 0)
            own = stage == 0 or ja == 0
            src = self.src.at[pl.ds(hf * self.rows, self.rows)] if own else ref
        return remote_copy(src, ref, self.send.at[k], self.recv.at[k], target)

    def landing(self, hf, stage, ja, way, forward):
        axis = self.axis(hf, stage)
        k = hf * 20 + (0 if stage == 0 else 4 + 4 * self.OFFS.index(ja)) + (0 if way > 0 else 1)
        k = k + (2 if forward else 0)
        back = 2 if forward else -way
        sub = (0 if way > 0 else 1) if forward else None
        ref = self.piece(hf, back, 0, sub) if stage == 0 else self.piece(hf, ja, back, sub)
        return remote_copy(ref, ref, self.send.at[k], self.recv.at[k], self.chip_at(axis, way))

    def hand(self, hf, ja, jb):
        p = hf * 16 + self.OFFS.index(ja) * 4 + self.OFFS.index(jb)
        ref = self.piece(hf, ja, jb)
        src = self.src.at[pl.ds(hf * self.rows, self.rows)] if ja == 0 and jb == 0 else ref
        partner = (self.at["z"], self.at["y"], 1 - self.core, self.x)
        return remote_copy(src, ref, self.core_send.at[p], self.core_recv.at[p], partner)

    def handed(self, hf, ja, jb):
        p = hf * 16 + self.OFFS.index(ja) * 4 + self.OFFS.index(jb)
        a, b = ("y", "z") if hf == 0 else ("z", "y")
        z, y = self.shifted([(a, ja), (b, jb)])
        row = ((z * NY + y) * 2 + 1 - self.core) * (2 * self.rows) + hf * self.rows
        ref = self.dst.at[pl.ds(pl.multiple_of(row, 16), self.rows)]
        partner = (self.at["z"], self.at["y"], 1 - self.core, self.x)
        return remote_copy(ref, ref, self.core_send.at[p], self.core_recv.at[p], partner)

    def keep(self):
        row = ((self.at["z"] * NY + self.at["y"]) * 2 + self.core) * (2 * self.rows)
        return pltpu.make_async_copy(
            self.src, self.dst.at[pl.ds(pl.multiple_of(row, 16), 2 * self.rows)], self.local.at[0])

    def start(self):
        for stage in range(2):
            for hf in range(2):
                for way in (1, -1):
                    self.hop(hf, stage, 0, way, False).start()
        for hf in range(2):
            self.hand(hf, 0, 0).start()
        self.keep().start()

    def second(self, hf, ja):
        for way in (1, -1):
            self.hop(hf, 1, ja, way, False).start()
        self.hand(hf, ja, 0).start()

    def near(self):
        for way in (1, -1):
            for hf in range(2):
                self.landing(hf, 0, 0, way, False).wait_recv()
                self.hop(hf, 0, 0, way, True).start()

    def near_second(self, hf):
        for way in (1, -1):
            self.second(hf, -way)

    def far(self):
        for hf in range(2):
            for way in (1, -1):
                self.landing(hf, 0, 0, way, True).wait_recv()
            self.second(hf, 2)

    def column(self, ja):
        for way in (1, -1):
            for hf in range(2):
                self.landing(hf, 1, ja, way, False).wait_recv()
                self.hop(hf, 1, ja, way, True).start()
                self.hand(hf, ja, -way).start()

    def column_far(self, ja):
        for hf in range(2):
            for way in (1, -1):
                self.landing(hf, 1, ja, way, True).wait_recv()
            self.hand(hf, ja, 2).start()

    def finish(self):
        self.keep().wait()
        for hf in range(2):
            for ja in self.OFFS:
                for jb in self.OFFS:
                    self.handed(hf, ja, jb).wait_recv()

    def drain(self):
        for hf in range(2):
            for way in (1, -1):
                for forward in (False, True):
                    self.hop(hf, 0, 0, way, forward).wait_send()
                    for ja in self.OFFS:
                        self.hop(hf, 1, ja, way, forward).wait_send()
            for ja in self.OFFS:
                for jb in self.OFFS:
                    self.hand(hf, ja, jb).wait_send()


class RowGather:
    SEMS = (6, 6, 3, 3)

    def __init__(self, rows, dst, sems):
        self.dst = dst
        self.send, self.recv, self.core_send, self.core_recv = sems
        self.z, self.y = lax.axis_index("sp_0"), lax.axis_index("sp_1")
        self.core, self.x = lax.axis_index("sp_2"), lax.axis_index("tp")
        self.rows = rows

    def piece(self, k, core, sub=None):
        size = self.rows // 2
        row = lax.rem(self.x + (k + 4), 4) * self.rows + core * size
        if sub is not None:
            size = size // 2
            row = row + sub * size
        return self.dst.at[pl.ds(pl.multiple_of(row, 16), size)]

    def side(self, way):
        return (self.z, self.y, self.core, lax.rem(self.x + (way + 4), 4))

    def copy(self, ref, k, way):
        return remote_copy(ref, ref, self.send.at[k], self.recv.at[k], self.side(way))

    def key(self, way, part):
        return (0 if way > 0 else 1) + 2 * part

    def hop(self, way, part):
        first = 0 if way > 0 else 1
        if part == 2:
            ref = self.piece(-way, self.core, first)
        else:
            ref = self.piece(0, self.core, first if part == 0 else 1 - first)
        return self.copy(ref, self.key(way, part), way)

    def landing(self, way, part):
        first = 0 if way > 0 else 1
        if part == 2:
            ref = self.piece(2, self.core, first)
        else:
            ref = self.piece(-way, self.core, first if part == 0 else 1 - first)
        return self.copy(ref, self.key(way, part), way)

    def hand(self, i, arriving=False):
        k = (-1, 1, 2)[i]
        ref = self.piece(k, 1 - self.core if arriving else self.core)
        return remote_copy(
            ref, ref, self.core_send.at[i], self.core_recv.at[i], (self.z, self.y, 1 - self.core, self.x))

    def start(self):
        for part in range(2):
            for way in (1, -1):
                self.hop(way, part).start()

    def near(self):
        for way in (1, -1):
            self.landing(way, 0).wait_recv()
            self.hop(way, 2).start()

    def near_hand(self):
        for i, way in enumerate((1, -1)):
            self.landing(way, 1).wait_recv()
            self.hand(i).start()

    def far(self):
        for way in (1, -1):
            self.landing(way, 2).wait_recv()
        self.hand(2).start()

    def finish(self):
        for i in range(3):
            self.hand(i, True).wait_recv()

    def drain(self):
        for way in (1, -1):
            for part in range(3):
                self.hop(way, part).wait_send()
        for i in range(3):
            self.hand(i).wait_send()


def plane_sems():
    return [pltpu.SemaphoreType.DMA((k,)) for k in PlaneGather.SEMS]


def layer_kernel(
    q_in, k_in, v_in, lg_in, gate_in, wo_in, stream_in, wg_in, wu_in, wd_in,
    bias_ref, extra_ref, doc_ref, gain_ref, ff_gain_ref,
    out_ref,
    q_ref, k_ref, v_ref, lg_ref, gate_ref, aux_ref, wg_ref, wu_ref, shard_ref, wd_ref,
    cum_ref, blk_ref, off_ref, states_ref, before_ref, run_ref, local_ref,
    own_t, own_e, part_t, part_e, chip_t, chip_e, ry_t, ry_e, row_t, row_e, rz_t, rz_e, mine_c, send_c, part_c, sum_ref,
    hm, st, wo_v, w_v, down_v, resid, normed, hidden, s2, s1, s3, ra, rb, rl, rr,
    local_sem, core_send, core_recv, t_send, t_recv, e_send, e_recv,
    own_rs, own_ls, fwd_rs, fwd_ls, left_in, right_in, opp_l, opp_r, rs_send, rs_recv,
    *gather_sems,
):
    rows = q_ref.shape[0]
    blocks = rows // BL
    groups = rows // GR
    per = GR // BL
    z, y = lax.axis_index("sp_0"), lax.axis_index("sp_1")
    core, me = lax.axis_index("sp_2"), lax.axis_index("tp")
    scale = DK ** (-0.5)
    n = 4
    q_rows = GR
    half = q_rows // 2
    d = out_ref.shape[1]
    units = hidden.shape[1]
    ix_r, ix_l = lax.rem(me + 1, n), lax.rem(me + n - 1, n)
    right, left = (z, y, core, ix_r), (z, y, core, ix_l)
    partner = (z, y, 1 - core, me)
    order = (2, 1, 3, 0)

    def quarter_of(owner, offset):
        return lax.rem(owner + offset, n)

    def along_y(k):
        return (z, lax.rem(y + k, NY), core, me)

    def along_z(k):
        return (lax.rem(z + k, NZ), y, core, me)

    wo_own = wo_in.shape[0]
    loads = {
        name: pltpu.make_async_copy(src, dst, local_sem.at[i])
        for i, (name, src, dst) in enumerate((
            ("wg", wg_in, wg_ref), ("wu", wu_in, wu_ref), ("wd", wd_in, wd_ref),
            ("wo", wo_in, wo_v.at[pl.ds(pl.multiple_of(me * wo_own, wo_own), wo_own)]),
            ("lg", lg_in, lg_ref), ("k", k_in, k_ref), ("v", v_in, v_ref), ("q", q_in, q_ref),
            ("gate", gate_in, gate_ref),
        ))
    }
    for copy in loads.values():
        copy.start()

    def load_stream(i):
        at = pl.multiple_of(quarter_of(me, order[i]) * q_rows, q_rows)
        return pltpu.make_async_copy(
            stream_in.at[pl.ds(at, q_rows)], st.at[i % 2], local_sem.at[9 + i])

    load_stream(0).start()
    load_stream(1).start()

    rz_t[pl.ds(z, 1)] = jnp.zeros((1, DV, DK), BF16)

    barrier = pltpu.get_barrier_semaphore()
    pl.semaphore_signal(barrier, inc=1, device_id=partner, device_id_type=MESH)
    pl.semaphore_signal(barrier, inc=1, device_id=right, device_id_type=MESH)
    pl.semaphore_signal(barrier, inc=1, device_id=left, device_id_type=MESH)
    for k in range(1, NY):
        pl.semaphore_signal(barrier, inc=1, device_id=along_y(k), device_id_type=MESH)
        pl.semaphore_signal(barrier, inc=1, device_id=along_z(k), device_id_type=MESH)

    loads["wg"].wait()
    loads["wu"].wait()
    for j in range(units // 128):
        shard_ref[:, j * 256 : j * 256 + 128] = wg_ref[:, j * 128 : (j + 1) * 128]
        shard_ref[:, j * 256 + 128 : (j + 1) * 256] = wu_ref[:, j * 128 : (j + 1) * 128]
    loads["wd"].wait()
    loads["wo"].wait()

    pl.semaphore_wait(barrier, 9)
    g1 = PlaneGather(shard_ref, w_v, gather_sems[:5])
    g2 = PlaneGather(wd_ref, down_v, gather_sems[5:10])
    ring = RowGather(wo_own, wo_v, gather_sems[10:])
    ring.start()
    g1.start()

    ri = lax.broadcasted_iota(jnp.int32, (GR, GR), 0)
    ci = lax.broadcasted_iota(jnp.int32, (GR, GR), 1)

    def columns(g, _):
        at = pl.multiple_of(g * GR, GR)
        for j in range(3):
            lanes = pl.ds(pl.multiple_of(g * GR, GR), GR)
            row = doc_ref[:, lanes].astype(F32) if j == 2 else extra_ref[j : j + 1, lanes]
            col = jnp.sum(jnp.where(ri == ci, row, 0.0), axis=1, keepdims=True)
            aux_ref[pl.ds(at, GR), j : j + 1] = col
        return 0

    lax.fori_loop(0, groups, columns, 0)
    loads["lg"].wait()
    loads["k"].wait()
    loads["v"].wait()
    run_ref[...] = jnp.zeros_like(run_ref)

    def doc_at(r):
        return aux_ref[pl.ds(r, 1), 2:3]

    def first(g, base):
        at = pl.multiple_of(g * GR, GR)
        same_block = (ri & (GR - BL)) == (ci & (GR - BL))
        tri = jnp.where(same_block & (ci <= ri), 1.0, 0.0).astype(BF16)
        logits = lg_ref[pl.ds(at, GR), :].astype(F32) + bias_ref[...]
        ld = (jnp.minimum(logits, 0.0) - jnp.log1p(jnp.exp(-jnp.abs(logits)))) / TAU
        extra0 = jnp.broadcast_to(aux_ref[pl.ds(at, GR), 0:1], (GR, DK))
        extra1 = jnp.broadcast_to(aux_ref[pl.ds(at, GR), 1:2], (GR, DK))
        ld = ld + jnp.concatenate([extra0, extra1], axis=1)
        hi = ld.astype(BF16)
        rest = ld - hi.astype(F32)
        mid = rest.astype(BF16)
        low = (rest - mid.astype(F32)).astype(BF16)
        cum = nn_dot(tri, hi) + nn_dot(tri, mid) + nn_dot(tri, low)
        cum_ref[pl.ds(at, GR), :] = cum
        cum3 = cum.reshape(per, BL, 2 * DK)
        ends = cum3[:, BL - 1 : BL, :]
        off = base
        for b in range(per):
            off_ref[pl.ds(g * per + b, 1)] = off[None]
            blk_ref[pl.ds(g * per + b, 1)] = ends[b : b + 1]
            off = off + ends[b]
        doc = aux_ref[pl.ds(at, GR), 2:3].reshape(per, BL, 1)
        tail_mask = jnp.where(doc == doc[:, BL - 1 : BL], 1.0, 0.0)
        head_mask = jnp.where(doc == doc[:, 0:1], 1.0, 0.0)
        kf = k_ref[pl.ds(at, GR), :].astype(F32).reshape(per, BL, 2 * DK)
        tail = (kf * jnp.exp(ends - cum3) * tail_mask).astype(BF16)
        head = (kf * jnp.exp(cum3) * head_mask).astype(BF16)
        for b in range(per):
            start = at + b * BL
            keep = jnp.where(doc_at(jnp.maximum(start - 1, 0)) == doc_at(start + BL - 1), 1.0, 0.0)
            decay = jnp.exp(ends[b]) * keep
            for h in range(2):
                c = slice(h * DK, (h + 1) * DK)
                keys = jnp.concatenate([tail[b][:, c], head[b][:, c]], axis=1)
                vals = v_ref[pl.ds(pl.multiple_of(start, BL), BL), h * DV : (h + 1) * DV]
                both = tn_dot(vals, keys)
                slot = (g * per + b) * 2 + h
                states_ref[pl.ds(slot, 1)] = both[None, :, DK:]
                fw = run_ref[h, :, :DK]
                before_ref[pl.ds(slot, 1), :, :DK] = fw.astype(BF16)[None]
                run_ref[h, :, :DK] = fw * decay[:, c] + both[:, :DK]
        return off

    total = lax.fori_loop(0, groups, first, jnp.zeros((1, 2 * DK), F32))
    sum_ref[...] = total

    def step(b, _):
        r = blocks - 1 - b
        hi = jnp.minimum(r * BL + BL, rows - 1)
        keep = jnp.where(doc_at(hi) == doc_at(r * BL), 1.0, 0.0)
        decay = jnp.exp(blk_ref[pl.ds(r, 1)][0]) * keep
        for h in range(2):
            bw = run_ref[h, :, DK:]
            before_ref[pl.ds(r * 2 + h, 1), :, DK:] = bw.astype(BF16)[None]
            run_ref[h, :, DK:] = bw * decay[:, h * DK : (h + 1) * DK] + states_ref[r * 2 + h]
        return 0

    lax.fori_loop(0, blocks, step, 0)
    first_doc = jnp.broadcast_to(doc_at(0), (1, DK))
    last_doc = jnp.broadcast_to(doc_at(rows - 1), (1, DK))
    for h in range(2):
        own_t[h, :DV] = run_ref[h, :, :DK].astype(BF16)
        own_t[h, DV:] = run_ref[h, :, DK:].astype(BF16)
        own_e[h, 0:1] = total[:, h * DK : (h + 1) * DK]
        own_e[h, 1:2] = first_doc
        own_e[h, 2:3] = last_doc
        own_e[h, 3:8] = jnp.zeros((5, DK), F32)

    g1.near()
    swap_t = pltpu.make_async_remote_copy(
        own_t.at[1 - core], part_t, core_send.at[0], core_recv.at[0],
        device_id=partner, device_id_type=MESH)
    swap_e = pltpu.make_async_remote_copy(
        own_e.at[1 - core], part_e, core_send.at[1], core_recv.at[1],
        device_id=partner, device_id_type=MESH)
    swap_t.start()
    swap_e.start()
    swap_t.wait()
    swap_e.wait()
    is0 = core == 0
    mine_e = own_e[pl.ds(core, 1)][0]
    other_e = part_e[...]
    e0 = jnp.where(is0, mine_e, other_e)
    e1 = jnp.where(is0, other_e, mine_e)
    mine_t = own_t[pl.ds(core, 1)][0].astype(F32)
    other_t = part_t[...].astype(F32)
    t0 = jnp.where(is0, mine_t, other_t)
    t1 = jnp.where(is0, other_t, mine_t)
    through1 = jnp.exp(e1[0:1]) * jnp.where(e0[2:3] == e1[2:3], 1.0, 0.0)
    through0 = jnp.exp(e0[0:1]) * jnp.where(e1[1:2] == e0[1:2], 1.0, 0.0)
    chip_t[0] = (t1[:DV] + through1 * t0[:DV]).astype(BF16)
    chip_t[1] = (t0[DV:] + through0 * t1[DV:]).astype(BF16)
    chip_row = jnp.concatenate(
        [e0[0:1] + e1[0:1], e0[1:2], e1[2:3], jnp.zeros((5, DK), F32)], axis=0)
    chip_e[...] = chip_row
    ry_e[pl.ds(y, 1)] = chip_row[None]
    ry_t[pl.ds(y, 1)] = chip_t[...][None]

    y_sends = []
    for k in range(1, NY):
        y_sends.append(remote_copy(chip_e, ry_e.at[y], e_send.at[k], e_recv.at[k], along_y(k)))
        y_sends.append(remote_copy(chip_t, ry_t.at[y], t_send.at[k], t_recv.at[k], along_y(k)))
    for s in y_sends:
        s.start()
    g1.near_second(0)
    g2.start()
    loads["q"].wait()

    def inside(g, _):
        at = pl.multiple_of(g * GR, GR)
        same_block = (ri & (GR - BL)) == (ci & (GR - BL))
        doc = aux_ref[pl.ds(at, GR), 2:3]
        same = same_block & (doc == doc_ref[:, pl.ds(at, GR)].astype(F32))
        below = same & (ci <= ri)
        above = same & (ci >= ri)
        cum3 = cum_ref[pl.ds(at, GR), :].reshape(per, BL, 2 * DK)
        middle = cum3[:, BL // 2 - 1 : BL // 2]
        ends = cum3[:, BL - 1 : BL]
        rising = jnp.exp(cum3 - middle)
        falling = jnp.exp(middle - cum3)
        qf = q_ref[pl.ds(at, GR), :].astype(F32).reshape(per, BL, 2 * DK) * scale
        kf = k_ref[pl.ds(at, GR), :].astype(F32).reshape(per, BL, 2 * DK)
        q_rise = (qf * rising).astype(BF16).reshape(GR, 2 * DK)
        q_fall = (qf * falling).astype(BF16).reshape(GR, 2 * DK)
        k_rise = (kf * rising).astype(BF16).reshape(GR, 2 * DK)
        k_fall = (kf * falling).astype(BF16).reshape(GR, 2 * DK)
        q_fwd = qf * jnp.exp(cum3)
        q_bwd = qf * jnp.exp(ends - cum3)
        for h in range(2):
            c = slice(h * DK, (h + 1) * DK)
            fw = nt_dot(q_rise[:, c], k_fall[:, c])
            bw = nt_dot(q_fall[:, c], k_rise[:, c])
            scores = jnp.where(below, fw, 0.0) + jnp.where(above, bw, 0.0)
            vals = v_ref[pl.ds(at, GR), h * DV : (h + 1) * DV]
            local_ref[pl.ds(at, GR), h * DV : (h + 1) * DV] = nn_dot(scores.astype(BF16), vals)
        for b in range(per):
            start = at + b * BL
            prev = doc_at(jnp.maximum(start - 1, 0))
            following = doc_at(jnp.minimum(start + BL, rows - 1))
            rows_doc = doc[b * BL : (b + 1) * BL]
            hit_f = jnp.where(rows_doc == prev, 1.0, 0.0)
            hit_b = jnp.where(rows_doc == following, 1.0, 0.0)
            for h in range(2):
                c = slice(h * DK, (h + 1) * DK)
                both = jnp.concatenate([q_fwd[b][:, c] * hit_f, q_bwd[b][:, c] * hit_b], axis=1)
                here = pl.ds(pl.multiple_of(start, BL), BL)
                local_ref[here, h * DV : (h + 1) * DV] += nt_dot(
                    both.astype(BF16), before_ref[(g * per + b) * 2 + h])
        return 0

    lax.fori_loop(0, groups // 2, inside, 0)
    g1.column(0)
    lax.fori_loop(groups // 2, groups, inside, 0)

    ring.near()
    for s in y_sends:
        s.wait()
    run_ref[0] = jnp.zeros_like(run_ref[0])

    def earlier(states, table):
        def body(j, _):
            e = table[j]
            p = table[jnp.maximum(j - 1, 0)]
            keep = jnp.exp(e[0:1]) * jnp.where(e[2:3] == p[2:3], 1.0, 0.0)
            run_ref[0, :, :DK] = states(j, 0).astype(F32) + run_ref[0, :, :DK] * keep
            return 0
        return body

    def later(states, table):
        def body(i, _):
            j = NY - 1 - i
            e = table[j]
            p = table[jnp.minimum(j + 1, NY - 1)]
            keep = jnp.exp(e[0:1]) * jnp.where(e[1:2] == p[1:2], 1.0, 0.0)
            run_ref[0, :, DK:] = states(j, 1).astype(F32) + run_ref[0, :, DK:] * keep
            return 0
        return body

    def row_state(j, way):
        return ry_t[j, way]

    def column_state(j, way):
        return rz_t[j]

    lax.fori_loop(0, y, earlier(row_state, ry_e), 0)
    lax.fori_loop(0, NY - 1 - y, later(row_state, ry_e), 0)
    run_ref[1] = run_ref[0]
    lax.fori_loop(y, NY, earlier(row_state, ry_e), 0)
    lax.fori_loop(NY - 1 - y, NY, later(row_state, ry_e), 0)
    row_t[0] = run_ref[0, :, :DK].astype(BF16)
    row_t[1] = run_ref[0, :, DK:].astype(BF16)
    in_row = [ry_e[j] for j in range(NY)]
    row_sum = in_row[0][0:1] + in_row[1][0:1] + in_row[2][0:1] + in_row[3][0:1]
    sum_before = jnp.zeros((1, DK), F32)
    sum_after = jnp.zeros((1, DK), F32)
    for j in range(NY):
        sum_before = sum_before + jnp.where(j < y, in_row[j][0:1], 0.0)
        sum_after = sum_after + jnp.where(j > y, in_row[j][0:1], 0.0)
    last_before = ry_e[jnp.maximum(y - 1, 0)][2:3]
    first_after = ry_e[jnp.minimum(y + 1, NY - 1)][1:2]
    row_row = jnp.concatenate(
        [row_sum, in_row[0][1:2], in_row[NY - 1][2:3], jnp.zeros((5, DK), F32)], axis=0)
    row_e[...] = row_row
    rz_e[pl.ds(z, 1)] = row_row[None]
    z_sends = []
    for k in range(1, NZ):
        back = jnp.where(lax.rem(z + k, NZ) > z, 0, 1)
        z_sends.append(
            remote_copy(row_e, rz_e.at[z], e_send.at[4 + k], e_recv.at[4 + k], along_z(k)))
        z_sends.append(
            remote_copy(row_t.at[back], rz_t.at[z], t_send.at[4 + k], t_recv.at[4 + k], along_z(k)))
    for s in z_sends:
        s.start()
    g1.near_second(1)
    g1.far()
    for s in z_sends:
        s.wait()
    g2.near()
    g2.near_second(0)
    g2.near_second(1)

    run_ref[0] = jnp.zeros_like(run_ref[0])
    lax.fori_loop(0, z, earlier(column_state, rz_e), 0)
    lax.fori_loop(0, NZ - 1 - z, later(column_state, rz_e), 0)
    prev_last = jnp.where(z > 0, rz_e[jnp.maximum(z - 1, 0)][2:3], -1.0)
    next_first = jnp.where(z < NZ - 1, rz_e[jnp.minimum(z + 1, NZ - 1)][1:2], -1.0)
    pass_f = jnp.exp(sum_before) * jnp.where(
        y == 0, 1.0, jnp.where(prev_last == last_before, 1.0, 0.0))
    pass_b = jnp.exp(sum_after) * jnp.where(
        y == NY - 1, 1.0, jnp.where(next_first == first_after, 1.0, 0.0))
    cf = run_ref[1, :, :DK] + pass_f * run_ref[0, :, :DK]
    cb = run_ref[1, :, DK:] + pass_b * run_ref[0, :, DK:]
    before_doc = jnp.where(y > 0, last_before, prev_last)
    after_doc = jnp.where(y < NY - 1, first_after, next_first)
    pass0 = jnp.exp(e0[0:1]) * jnp.where(before_doc == e0[2:3], 1.0, 0.0)
    pass1 = jnp.exp(e1[0:1]) * jnp.where(after_doc == e1[1:2], 1.0, 0.0)
    mine_t = own_t[pl.ds(core, 1)][0].astype(F32)
    other_t = part_t[...].astype(F32)
    t0f = jnp.where(is0, mine_t[:DV], other_t[:DV])
    t1b = jnp.where(is0, other_t[DV:], mine_t[DV:])
    c0 = jnp.concatenate([cf, t1b + pass1 * cb], axis=1)
    c1 = jnp.concatenate([t0f + pass0 * cf, cb], axis=1)
    mine_c[...] = jnp.where(is0, c0, c1).astype(BF16)
    send_c[...] = jnp.where(is0, c1, c0).astype(BF16)
    swap_c = pltpu.make_async_remote_copy(
        send_c, part_c, core_send.at[2], core_recv.at[2],
        device_id=partner, device_id_type=MESH)
    swap_c.start()
    ring.near_hand()
    enter_f = jnp.where(is0, before_doc, e0[2:3])[:, 0:1]
    enter_b = jnp.where(is0, e1[1:2], after_doc)[:, 0:1]
    swap_c.wait()

    loads["gate"].wait()

    def last(g):
        at = pl.multiple_of(g * GR, GR)
        doc = aux_ref[pl.ds(at, GR), 2:3]
        hit_f = jnp.where(doc == enter_f, 1.0, 0.0)
        hit_b = jnp.where(doc == enter_b, 1.0, 0.0)
        glob = cum_ref[pl.ds(at, GR), :].reshape(per, BL, 2 * DK) + off_ref[pl.ds(g * per, per)]
        glob = glob.reshape(GR, 2 * DK)
        qf = q_ref[pl.ds(at, GR), :].astype(F32) * scale
        q_fwd = (qf * jnp.exp(glob) * hit_f).astype(BF16)
        q_bwd = (qf * jnp.exp(sum_ref[...] - glob) * hit_b).astype(BF16)
        gain = gain_ref[...].astype(F32).reshape(1, DV)
        for h in range(2):
            c = slice(h * DK, (h + 1) * DK)
            both = jnp.concatenate([q_fwd[:, c], q_bwd[:, c]], axis=1)
            carry = jnp.where(h == core, mine_c[...], part_c[...])
            out = local_ref[pl.ds(at, GR), h * DV : (h + 1) * DV] + nt_dot(both, carry)
            out = out * lax.rsqrt(jnp.mean(out * out, axis=-1, keepdims=True) + EPS) * gain
            u = gate_ref[pl.ds(at, GR), h * DV : (h + 1) * DV].astype(F32)
            hm[pl.ds(at, GR), pl.ds(pl.multiple_of(me * 2 * DV + h * DV, DV), DV)] = (
                out * (u / (1.0 + jnp.exp(-u)))).astype(BF16)

    def three(i, _):
        last(quarter_of(me, i + i // 2))
        return 0

    lax.fori_loop(0, 3, three, 0)

    def piece(slot, r, part):
        return hm.at[
            pl.ds(pl.multiple_of(r * q_rows + part * half, half), half),
            pl.ds(pl.multiple_of(slot * 2 * DV, 2 * DV), 2 * DV)]

    def remote(ref, send, recv, target, dst=None):
        return pltpu.make_async_remote_copy(
            ref, ref if dst is None else dst, send, recv, device_id=target, device_id_type=MESH)

    def wire(slot, quarter, part, send, recv, target):
        return remote(piece(slot, quarter, part), send, recv, target)

    to_right = (((0, 0), (3, 0), (3, 1)), ((2, 0), (2, 1)), ((1, 0), (0, 1)), ((1, 1),))
    to_left = (((0, 1), (1, 1), (1, 0)), ((3, 1), (0, 0)), ((2, 1), (2, 0)), ((3, 0),))

    def own_right(o, p):
        return wire(me, quarter_of(me, o), p, own_rs.at[o * 2 + p], left_in.at[o * 2 + p], right)

    def own_left(o, p):
        return wire(me, quarter_of(me, o), p, own_ls.at[o * 2 + p], right_in.at[o * 2 + p], left)

    def came_left(o, p):
        return wire(ix_l, quarter_of(ix_l, o), p, own_rs.at[o * 2 + p], left_in.at[o * 2 + p], right)

    def came_right(o, p):
        return wire(ix_r, quarter_of(ix_r, o), p, own_ls.at[o * 2 + p], right_in.at[o * 2 + p], left)

    def fwd_right(i):
        return wire(ix_l, quarter_of(ix_r, order[i]), 0, fwd_rs.at[i], opp_l.at[i], right)

    def fwd_left(i):
        return wire(ix_r, quarter_of(ix_l, order[i]), 1, fwd_ls.at[i], opp_r.at[i], left)

    opposite = lax.rem(me + 2, n)

    def came_opp_l(i):
        return wire(opposite, quarter_of(me, order[i]), 0, fwd_rs.at[i], opp_l.at[i], right)

    def came_opp_r(i):
        return wire(opposite, quarter_of(me, order[i]), 1, fwd_ls.at[i], opp_r.at[i], left)

    def send_own(i):
        for k in range(len(to_right[i])):
            own_right(*to_right[i][k]).start()
            own_left(*to_left[i][k]).start()

    seen = set()

    def arrived(side, o, p):
        if (side, o, p) not in seen:
            seen.add((side, o, p))
            (came_left if side == "l" else came_right)(o, p).wait_recv()

    def pump(i):
        arrived("l", (2 + order[i]) % n, 0)
        fwd_right(i).start()
        arrived("r", (n - 2 + order[i]) % n, 1)
        fwd_left(i).start()

    send_own(0)
    last(quarter_of(me, 2))
    for ja in (-1, 1):
        g1.column(ja)
    g2.column(0)
    ring.far()
    pump(0)
    send_own(1)
    g1.column(2)
    g2.far()
    send_own(2)
    for ja in (0, -1, 1):
        g1.column_far(ja)
    for ja in (-1, 1):
        g2.column(ja)
    ring.finish()

    dh = d // 2
    to_r_a = remote(s2.at[:, pl.ds(0, dh)], rs_send.at[0], rs_recv.at[0], right, ra)
    to_l_b = remote(s2.at[:, pl.ds(dh, dh)], rs_send.at[1], rs_recv.at[1], left, rb)
    lo, up = pl.ds(0, dh), pl.ds(dh, dh)
    to_r = remote(s1.at[:, up], rs_send.at[2], rs_recv.at[2], right, rl.at[:, up])
    to_l = remote(s3.at[:, lo], rs_send.at[3], rs_recv.at[3], left, rr.at[:, lo])
    to_r_sum = remote(s1.at[:, lo], rs_send.at[4], rs_recv.at[4], right, rl.at[:, lo])
    to_l_sum = remote(s3.at[:, up], rs_send.at[5], rs_recv.at[5], left, rr.at[:, up])

    def prepare(i):
        at = pl.multiple_of(quarter_of(me, order[i]) * q_rows, q_rows)
        rows = pl.ds(at, q_rows)
        for p in range(2):
            arrived("l", (1 + order[i]) % n, p)
            arrived("r", (n - 1 + order[i]) % n, p)
        came_opp_l(i).wait_recv()
        came_opp_r(i).wait_recv()
        load_stream(i).wait()

        def project(j, total):
            cols = pl.ds(pl.multiple_of(j * 1024, 1024), 1024)
            acc = st[i % 2, :, cols].astype(F32) + nn_dot(hm[rows, :], wo_v[:, cols])
            resid[:, cols] = acc
            return total + jnp.sum(acc * acc, axis=-1, keepdims=True)

        squares = lax.fori_loop(0, d // 1024, project, jnp.zeros((q_rows, 1), F32))
        if i < n - 2:
            load_stream(i + 2).start()
        factor = lax.rsqrt(squares / d + EPS)
        normed[...] = (resid[...] * factor * ff_gain_ref[...].astype(F32).reshape(1, d)).astype(BF16)

    prepare(0)
    pump(1)
    send_own(3)
    g2.column(2)
    g1.column_far(2)
    for ja in (0, -1, 1):
        g2.column_far(ja)
    for i in range(n):
        if i == 0:
            g1.finish()
        else:
            prepare(i)

        def gate_up(at, width):
            both = nn_dot(normed[...], w_v[:, pl.ds(pl.multiple_of(at * 2, 256), 2 * width)])
            for b in range(width // 128):
                g = both[:, b * 256 : b * 256 + 128]
                u = both[:, b * 256 + 128 : (b + 1) * 256]
                hidden[:, pl.ds(pl.multiple_of(at + b * 128, 128), 128)] = (
                    g / (1.0 + jnp.exp(-g)) * u).astype(BF16)

        def gate_up_pair(j, _):
            gate_up(j * 256, 256)
            return 0

        lax.fori_loop(0, units // 256, gate_up_pair, 0)
        gate_up(units // 256 * 256, units % 256)
        if i == 0:
            g2.column_far(2)
            pump(2)
            pump(3)
            g2.finish()
        target = (s2, s1, s3, resid)[i]

        def down(j, _):
            cols = pl.ds(pl.multiple_of(j * 512, 512), 512)
            part = nt_dot(hidden[...], down_v[cols, :]).astype(BF16)
            if i < n - 1:
                target[:, cols] = part
            else:
                target[:, cols] = target[:, cols] + part.astype(F32)
            return 0

        tiles = d // 1024
        first_half, second_half = ((tiles, 2 * tiles), (0, tiles)) if i == 1 else (
            (0, tiles), (tiles, 2 * tiles))
        lax.fori_loop(*first_half, down, 0)
        if i == 0:
            to_r_a.start()
        if i == 1:
            to_r.start()
        if i == 2:
            to_l.start()
            to_r_a.wait_recv()
            s1[:, :dh] = (s1[:, :dh].astype(F32) + ra[...].astype(F32)).astype(BF16)
            to_r_sum.start()
        lax.fori_loop(*second_half, down, 0)
        if i == 0:
            to_l_b.start()
        if i == 2:
            to_l_b.wait_recv()
            s3[:, dh:] = (s3[:, dh:].astype(F32) + rb[...].astype(F32)).astype(BF16)
            to_l_sum.start()

    to_r.wait_recv()
    to_l.wait_recv()
    to_r_sum.wait_recv()
    to_l_sum.wait_recv()
    out_ref[...] = (resid[...] + rl[...].astype(F32) + rr[...].astype(F32)).astype(BF16)

    for o in range(n):
        for p in range(2):
            own_right(o, p).wait_send()
            own_left(o, p).wait_send()
    for i in range(n):
        fwd_right(i).wait_send()
        fwd_left(i).wait_send()
    g1.drain()
    g2.drain()
    ring.drain()
    to_r_a.wait_send()
    to_l_b.wait_send()
    to_r.wait_send()
    to_l.wait_send()
    to_r_sum.wait_send()
    to_l_sum.wait_send()


def layer(q, k, v, lg, bias, extra, doc, gate, gain, wo, stream, ff_gain, wg, wu, wd):
    rows, d = stream.shape
    units = wg.shape[1]
    vm = pl.BlockSpec(memory_space=pltpu.VMEM)
    hbm = pl.BlockSpec(memory_space=pl.ANY)
    blocks = rows // BL
    dma = pltpu.SemaphoreType.DMA

    def buf(*shape, dtype=BF16):
        return pltpu.VMEM(shape, dtype)

    return pl.pallas_call(
        layer_kernel,
        out_shape=jax.ShapeDtypeStruct((GR, d), BF16),
        in_specs=[hbm] * 10 + [vm] * 5,
        out_specs=vm,
        scratch_shapes=[
            buf(rows, 2 * DK), buf(rows, 2 * DK), buf(rows, 2 * DV), buf(rows, 2 * DK),
            buf(rows, 2 * DV), buf(rows, 3, dtype=F32),
            buf(*wg.shape), buf(*wu.shape), buf(wg.shape[0], 2 * units), buf(*wd.shape),
            buf(rows, 2 * DK, dtype=F32),
            buf(blocks, 1, 2 * DK, dtype=F32),
            buf(blocks, 1, 2 * DK, dtype=F32),
            buf(blocks * 2, DV, DK, dtype=F32),
            buf(blocks * 2, DV, 2 * DK),
            buf(2, DV, 2 * DK, dtype=F32),
            buf(rows, 2 * DV, dtype=F32),
            buf(2, 2 * DV, DK), buf(2, 8, DK, dtype=F32),
            buf(2 * DV, DK), buf(8, DK, dtype=F32),
            buf(2, DV, DK), buf(8, DK, dtype=F32),
            buf(NY, 2, DV, DK), buf(NY, 8, DK, dtype=F32),
            buf(2, DV, DK), buf(8, DK, dtype=F32),
            buf(NZ, DV, DK), buf(NZ, 8, DK, dtype=F32),
            buf(DV, 2 * DK), buf(DV, 2 * DK), buf(DV, 2 * DK),
            buf(1, 2 * DK, dtype=F32),
            buf(rows, 4 * 2 * DV), buf(2, GR, d), buf(4 * wo.shape[0], d),
            buf(2 * NCHIP * wg.shape[0], 2 * units), buf(2 * NCHIP * wd.shape[0], units),
            buf(GR, d, dtype=F32), buf(GR, d), buf(GR, units),
            buf(GR, d), buf(GR, d), buf(GR, d), buf(GR, d // 2), buf(GR, d // 2), buf(GR, d), buf(GR, d),
            dma((13,)), dma((3,)), dma((3,)),
            dma((8,)), dma((8,)), dma((8,)), dma((8,)),
            dma((8,)), dma((8,)), dma((4,)), dma((4,)),
            dma((8,)), dma((8,)), dma((4,)), dma((4,)), dma((6,)), dma((6,)),
        ] + plane_sems() + plane_sems() + [dma((k,)) for k in RowGather.SEMS],
        compiler_params=pltpu.CompilerParams(
            collective_id=0, has_side_effects=True, vmem_limit_bytes=67_043_328),
        cost_estimate=pl.CostEstimate(
            flops=29_000_000_000, bytes_accessed=16_000_000, transcendentals=0),
        name="layer",
    )(q, k, v, lg, gate, wo, stream, wg, wu, wd,
      bias.reshape(1, -1), extra.T, doc.reshape(1, -1), gain, ff_gain)


def per_device(
    stream, queries, projected_keys, values, decay_gate_logits, decay_gate_bias, extra_log_decay,
    document_index, output_gate, head_norm_gain, output_weight, feedforward_norm_gain,
    gate_weight, up_weight, down_weight,
):
    return layer(
        queries, projected_keys, values, decay_gate_logits, decay_gate_bias, extra_log_decay,
        document_index, output_gate, head_norm_gain, output_weight, stream,
        feedforward_norm_gain, gate_weight, up_weight, down_weight.T)


def solution(mesh):
    torus = Mesh(mesh.devices.reshape(4, 4, 2, mesh.shape["tp"]), ("sp_0", "sp_1", "sp_2", "tp"))
    placed = (
        P(SP, None), P(SP, "tp"), P(SP, "tp"), P(SP, "tp"), P(SP, "tp"), P("tp"), P(SP, "tp"),
        P(SP), P(SP, "tp"), P(), P("tp", None), P(), P(SP, "tp"), P(SP, "tp"), P("tp", SP),
    )
    return jax.shard_map(
        per_device, mesh=torus, in_specs=placed, out_specs=P(SP_TP, None), check_vma=False
    )
```

```python
import functools
import jax
import jax.numpy as jnp
from jax import lax
from jax.experimental import pallas as pl
from jax.experimental.pallas import tpu as pltpu
from jax.sharding import Mesh
from jax.sharding import PartitionSpec as P

SP = ("sp_0", "sp_1", "sp_2")
SP_TP = ("sp_0", "sp_1", "sp_2", "tp")
MESH = pl.DeviceIdType.MESH
F32 = jnp.float32
BF16 = jnp.bfloat16
TAU = 16.0
EPS = 1e-06
BL = 64
GR = 256
DK = 128
DV = 256
NZ, NY = 4, 4
NCHIP = NZ * NY


def nt_dot(a, b):
    return lax.dot_general(a, b, (((1,), (1,)), ((), ())), preferred_element_type=F32)


def tn_dot(a, b):
    return lax.dot_general(a, b, (((0,), (0,)), ((), ())), preferred_element_type=F32)


def nn_dot(a, b):
    return lax.dot_general(a, b, (((1,), (0,)), ((), ())), preferred_element_type=F32)


def remote_copy(src, dst, send, recv, target):
    return pltpu.make_async_remote_copy(
        src, dst, send, recv, device_id=target, device_id_type=MESH)


class PlaneGather:
    SEMS = (40, 40, 32, 32, 1)

    def __init__(self, src, dst, sems):
        self.src, self.dst = src, dst
        self.send, self.recv, self.core_send, self.core_recv, self.local = sems
        self.at = {"z": lax.axis_index("sp_0"), "y": lax.axis_index("sp_1")}
        self.core, self.x = lax.axis_index("sp_2"), lax.axis_index("tp")
        self.rows = src.shape[0] // 2

    def shifted(self, moves):
        at = dict(self.at)
        for axis, k in moves:
            at[axis] = lax.rem(at[axis] + (k + 4), 4)
        return at["z"], at["y"]

    def chip_at(self, axis, k):
        z, y = self.shifted([(axis, k)])
        return z, y, self.core, self.x

    def piece(self, hf, ja, jb, sub=None):
        a, b = ("y", "z") if hf == 0 else ("z", "y")
        z, y = self.shifted([(a, ja), (b, jb)])
        row = ((z * NY + y) * 2 + self.core) * (2 * self.rows) + hf * self.rows
        size = self.rows
        if sub is not None:
            size = size // 2
            row = row + sub * size
        return self.dst.at[pl.ds(pl.multiple_of(row, 16), size)]

    def axis(self, hf, stage):
        return ("y", "z")[(hf + stage) % 2]

    OFFS = (0, -1, 1, 2)

    def hop(self, hf, stage, ja, way, forward):
        axis = self.axis(hf, stage)
        k = hf * 20 + (0 if stage == 0 else 4 + 4 * self.OFFS.index(ja)) + (0 if way > 0 else 1)
        k = k + (2 if forward else 0)
        target = self.chip_at(axis, way)
        if forward:
            sub = 0 if way > 0 else 1
            ref = self.piece(hf, -way, 0, sub) if stage == 0 else self.piece(hf, ja, -way, sub)
            src = ref
        else:
            ref = self.piece(hf, 0, 0) if stage == 0 else self.piece(hf, ja, 0)
            own = stage == 0 or ja == 0
            src = self.src.at[pl.ds(hf * self.rows, self.rows)] if own else ref
        return remote_copy(src, ref, self.send.at[k], self.recv.at[k], target)

    def landing(self, hf, stage, ja, way, forward):
        axis = self.axis(hf, stage)
        k = hf * 20 + (0 if stage == 0 else 4 + 4 * self.OFFS.index(ja)) + (0 if way > 0 else 1)
        k = k + (2 if forward else 0)
        back = 2 if forward else -way
        sub = (0 if way > 0 else 1) if forward else None
        ref = self.piece(hf, back, 0, sub) if stage == 0 else self.piece(hf, ja, back, sub)
        return remote_copy(ref, ref, self.send.at[k], self.recv.at[k], self.chip_at(axis, way))

    def hand(self, hf, ja, jb):
        p = hf * 16 + self.OFFS.index(ja) * 4 + self.OFFS.index(jb)
        ref = self.piece(hf, ja, jb)
        src = self.src.at[pl.ds(hf * self.rows, self.rows)] if ja == 0 and jb == 0 else ref
        partner = (self.at["z"], self.at["y"], 1 - self.core, self.x)
        return remote_copy(src, ref, self.core_send.at[p], self.core_recv.at[p], partner)

    def handed(self, hf, ja, jb):
        p = hf * 16 + self.OFFS.index(ja) * 4 + self.OFFS.index(jb)
        a, b = ("y", "z") if hf == 0 else ("z", "y")
        z, y = self.shifted([(a, ja), (b, jb)])
        row = ((z * NY + y) * 2 + 1 - self.core) * (2 * self.rows) + hf * self.rows
        ref = self.dst.at[pl.ds(pl.multiple_of(row, 16), self.rows)]
        partner = (self.at["z"], self.at["y"], 1 - self.core, self.x)
        return remote_copy(ref, ref, self.core_send.at[p], self.core_recv.at[p], partner)

    def keep(self):
        row = ((self.at["z"] * NY + self.at["y"]) * 2 + self.core) * (2 * self.rows)
        return pltpu.make_async_copy(
            self.src, self.dst.at[pl.ds(pl.multiple_of(row, 16), 2 * self.rows)], self.local.at[0])

    def start(self):
        for stage in range(2):
            for hf in range(2):
                for way in (1, -1):
                    self.hop(hf, stage, 0, way, False).start()
        for hf in range(2):
            self.hand(hf, 0, 0).start()
        self.keep().start()

    def second(self, hf, ja):
        for way in (1, -1):
            self.hop(hf, 1, ja, way, False).start()
        self.hand(hf, ja, 0).start()

    def near(self):
        for way in (1, -1):
            for hf in range(2):
                self.landing(hf, 0, 0, way, False).wait_recv()
                self.hop(hf, 0, 0, way, True).start()

    def near_second(self, hf):
        for way in (1, -1):
            self.second(hf, -way)

    def far(self):
        for hf in range(2):
            for way in (1, -1):
                self.landing(hf, 0, 0, way, True).wait_recv()
            self.second(hf, 2)

    def column(self, ja):
        for way in (1, -1):
            for hf in range(2):
                self.landing(hf, 1, ja, way, False).wait_recv()
                self.hop(hf, 1, ja, way, True).start()
                self.hand(hf, ja, -way).start()

    def column_far(self, ja):
        for hf in range(2):
            for way in (1, -1):
                self.landing(hf, 1, ja, way, True).wait_recv()
            self.hand(hf, ja, 2).start()

    def finish(self):
        self.keep().wait()
        for hf in range(2):
            for ja in self.OFFS:
                for jb in self.OFFS:
                    self.handed(hf, ja, jb).wait_recv()

    def drain(self):
        for hf in range(2):
            for way in (1, -1):
                for forward in (False, True):
                    self.hop(hf, 0, 0, way, forward).wait_send()
                    for ja in self.OFFS:
                        self.hop(hf, 1, ja, way, forward).wait_send()
            for ja in self.OFFS:
                for jb in self.OFFS:
                    self.hand(hf, ja, jb).wait_send()


class RowGather:
    SEMS = (6, 6, 3, 3)

    def __init__(self, rows, dst, sems):
        self.dst = dst
        self.send, self.recv, self.core_send, self.core_recv = sems
        self.z, self.y = lax.axis_index("sp_0"), lax.axis_index("sp_1")
        self.core, self.x = lax.axis_index("sp_2"), lax.axis_index("tp")
        self.rows = rows

    def piece(self, k, core, sub=None):
        size = self.rows // 2
        row = lax.rem(self.x + (k + 4), 4) * self.rows + core * size
        if sub is not None:
            size = size // 2
            row = row + sub * size
        return self.dst.at[pl.ds(pl.multiple_of(row, 16), size)]

    def side(self, way):
        return (self.z, self.y, self.core, lax.rem(self.x + (way + 4), 4))

    def copy(self, ref, k, way):
        return remote_copy(ref, ref, self.send.at[k], self.recv.at[k], self.side(way))

    def key(self, way, part):
        return (0 if way > 0 else 1) + 2 * part

    def hop(self, way, part):
        first = 0 if way > 0 else 1
        if part == 2:
            ref = self.piece(-way, self.core, first)
        else:
            ref = self.piece(0, self.core, first if part == 0 else 1 - first)
        return self.copy(ref, self.key(way, part), way)

    def landing(self, way, part):
        first = 0 if way > 0 else 1
        if part == 2:
            ref = self.piece(2, self.core, first)
        else:
            ref = self.piece(-way, self.core, first if part == 0 else 1 - first)
        return self.copy(ref, self.key(way, part), way)

    def hand(self, i, arriving=False):
        k = (-1, 1, 2)[i]
        ref = self.piece(k, 1 - self.core if arriving else self.core)
        return remote_copy(
            ref, ref, self.core_send.at[i], self.core_recv.at[i], (self.z, self.y, 1 - self.core, self.x))

    def start(self):
        for part in range(2):
            for way in (1, -1):
                self.hop(way, part).start()

    def near(self):
        for way in (1, -1):
            self.landing(way, 0).wait_recv()
            self.hop(way, 2).start()

    def near_hand(self):
        for i, way in enumerate((1, -1)):
            self.landing(way, 1).wait_recv()
            self.hand(i).start()

    def far(self):
        for way in (1, -1):
            self.landing(way, 2).wait_recv()
        self.hand(2).start()

    def finish(self):
        for i in range(3):
            self.hand(i, True).wait_recv()

    def drain(self):
        for way in (1, -1):
            for part in range(3):
                self.hop(way, part).wait_send()
        for i in range(3):
            self.hand(i).wait_send()


def plane_sems():
    return [pltpu.SemaphoreType.DMA((k,)) for k in PlaneGather.SEMS]


def layer_kernel(
    q_in, k_in, v_in, lg_in, gate_in, wo_in, stream_in, wg_in, wu_in, wd_in,
    bias_ref, extra_ref, doc_ref, gain_ref, ff_gain_ref,
    out_ref,
    q_ref, k_ref, v_ref, lg_ref, gate_ref, aux_ref, wg_ref, wu_ref, shard_ref, wd_ref,
    cum_ref, blk_ref, off_ref, states_ref, before_ref, run_ref, local_ref,
    own_t, own_e, part_t, part_e, chip_t, chip_e, ry_t, ry_e, row_t, row_e, rz_t, rz_e, mine_c, send_c, part_c, sum_ref,
    hm, st, wo_v, w_v, down_v, resid, normed, hidden, s2, s1, s3, ra, rb, rl, rr,
    local_sem, core_send, core_recv, t_send, t_recv, e_send, e_recv,
    own_rs, own_ls, fwd_rs, fwd_ls, left_in, right_in, opp_l, opp_r, rs_send, rs_recv,
    *gather_sems,
):
    rows = q_ref.shape[0]
    blocks = rows // BL
    groups = rows // GR
    per = GR // BL
    z, y = lax.axis_index("sp_0"), lax.axis_index("sp_1")
    core, me = lax.axis_index("sp_2"), lax.axis_index("tp")
    scale = DK ** (-0.5)
    n = 4
    q_rows = GR
    half = q_rows // 2
    d = out_ref.shape[1]
    units = hidden.shape[1]
    ix_r, ix_l = lax.rem(me + 1, n), lax.rem(me + n - 1, n)
    right, left = (z, y, core, ix_r), (z, y, core, ix_l)
    partner = (z, y, 1 - core, me)
    order = (2, 1, 3, 0)

    def quarter_of(owner, offset):
        return lax.rem(owner + offset, n)

    def along_y(k):
        return (z, lax.rem(y + k, NY), core, me)

    def along_z(k):
        return (lax.rem(z + k, NZ), y, core, me)

    wo_own = wo_in.shape[0]
    loads = {
        name: pltpu.make_async_copy(src, dst, local_sem.at[i])
        for i, (name, src, dst) in enumerate((
            ("wg", wg_in, wg_ref), ("wu", wu_in, wu_ref), ("wd", wd_in, wd_ref),
            ("wo", wo_in, wo_v.at[pl.ds(pl.multiple_of(me * wo_own, wo_own), wo_own)]),
            ("lg", lg_in, lg_ref), ("k", k_in, k_ref), ("v", v_in, v_ref), ("q", q_in, q_ref),
            ("gate", gate_in, gate_ref),
        ))
    }
    for copy in loads.values():
        copy.start()

    def load_stream(i):
        at = pl.multiple_of(quarter_of(me, order[i]) * q_rows, q_rows)
        return pltpu.make_async_copy(
            stream_in.at[pl.ds(at, q_rows)], st.at[i % 2], local_sem.at[9 + i])

    load_stream(0).start()
    load_stream(1).start()

    rz_t[pl.ds(z, 1)] = jnp.zeros((1, DV, DK), BF16)

    barrier = pltpu.get_barrier_semaphore()
    pl.semaphore_signal(barrier, inc=1, device_id=partner, device_id_type=MESH)
    pl.semaphore_signal(barrier, inc=1, device_id=right, device_id_type=MESH)
    pl.semaphore_signal(barrier, inc=1, device_id=left, device_id_type=MESH)
    for k in range(1, NY):
        pl.semaphore_signal(barrier, inc=1, device_id=along_y(k), device_id_type=MESH)
        pl.semaphore_signal(barrier, inc=1, device_id=along_z(k), device_id_type=MESH)

    loads["wg"].wait()
    loads["wu"].wait()
    for j in range(units // 128):
        shard_ref[:, j * 256 : j * 256 + 128] = wg_ref[:, j * 128 : (j + 1) * 128]
        shard_ref[:, j * 256 + 128 : (j + 1) * 256] = wu_ref[:, j * 128 : (j + 1) * 128]
    loads["wd"].wait()
    loads["wo"].wait()

    pl.semaphore_wait(barrier, 9)
    g1 = PlaneGather(shard_ref, w_v, gather_sems[:5])
    g2 = PlaneGather(wd_ref, down_v, gather_sems[5:10])
    ring = RowGather(wo_own, wo_v, gather_sems[10:])
    ring.start()
    g1.start()

    ri = lax.broadcasted_iota(jnp.int32, (GR, GR), 0)
    ci = lax.broadcasted_iota(jnp.int32, (GR, GR), 1)

    def columns(g, _):
        at = pl.multiple_of(g * GR, GR)
        for j in range(3):
            lanes = pl.ds(pl.multiple_of(g * GR, GR), GR)
            row = doc_ref[:, lanes].astype(F32) if j == 2 else extra_ref[j : j + 1, lanes]
            col = jnp.sum(jnp.where(ri == ci, row, 0.0), axis=1, keepdims=True)
            aux_ref[pl.ds(at, GR), j : j + 1] = col
        return 0

    lax.fori_loop(0, groups, columns, 0)
    loads["lg"].wait()
    loads["k"].wait()
    loads["v"].wait()
    run_ref[...] = jnp.zeros_like(run_ref)

    def doc_at(r):
        return aux_ref[pl.ds(r, 1), 2:3]

    def first(g, base):
        at = pl.multiple_of(g * GR, GR)
        same_block = (ri & (GR - BL)) == (ci & (GR - BL))
        tri = jnp.where(same_block & (ci <= ri), 1.0, 0.0).astype(BF16)
        logits = lg_ref[pl.ds(at, GR), :].astype(F32) + bias_ref[...]
        ld = (jnp.minimum(logits, 0.0) - jnp.log1p(jnp.exp(-jnp.abs(logits)))) / TAU
        extra0 = jnp.broadcast_to(aux_ref[pl.ds(at, GR), 0:1], (GR, DK))
        extra1 = jnp.broadcast_to(aux_ref[pl.ds(at, GR), 1:2], (GR, DK))
        ld = ld + jnp.concatenate([extra0, extra1], axis=1)
        hi = ld.astype(BF16)
        rest = ld - hi.astype(F32)
        mid = rest.astype(BF16)
        low = (rest - mid.astype(F32)).astype(BF16)
        cum = nn_dot(tri, hi) + nn_dot(tri, mid) + nn_dot(tri, low)
        cum_ref[pl.ds(at, GR), :] = cum
        cum3 = cum.reshape(per, BL, 2 * DK)
        ends = cum3[:, BL - 1 : BL, :]
        off = base
        for b in range(per):
            off_ref[pl.ds(g * per + b, 1)] = off[None]
            blk_ref[pl.ds(g * per + b, 1)] = ends[b : b + 1]
            off = off + ends[b]
        doc = aux_ref[pl.ds(at, GR), 2:3].reshape(per, BL, 1)
        tail_mask = jnp.where(doc == doc[:, BL - 1 : BL], 1.0, 0.0)
        head_mask = jnp.where(doc == doc[:, 0:1], 1.0, 0.0)
        kf = k_ref[pl.ds(at, GR), :].astype(F32).reshape(per, BL, 2 * DK)
        tail = (kf * jnp.exp(ends - cum3) * tail_mask).astype(BF16)
        head = (kf * jnp.exp(cum3) * head_mask).astype(BF16)
        for b in range(per):
            start = at + b * BL
            keep = jnp.where(doc_at(jnp.maximum(start - 1, 0)) == doc_at(start + BL - 1), 1.0, 0.0)
            decay = jnp.exp(ends[b]) * keep
            for h in range(2):
                c = slice(h * DK, (h + 1) * DK)
                keys = jnp.concatenate([tail[b][:, c], head[b][:, c]], axis=1)
                vals = v_ref[pl.ds(pl.multiple_of(start, BL), BL), h * DV : (h + 1) * DV]
                both = tn_dot(vals, keys)
                slot = (g * per + b) * 2 + h
                states_ref[pl.ds(slot, 1)] = both[None, :, DK:]
                fw = run_ref[h, :, :DK]
                before_ref[pl.ds(slot, 1), :, :DK] = fw.astype(BF16)[None]
                run_ref[h, :, :DK] = fw * decay[:, c] + both[:, :DK]
        return off

    total = lax.fori_loop(0, groups, first, jnp.zeros((1, 2 * DK), F32))
    sum_ref[...] = total

    def step(b, _):
        r = blocks - 1 - b
        hi = jnp.minimum(r * BL + BL, rows - 1)
        keep = jnp.where(doc_at(hi) == doc_at(r * BL), 1.0, 0.0)
        decay = jnp.exp(blk_ref[pl.ds(r, 1)][0]) * keep
        for h in range(2):
            bw = run_ref[h, :, DK:]
            before_ref[pl.ds(r * 2 + h, 1), :, DK:] = bw.astype(BF16)[None]
            run_ref[h, :, DK:] = bw * decay[:, h * DK : (h + 1) * DK] + states_ref[r * 2 + h]
        return 0

    lax.fori_loop(0, blocks, step, 0)
    first_doc = jnp.broadcast_to(doc_at(0), (1, DK))
    last_doc = jnp.broadcast_to(doc_at(rows - 1), (1, DK))
    for h in range(2):
        own_t[h, :DV] = run_ref[h, :, :DK].astype(BF16)
        own_t[h, DV:] = run_ref[h, :, DK:].astype(BF16)
        own_e[h, 0:1] = total[:, h * DK : (h + 1) * DK]
        own_e[h, 1:2] = first_doc
        own_e[h, 2:3] = last_doc
        own_e[h, 3:8] = jnp.zeros((5, DK), F32)

    swap_t = pltpu.make_async_remote_copy(
        own_t.at[1 - core], part_t, core_send.at[0], core_recv.at[0],
        device_id=partner, device_id_type=MESH)
    swap_e = pltpu.make_async_remote_copy(
        own_e.at[1 - core], part_e, core_send.at[1], core_recv.at[1],
        device_id=partner, device_id_type=MESH)
    swap_t.start()
    swap_e.start()
    g1.near()
    swap_t.wait()
    swap_e.wait()
    is0 = core == 0
    mine_e = own_e[pl.ds(core, 1)][0]
    other_e = part_e[...]
    e0 = jnp.where(is0, mine_e, other_e)
    e1 = jnp.where(is0, other_e, mine_e)
    mine_t = own_t[pl.ds(core, 1)][0].astype(F32)
    other_t = part_t[...].astype(F32)
    t0 = jnp.where(is0, mine_t, other_t)
    t1 = jnp.where(is0, other_t, mine_t)
    through1 = jnp.exp(e1[0:1]) * jnp.where(e0[2:3] == e1[2:3], 1.0, 0.0)
    through0 = jnp.exp(e0[0:1]) * jnp.where(e1[1:2] == e0[1:2], 1.0, 0.0)
    chip_t[0] = (t1[:DV] + through1 * t0[:DV]).astype(BF16)
    chip_t[1] = (t0[DV:] + through0 * t1[DV:]).astype(BF16)
    chip_row = jnp.concatenate(
        [e0[0:1] + e1[0:1], e0[1:2], e1[2:3], jnp.zeros((5, DK), F32)], axis=0)
    chip_e[...] = chip_row
    ry_e[pl.ds(y, 1)] = chip_row[None]
    ry_t[pl.ds(y, 1)] = chip_t[...][None]

    y_sends = []
    for k in range(1, NY):
        y_sends.append(remote_copy(chip_e, ry_e.at[y], e_send.at[k], e_recv.at[k], along_y(k)))
        y_sends.append(remote_copy(chip_t, ry_t.at[y], t_send.at[k], t_recv.at[k], along_y(k)))
    for s in y_sends:
        s.start()
    g1.near_second(0)
    g2.start()
    loads["q"].wait()

    def inside(g, _):
        at = pl.multiple_of(g * GR, GR)
        same_block = (ri & (GR - BL)) == (ci & (GR - BL))
        doc = aux_ref[pl.ds(at, GR), 2:3]
        same = same_block & (doc == doc_ref[:, pl.ds(at, GR)].astype(F32))
        below = same & (ci <= ri)
        above = same & (ci >= ri)
        cum3 = cum_ref[pl.ds(at, GR), :].reshape(per, BL, 2 * DK)
        middle = cum3[:, BL // 2 - 1 : BL // 2]
        ends = cum3[:, BL - 1 : BL]
        rising = jnp.exp(cum3 - middle)
        falling = jnp.exp(middle - cum3)
        qf = q_ref[pl.ds(at, GR), :].astype(F32).reshape(per, BL, 2 * DK) * scale
        kf = k_ref[pl.ds(at, GR), :].astype(F32).reshape(per, BL, 2 * DK)
        q_rise = (qf * rising).astype(BF16).reshape(GR, 2 * DK)
        q_fall = (qf * falling).astype(BF16).reshape(GR, 2 * DK)
        k_rise = (kf * rising).astype(BF16).reshape(GR, 2 * DK)
        k_fall = (kf * falling).astype(BF16).reshape(GR, 2 * DK)
        q_fwd = qf * jnp.exp(cum3)
        q_bwd = qf * jnp.exp(ends - cum3)
        for h in range(2):
            c = slice(h * DK, (h + 1) * DK)
            fw = nt_dot(q_rise[:, c], k_fall[:, c])
            bw = nt_dot(q_fall[:, c], k_rise[:, c])
            scores = jnp.where(below, fw, 0.0) + jnp.where(above, bw, 0.0)
            vals = v_ref[pl.ds(at, GR), h * DV : (h + 1) * DV]
            local_ref[pl.ds(at, GR), h * DV : (h + 1) * DV] = nn_dot(scores.astype(BF16), vals)
        for b in range(per):
            start = at + b * BL
            prev = doc_at(jnp.maximum(start - 1, 0))
            following = doc_at(jnp.minimum(start + BL, rows - 1))
            rows_doc = doc[b * BL : (b + 1) * BL]
            hit_f = jnp.where(rows_doc == prev, 1.0, 0.0)
            hit_b = jnp.where(rows_doc == following, 1.0, 0.0)
            for h in range(2):
                c = slice(h * DK, (h + 1) * DK)
                both = jnp.concatenate([q_fwd[b][:, c] * hit_f, q_bwd[b][:, c] * hit_b], axis=1)
                here = pl.ds(pl.multiple_of(start, BL), BL)
                local_ref[here, h * DV : (h + 1) * DV] += nt_dot(
                    both.astype(BF16), before_ref[(g * per + b) * 2 + h])
        return 0

    lax.fori_loop(0, groups // 2, inside, 0)
    g1.column(0)
    lax.fori_loop(groups // 2, groups, inside, 0)

    ring.near()
    for s in y_sends:
        s.wait()
    run_ref[0] = jnp.zeros_like(run_ref[0])

    def earlier(states, table):
        def body(j, _):
            e = table[j]
            p = table[jnp.maximum(j - 1, 0)]
            keep = jnp.exp(e[0:1]) * jnp.where(e[2:3] == p[2:3], 1.0, 0.0)
            run_ref[0, :, :DK] = states(j, 0).astype(F32) + run_ref[0, :, :DK] * keep
            return 0
        return body

    def later(states, table):
        def body(i, _):
            j = NY - 1 - i
            e = table[j]
            p = table[jnp.minimum(j + 1, NY - 1)]
            keep = jnp.exp(e[0:1]) * jnp.where(e[1:2] == p[1:2], 1.0, 0.0)
            run_ref[0, :, DK:] = states(j, 1).astype(F32) + run_ref[0, :, DK:] * keep
            return 0
        return body

    def row_state(j, way):
        return ry_t[j, way]

    def column_state(j, way):
        return rz_t[j]

    lax.fori_loop(0, y, earlier(row_state, ry_e), 0)
    lax.fori_loop(0, NY - 1 - y, later(row_state, ry_e), 0)
    run_ref[1] = run_ref[0]
    lax.fori_loop(y, NY, earlier(row_state, ry_e), 0)
    lax.fori_loop(NY - 1 - y, NY, later(row_state, ry_e), 0)
    row_t[0] = run_ref[0, :, :DK].astype(BF16)
    row_t[1] = run_ref[0, :, DK:].astype(BF16)
    in_row = [ry_e[j] for j in range(NY)]
    row_sum = in_row[0][0:1] + in_row[1][0:1] + in_row[2][0:1] + in_row[3][0:1]
    sum_before = jnp.zeros((1, DK), F32)
    sum_after = jnp.zeros((1, DK), F32)
    for j in range(NY):
        sum_before = sum_before + jnp.where(j < y, in_row[j][0:1], 0.0)
        sum_after = sum_after + jnp.where(j > y, in_row[j][0:1], 0.0)
    last_before = ry_e[jnp.maximum(y - 1, 0)][2:3]
    first_after = ry_e[jnp.minimum(y + 1, NY - 1)][1:2]
    row_row = jnp.concatenate(
        [row_sum, in_row[0][1:2], in_row[NY - 1][2:3], jnp.zeros((5, DK), F32)], axis=0)
    row_e[...] = row_row
    rz_e[pl.ds(z, 1)] = row_row[None]
    z_sends = []
    for k in range(1, NZ):
        back = jnp.where(lax.rem(z + k, NZ) > z, 0, 1)
        z_sends.append(
            remote_copy(row_e, rz_e.at[z], e_send.at[4 + k], e_recv.at[4 + k], along_z(k)))
        z_sends.append(
            remote_copy(row_t.at[back], rz_t.at[z], t_send.at[4 + k], t_recv.at[4 + k], along_z(k)))
    for s in z_sends:
        s.start()
    g1.near_second(1)
    g1.far()
    for s in z_sends:
        s.wait()
    g2.near()
    g2.near_second(0)
    g2.near_second(1)

    run_ref[0] = jnp.zeros_like(run_ref[0])
    lax.fori_loop(0, z, earlier(column_state, rz_e), 0)
    lax.fori_loop(0, NZ - 1 - z, later(column_state, rz_e), 0)
    prev_last = jnp.where(z > 0, rz_e[jnp.maximum(z - 1, 0)][2:3], -1.0)
    next_first = jnp.where(z < NZ - 1, rz_e[jnp.minimum(z + 1, NZ - 1)][1:2], -1.0)
    pass_f = jnp.exp(sum_before) * jnp.where(
        y == 0, 1.0, jnp.where(prev_last == last_before, 1.0, 0.0))
    pass_b = jnp.exp(sum_after) * jnp.where(
        y == NY - 1, 1.0, jnp.where(next_first == first_after, 1.0, 0.0))
    cf = run_ref[1, :, :DK] + pass_f * run_ref[0, :, :DK]
    cb = run_ref[1, :, DK:] + pass_b * run_ref[0, :, DK:]
    before_doc = jnp.where(y > 0, last_before, prev_last)
    after_doc = jnp.where(y < NY - 1, first_after, next_first)
    pass0 = jnp.exp(e0[0:1]) * jnp.where(before_doc == e0[2:3], 1.0, 0.0)
    pass1 = jnp.exp(e1[0:1]) * jnp.where(after_doc == e1[1:2], 1.0, 0.0)
    mine_t = own_t[pl.ds(core, 1)][0].astype(F32)
    other_t = part_t[...].astype(F32)
    t0f = jnp.where(is0, mine_t[:DV], other_t[:DV])
    t1b = jnp.where(is0, other_t[DV:], mine_t[DV:])
    c0 = jnp.concatenate([cf, t1b + pass1 * cb], axis=1)
    c1 = jnp.concatenate([t0f + pass0 * cf, cb], axis=1)
    mine_c[...] = jnp.where(is0, c0, c1).astype(BF16)
    send_c[...] = jnp.where(is0, c1, c0).astype(BF16)
    swap_c = pltpu.make_async_remote_copy(
        send_c, part_c, core_send.at[2], core_recv.at[2],
        device_id=partner, device_id_type=MESH)
    swap_c.start()
    ring.near_hand()
    enter_f = jnp.where(is0, before_doc, e0[2:3])[:, 0:1]
    enter_b = jnp.where(is0, e1[1:2], after_doc)[:, 0:1]
    swap_c.wait()

    loads["gate"].wait()

    def last(g):
        at = pl.multiple_of(g * GR, GR)
        doc = aux_ref[pl.ds(at, GR), 2:3]
        hit_f = jnp.where(doc == enter_f, 1.0, 0.0)
        hit_b = jnp.where(doc == enter_b, 1.0, 0.0)
        glob = cum_ref[pl.ds(at, GR), :].reshape(per, BL, 2 * DK) + off_ref[pl.ds(g * per, per)]
        glob = glob.reshape(GR, 2 * DK)
        qf = q_ref[pl.ds(at, GR), :].astype(F32) * scale
        q_fwd = (qf * jnp.exp(glob) * hit_f).astype(BF16)
        q_bwd = (qf * jnp.exp(sum_ref[...] - glob) * hit_b).astype(BF16)
        gain = gain_ref[...].astype(F32).reshape(1, DV)
        for h in range(2):
            c = slice(h * DK, (h + 1) * DK)
            both = jnp.concatenate([q_fwd[:, c], q_bwd[:, c]], axis=1)
            carry = jnp.where(h == core, mine_c[...], part_c[...])
            out = local_ref[pl.ds(at, GR), h * DV : (h + 1) * DV] + nt_dot(both, carry)
            out = out * lax.rsqrt(jnp.mean(out * out, axis=-1, keepdims=True) + EPS) * gain
            u = gate_ref[pl.ds(at, GR), h * DV : (h + 1) * DV].astype(F32)
            hm[pl.ds(at, GR), pl.ds(pl.multiple_of(me * 2 * DV + h * DV, DV), DV)] = (
                out * (u / (1.0 + jnp.exp(-u)))).astype(BF16)

    def three(i, _):
        last(quarter_of(me, i + i // 2))
        return 0

    lax.fori_loop(0, 3, three, 0)

    def piece(slot, r, part):
        return hm.at[
            pl.ds(pl.multiple_of(r * q_rows + part * half, half), half),
            pl.ds(pl.multiple_of(slot * 2 * DV, 2 * DV), 2 * DV)]

    def remote(ref, send, recv, target, dst=None):
        return pltpu.make_async_remote_copy(
            ref, ref if dst is None else dst, send, recv, device_id=target, device_id_type=MESH)

    def wire(slot, quarter, part, send, recv, target):
        return remote(piece(slot, quarter, part), send, recv, target)

    to_right = (((0, 0), (3, 0), (3, 1)), ((2, 0), (2, 1)), ((1, 0), (0, 1)), ((1, 1),))
    to_left = (((0, 1), (1, 1), (1, 0)), ((3, 1), (0, 0)), ((2, 1), (2, 0)), ((3, 0),))

    def own_right(o, p):
        return wire(me, quarter_of(me, o), p, own_rs.at[o * 2 + p], left_in.at[o * 2 + p], right)

    def own_left(o, p):
        return wire(me, quarter_of(me, o), p, own_ls.at[o * 2 + p], right_in.at[o * 2 + p], left)

    def came_left(o, p):
        return wire(ix_l, quarter_of(ix_l, o), p, own_rs.at[o * 2 + p], left_in.at[o * 2 + p], right)

    def came_right(o, p):
        return wire(ix_r, quarter_of(ix_r, o), p, own_ls.at[o * 2 + p], right_in.at[o * 2 + p], left)

    def fwd_right(i):
        return wire(ix_l, quarter_of(ix_r, order[i]), 0, fwd_rs.at[i], opp_l.at[i], right)

    def fwd_left(i):
        return wire(ix_r, quarter_of(ix_l, order[i]), 1, fwd_ls.at[i], opp_r.at[i], left)

    opposite = lax.rem(me + 2, n)

    def came_opp_l(i):
        return wire(opposite, quarter_of(me, order[i]), 0, fwd_rs.at[i], opp_l.at[i], right)

    def came_opp_r(i):
        return wire(opposite, quarter_of(me, order[i]), 1, fwd_ls.at[i], opp_r.at[i], left)

    def send_own(i):
        for k in range(len(to_right[i])):
            own_right(*to_right[i][k]).start()
            own_left(*to_left[i][k]).start()

    seen = set()

    def arrived(side, o, p):
        if (side, o, p) not in seen:
            seen.add((side, o, p))
            (came_left if side == "l" else came_right)(o, p).wait_recv()

    def pump(i):
        arrived("l", (2 + order[i]) % n, 0)
        fwd_right(i).start()
        arrived("r", (n - 2 + order[i]) % n, 1)
        fwd_left(i).start()

    send_own(0)
    last(quarter_of(me, 2))
    for ja in (-1, 1):
        g1.column(ja)
    g2.column(0)
    ring.far()
    pump(0)
    send_own(1)
    g1.column(2)
    g2.far()
    send_own(2)
    for ja in (0, -1, 1):
        g1.column_far(ja)
    for ja in (-1, 1):
        g2.column(ja)
    ring.finish()

    dh = d // 2
    to_r_a = remote(s2.at[:, pl.ds(0, dh)], rs_send.at[0], rs_recv.at[0], right, ra)
    to_l_b = remote(s2.at[:, pl.ds(dh, dh)], rs_send.at[1], rs_recv.at[1], left, rb)
    lo, up = pl.ds(0, dh), pl.ds(dh, dh)
    to_r = remote(s1.at[:, up], rs_send.at[2], rs_recv.at[2], right, rl.at[:, up])
    to_l = remote(s3.at[:, lo], rs_send.at[3], rs_recv.at[3], left, rr.at[:, lo])
    to_r_sum = remote(s1.at[:, lo], rs_send.at[4], rs_recv.at[4], right, rl.at[:, lo])
    to_l_sum = remote(s3.at[:, up], rs_send.at[5], rs_recv.at[5], left, rr.at[:, up])

    def prepare(i):
        at = pl.multiple_of(quarter_of(me, order[i]) * q_rows, q_rows)
        rows = pl.ds(at, q_rows)
        for p in range(2):
            arrived("l", (1 + order[i]) % n, p)
            arrived("r", (n - 1 + order[i]) % n, p)
        came_opp_l(i).wait_recv()
        came_opp_r(i).wait_recv()
        load_stream(i).wait()

        def project(j, total):
            cols = pl.ds(pl.multiple_of(j * 1024, 1024), 1024)
            acc = st[i % 2, :, cols].astype(F32) + nn_dot(hm[rows, :], wo_v[:, cols])
            resid[:, cols] = acc
            return total + jnp.sum(acc * acc, axis=-1, keepdims=True)

        squares = lax.fori_loop(0, d // 1024, project, jnp.zeros((q_rows, 1), F32))
        if i < n - 2:
            load_stream(i + 2).start()
        factor = lax.rsqrt(squares / d + EPS)
        normed[...] = (resid[...] * factor * ff_gain_ref[...].astype(F32).reshape(1, d)).astype(BF16)

    prepare(0)
    pump(1)
    send_own(3)
    g2.column(2)
    g1.column_far(2)
    for ja in (0, -1, 1):
        g2.column_far(ja)
    for i in range(n):
        if i == 0:
            g1.finish()
        else:
            prepare(i)

        def gate_up(at, width):
            both = nn_dot(normed[...], w_v[:, pl.ds(pl.multiple_of(at * 2, 256), 2 * width)])
            for b in range(width // 128):
                g = both[:, b * 256 : b * 256 + 128]
                u = both[:, b * 256 + 128 : (b + 1) * 256]
                hidden[:, pl.ds(pl.multiple_of(at + b * 128, 128), 128)] = (
                    g / (1.0 + jnp.exp(-g)) * u).astype(BF16)

        def gate_up_pair(j, _):
            gate_up(j * 256, 256)
            return 0

        lax.fori_loop(0, units // 256, gate_up_pair, 0)
        gate_up(units // 256 * 256, units % 256)
        if i == 0:
            g2.column_far(2)
            pump(2)
            pump(3)
            g2.finish()
        target = (s2, s1, s3, resid)[i]

        def down(j, _):
            cols = pl.ds(pl.multiple_of(j * 512, 512), 512)
            part = nt_dot(hidden[...], down_v[cols, :]).astype(BF16)
            if i < n - 1:
                target[:, cols] = part
            else:
                target[:, cols] = target[:, cols] + part.astype(F32)
            return 0

        tiles = d // 1024
        first_half, second_half = ((tiles, 2 * tiles), (0, tiles)) if i == 1 else (
            (0, tiles), (tiles, 2 * tiles))
        lax.fori_loop(*first_half, down, 0)
        if i == 0:
            to_r_a.start()
        if i == 1:
            to_r.start()
        if i == 2:
            to_l.start()
            to_r_a.wait_recv()
            s1[:, :dh] = (s1[:, :dh].astype(F32) + ra[...].astype(F32)).astype(BF16)
            to_r_sum.start()
        lax.fori_loop(*second_half, down, 0)
        if i == 0:
            to_l_b.start()
        if i == 2:
            to_l_b.wait_recv()
            s3[:, dh:] = (s3[:, dh:].astype(F32) + rb[...].astype(F32)).astype(BF16)
            to_l_sum.start()

    to_r.wait_recv()
    to_l.wait_recv()
    to_r_sum.wait_recv()
    to_l_sum.wait_recv()
    out_ref[...] = (resid[...] + rl[...].astype(F32) + rr[...].astype(F32)).astype(BF16)

    for o in range(n):
        for p in range(2):
            own_right(o, p).wait_send()
            own_left(o, p).wait_send()
    for i in range(n):
        fwd_right(i).wait_send()
        fwd_left(i).wait_send()
    g1.drain()
    g2.drain()
    ring.drain()
    to_r_a.wait_send()
    to_l_b.wait_send()
    to_r.wait_send()
    to_l.wait_send()
    to_r_sum.wait_send()
    to_l_sum.wait_send()


def layer(q, k, v, lg, bias, extra, doc, gate, gain, wo, stream, ff_gain, wg, wu, wd):
    rows, d = stream.shape
    units = wg.shape[1]
    vm = pl.BlockSpec(memory_space=pltpu.VMEM)
    hbm = pl.BlockSpec(memory_space=pl.ANY)
    blocks = rows // BL
    dma = pltpu.SemaphoreType.DMA

    def buf(*shape, dtype=BF16):
        return pltpu.VMEM(shape, dtype)

    return pl.pallas_call(
        layer_kernel,
        out_shape=jax.ShapeDtypeStruct((GR, d), BF16),
        in_specs=[hbm] * 10 + [vm] * 5,
        out_specs=vm,
        scratch_shapes=[
            buf(rows, 2 * DK), buf(rows, 2 * DK), buf(rows, 2 * DV), buf(rows, 2 * DK),
            buf(rows, 2 * DV), buf(rows, 3, dtype=F32),
            buf(*wg.shape), buf(*wu.shape), buf(wg.shape[0], 2 * units), buf(*wd.shape),
            buf(rows, 2 * DK, dtype=F32),
            buf(blocks, 1, 2 * DK, dtype=F32),
            buf(blocks, 1, 2 * DK, dtype=F32),
            buf(blocks * 2, DV, DK, dtype=F32),
            buf(blocks * 2, DV, 2 * DK),
            buf(2, DV, 2 * DK, dtype=F32),
            buf(rows, 2 * DV, dtype=F32),
            buf(2, 2 * DV, DK), buf(2, 8, DK, dtype=F32),
            buf(2 * DV, DK), buf(8, DK, dtype=F32),
            buf(2, DV, DK), buf(8, DK, dtype=F32),
            buf(NY, 2, DV, DK), buf(NY, 8, DK, dtype=F32),
            buf(2, DV, DK), buf(8, DK, dtype=F32),
            buf(NZ, DV, DK), buf(NZ, 8, DK, dtype=F32),
            buf(DV, 2 * DK), buf(DV, 2 * DK), buf(DV, 2 * DK),
            buf(1, 2 * DK, dtype=F32),
            buf(rows, 4 * 2 * DV), buf(2, GR, d), buf(4 * wo.shape[0], d),
            buf(2 * NCHIP * wg.shape[0], 2 * units), buf(2 * NCHIP * wd.shape[0], units),
            buf(GR, d, dtype=F32), buf(GR, d), buf(GR, units),
            buf(GR, d), buf(GR, d), buf(GR, d), buf(GR, d // 2), buf(GR, d // 2), buf(GR, d), buf(GR, d),
            dma((13,)), dma((3,)), dma((3,)),
            dma((8,)), dma((8,)), dma((8,)), dma((8,)),
            dma((8,)), dma((8,)), dma((4,)), dma((4,)),
            dma((8,)), dma((8,)), dma((4,)), dma((4,)), dma((6,)), dma((6,)),
        ] + plane_sems() + plane_sems() + [dma((k,)) for k in RowGather.SEMS],
        compiler_params=pltpu.CompilerParams(
            collective_id=0, has_side_effects=True, vmem_limit_bytes=67_043_328),
        cost_estimate=pl.CostEstimate(
            flops=29_000_000_000, bytes_accessed=16_000_000, transcendentals=0),
        name="layer",
    )(q, k, v, lg, gate, wo, stream, wg, wu, wd,
      bias.reshape(1, -1), extra.T, doc.reshape(1, -1), gain, ff_gain)


def per_device(
    stream, queries, projected_keys, values, decay_gate_logits, decay_gate_bias, extra_log_decay,
    document_index, output_gate, head_norm_gain, output_weight, feedforward_norm_gain,
    gate_weight, up_weight, down_weight,
):
    return layer(
        queries, projected_keys, values, decay_gate_logits, decay_gate_bias, extra_log_decay,
        document_index, output_gate, head_norm_gain, output_weight, stream,
        feedforward_norm_gain, gate_weight, up_weight, down_weight.T)


def solution(mesh):
    torus = Mesh(mesh.devices.reshape(4, 4, 2, mesh.shape["tp"]), ("sp_0", "sp_1", "sp_2", "tp"))
    placed = (
        P(SP, None), P(SP, "tp"), P(SP, "tp"), P(SP, "tp"), P(SP, "tp"), P("tp"), P(SP, "tp"),
        P(SP), P(SP, "tp"), P(), P("tp", None), P(), P(SP, "tp"), P(SP, "tp"), P("tp", SP),
    )
    return jax.shard_map(
        per_device, mesh=torus, in_specs=placed, out_specs=P(SP_TP, None), check_vma=False
    )
```
